32 devices in a mesh: sp: 8 (over z, x), tp: 4 (over y, core).
Axes of the slice: x: 2, y: 2, z: 4, core: 2. Of those that a mesh axis runs over, the one named last changes fastest.
Arguments:
- queries: bfloat16 [2048, 2048], P('sp', 'tp'), may hold values from -6 to 6
- key_matrix: bfloat16 [2048, 2048], P('sp', 'tp'), may hold values from -6 to 6
- value_matrix: bfloat16 [2048, 4096], P('sp', 'tp'), may hold values from -6 to 6
- output_gate_preactivation: bfloat16 [2048, 4096], P('sp', 'tp'), may hold values from -6 to 6
- decay_preactivation: bfloat16 [2048, 2048], P('sp', 'tp')
- extra_log_decay: float32 [2048, 16], P('sp', 'tp'), may hold values from -0.7 to 0
- head_norm_gain: bfloat16 [256], replicated, may hold values from 0.099609375 to 1.8984375
- output_projection: bfloat16 [4096, 2048], P(None, 'tp'), may hold values from -0.09375 to 0.09375
- residual: bfloat16 [2048, 2048], P('sp', 'tp'), may hold values from -210 to 210
- feedforward_gain: bfloat16 [2048], replicated, may hold values from 0.099609375 to 1.8984375
- routing: int32 [2048, 4], P('sp'), may hold values from 0 to 7, all different within a row; in each aligned block of 256 rows (0 to 255, 256 to 511, ...) at most 192 rows name the same one
- router_score: float32 [2048, 4], P('sp'), may hold values from 0.05 to 1
- expert_gate_weight: bfloat16 [2048, 8192], P(None, ('sp', 'tp')), may hold values from -0.125 to 0.125
- expert_up_weight: bfloat16 [2048, 8192], P(None, ('sp', 'tp')), may hold values from -0.125 to 0.125
- expert_down_weight: bfloat16 [8192, 2048], P(('sp', 'tp')), may hold values from -0.1875 to 0.1875
- shared_expert_gate: bfloat16 [2048, 512], P(None, 'tp'), may hold values from -0.125 to 0.125
- shared_expert_up: bfloat16 [2048, 512], P(None, 'tp'), may hold values from -0.125 to 0.125
- shared_expert_down: bfloat16 [512, 2048], P(None, 'tp'), may hold values from -0.25 to 0.25
Outputs:
- layer_out: bfloat16 [2048, 2048], P('sp', 'tp')
The draws below stay inside these ranges and needn't reach their ends.
Inputs may be any that keep to these rules, and one draw needn't show every extreme that they name: `routing`: each row names 4 different experts. In each aligned block of 256 rows, the rows of one index of sp, no expert is named by more than 192 rows, a bound that some expert reaches in some blocks.
All inputs are finite; a program needn't handle non-finite values.
Results may differ from the reference program's by a relative error of at most 0.01.
Values may be sent and summed in bfloat16 or wider, within the bound.
A program may use at most 128 MiB of HBM per device.

```python
import math
import jax
import jax.numpy as jnp
import numpy as np
from jax import lax

D = 2048
ATTENTION_HEADS = 16
DK = 128
DV = 256
BLOCK_POSITIONS = 64
FF = 1024
SF = 512
K = 4
TOK_DEV = 256
SEQUENCE_LENGTH = 2048
E = 8
MOST = 192
N_SP = 8


def draw_decay_preactivation(key, part):
    key_head, key_block, key_jitter = jax.random.split(key, 3)
    head_kind = jax.random.randint(key_head, (ATTENTION_HEADS,), 0, 2)
    slow_head = head_kind.astype(jnp.float32)
    slow_level = math.log(SEQUENCE_LENGTH / 4.0)
    base_level = 0.7 + slow_head * (slow_level - 0.7)
    block_shift = jax.random.uniform(key_block, (SEQUENCE_LENGTH // BLOCK_POSITIONS, 1, 1, 1), jnp.float32, -0.7, 0.7)
    jitter = jnp.clip(jax.random.normal(key_jitter, (SEQUENCE_LENGTH // BLOCK_POSITIONS, BLOCK_POSITIONS, ATTENTION_HEADS, DK), jnp.float32), -2.5, 2.5)
    logit = base_level[None, None, :, None] + block_shift + jitter
    return logit.reshape(SEQUENCE_LENGTH, ATTENTION_HEADS * DK).astype(jnp.bfloat16)


def draw_extra_log_decay(key, part):
    key_place, key_width = jax.random.split(key)
    third = SEQUENCE_LENGTH // 3
    position_list = jnp.arange(3, dtype=jnp.int32)[:, None] * third + jax.random.randint(key_place, (3, ATTENTION_HEADS), 0, third)
    spike_magnitude = jnp.log(jax.random.uniform(key_width, (3, ATTENTION_HEADS), jnp.float32, 0.5, 0.8))
    spike_positions = (jnp.arange(SEQUENCE_LENGTH, dtype=jnp.int32)[:, None, None] == position_list[None]).astype(jnp.float32)
    return jnp.sum(spike_positions * spike_magnitude[None], axis=1)


def draw_residual(key, part):
    key_row, key_col, key_value = jax.random.split(key, 3)
    column_pos = jnp.arange(D, dtype=jnp.float32) / D
    row_scale = jnp.exp(jax.random.uniform(key_row, (SEQUENCE_LENGTH,), jnp.float32, math.log(0.3), math.log(3.0)))
    column_rise = math.log(5.0)
    column_scale = 0.5 * jnp.exp(column_rise * column_pos) * jax.random.uniform(key_col, (D,), jnp.float32, 0.7, 1.4)
    values = jnp.clip(jax.random.normal(key_value, (SEQUENCE_LENGTH, D), jnp.float32), -5.0, 5.0)
    return (values * row_scale[:, None] * column_scale[None, :]).astype(jnp.bfloat16)


def level_of(own_key, shape, cuts, least, top_value):
    loudness, own = 1.0, jax.random.fold_in(own_key, 6)
    for axis_at, blocks in cuts:
        draws = jnp.exp(jax.random.uniform(jax.random.fold_in(own, axis_at), (blocks,), jnp.float32, least / len(cuts), top_value / len(cuts)))
        loudness = loudness * jnp.repeat(draws, shape[axis_at] // blocks).reshape([-1 if axis == axis_at else 1 for axis in range(len(shape))])
    return loudness


def assign_block(key, own, number, rows, amount, top, bound, slope):
    sequence = jax.random.permutation(key, amount)
    crowded, ordinary = portions_of(amount, rows * top, bound, slope, True), portions_of(amount, rows * top, bound, slope, False)
    places = jnp.arange(amount)

    def named(tallies, offset_by):
        used = int((tallies > 0).sum())
        fixed = max(1, used // 4)
        shifted = fixed + (places - fixed + offset_by * (used - fixed)) % max(1, amount - fixed)
        return jnp.zeros((amount,), jnp.int32).at[sequence[jnp.where(places < fixed, places, shifted)]].set(jnp.asarray(tallies, jnp.int32))

    tallies = jnp.where(number % 4 == 0, named(crowded, number // 4), named(ordinary, number - number // 4 - 1))
    mixed = jax.random.permutation(jax.random.fold_in(own, 3), amount)
    giver, sink = mixed[0:amount // 2 * 2:2], mixed[1:amount // 2 * 2:2]
    slack = jnp.minimum(tallies[giver] - 1, bound - tallies[sink]) // 2
    slack = jnp.where((giver == sequence[0]) | (sink == sequence[0]) | (tallies[sink] == 0), 0, jnp.maximum(slack, 0))
    shifted = jax.random.randint(jax.random.fold_in(own, 4), (amount // 2,), 0, 1 << 20) % (slack + 1)
    tallies = tallies.at[giver].add(-shifted).at[sink].add(shifted)
    labels = jnp.searchsorted(jnp.cumsum(tallies), jnp.arange(rows * top), side="right").astype(jnp.int32)
    grid = labels.reshape(top, rows).T
    grid = grid[jax.random.permutation(jax.random.fold_in(own, 1), rows)]
    offset_by = jax.random.randint(jax.random.fold_in(own, 2), (rows, 1), 0, top)
    return jnp.take_along_axis(grid, (jnp.arange(top)[None, :] + offset_by) % top, axis=1)


def portions_of(count, total, reach, skew, full):
    weights = [(1 << 20) // math.isqrt(grade ** skew) + 1 for grade in range(1, count + 1)]
    largest = reach if full else min(reach, max(-(-total // count), total * weights[0] // sum(weights)))
    least = 1 if total - largest >= count - 1 else 0
    counts, surplus = [largest] + [least] * (count - 1), total - largest - least * (count - 1)
    while surplus > 0:
        candidates = [i for i in range(1, count) if counts[i] < largest] or [i for i in range(1, count) if counts[i] < reach]
        pool, budget = sum([weights[i] for i in candidates]), surplus
        for i in candidates:
            extra = min(reach - counts[i], max(1, budget * weights[i] // pool), surplus)
            counts[i] = counts[i] + extra
            surplus = surplus - extra
    return np.array(counts)


def gaussian(rng, extent, deviation, bound, shards=(), held_as=jnp.bfloat16):
    entries = deviation * jax.random.normal(rng, extent, jnp.float32)
    if shards:
        entries = entries * level_of(rng, extent, shards, -0.22, 0.18)
    return jnp.clip(entries, -bound, bound).astype(held_as)


def setup_inputs(seed: int = 0) -> dict:
    keys = jax.random.split(jax.random.key(seed), 19)
    queries = gaussian(keys[0], (SEQUENCE_LENGTH, ATTENTION_HEADS * DK), 1.0, 6.0, ((0, 8), (1, 4)))
    key_matrix = gaussian(keys[1], (SEQUENCE_LENGTH, ATTENTION_HEADS * DK), 1.0, 6.0, ((0, 8), (1, 4)))
    value_matrix = gaussian(keys[2], (SEQUENCE_LENGTH, ATTENTION_HEADS * DV), 1.0, 6.0, ((0, 8), (1, 4)))
    output_gate_preactivation = gaussian(keys[3], (SEQUENCE_LENGTH, ATTENTION_HEADS * DV), 1.0, 6.0, ((0, 8), (1, 4)))
    decay_preactivation = draw_decay_preactivation(jax.random.fold_in(keys[18], 71), 0)
    extra_log_decay = draw_extra_log_decay(jax.random.fold_in(keys[18], 71), 0)
    head_norm_gain = jnp.clip(1.0 + 0.18 * jax.random.normal(keys[6], (DV,), jnp.float32), 0.099609375, 1.8984375).astype(jnp.bfloat16)
    output_projection = gaussian(keys[7], (ATTENTION_HEADS * DV, D), (ATTENTION_HEADS * DV) ** -0.5, 0.09375, ((1, 4),))
    residual = draw_residual(jax.random.fold_in(keys[18], 71), 0)
    feedforward_gain = jnp.clip(1.0 + 0.18 * jax.random.normal(keys[9], (D,), jnp.float32), 0.099609375, 1.8984375).astype(jnp.bfloat16)
    routing_keys = jax.random.split(jax.random.fold_in(keys[10], 1), SEQUENCE_LENGTH // TOK_DEV)
    routing_turns = jax.random.permutation(jax.random.fold_in(keys[10], 3), SEQUENCE_LENGTH // TOK_DEV)
    routing = jax.vmap(lambda own, number: assign_block(jax.random.fold_in(keys[10], 2), own, number, TOK_DEV, E, K, MOST, 1))(routing_keys, routing_turns).reshape((SEQUENCE_LENGTH, K))
    router_score = jnp.clip(jnp.exp(math.log(1.0) - 2.9957323 * jax.random.uniform(keys[11], (SEQUENCE_LENGTH, K), jnp.float32) ** level_of(keys[11], (SEQUENCE_LENGTH, K), ((0, 8),), -0.2, 0.2)), 0.05, 1.0)
    expert_gate_weight = gaussian(keys[12], (D, E * FF), D ** -0.5, 0.125, ((1, 32),))
    expert_up_weight = gaussian(keys[13], (D, E * FF), D ** -0.5, 0.125, ((1, 32),))
    expert_down_weight = gaussian(keys[14], (E * FF, D), FF ** -0.5, 0.1875, ((0, 32),))
    shared_expert_gate = gaussian(keys[15], (D, SF), D ** -0.5, 0.125, ((1, 4),))
    shared_expert_up = gaussian(keys[16], (D, SF), D ** -0.5, 0.125, ((1, 4),))
    shared_expert_down = gaussian(keys[17], (SF, D), SF ** -0.5, 0.25, ((1, 4),))
    return dict(queries=queries, key_matrix=key_matrix, value_matrix=value_matrix, output_gate_preactivation=output_gate_preactivation, decay_preactivation=decay_preactivation, extra_log_decay=extra_log_decay, head_norm_gain=head_norm_gain, output_projection=output_projection, residual=residual, feedforward_gain=feedforward_gain, routing=routing, router_score=router_score, expert_gate_weight=expert_gate_weight, expert_up_weight=expert_up_weight, expert_down_weight=expert_down_weight, shared_expert_gate=shared_expert_gate, shared_expert_up=shared_expert_up, shared_expert_down=shared_expert_down)


HIGHEST = lax.Precision.HIGHEST
EPSILON = 1e-06
ROUTE_SCALE = 2.5
GATE_TEMPER = 16.0

def attention_check(queries, key_matrix, value_matrix, decay_preactivation, extra_log_decay):
    block_count = SEQUENCE_LENGTH // BLOCK_POSITIONS
    query_block = queries.astype(jnp.float32).reshape(block_count, BLOCK_POSITIONS, ATTENTION_HEADS, DK) * DK ** (-0.5)
    key_block = key_matrix.astype(jnp.float32).reshape(block_count, BLOCK_POSITIONS, ATTENTION_HEADS, DK)
    value_block = value_matrix.astype(jnp.float32).reshape(block_count, BLOCK_POSITIONS, ATTENTION_HEADS, DV)
    log_decay_rows = jax.nn.log_sigmoid(decay_preactivation.astype(jnp.float32)).reshape(block_count, BLOCK_POSITIONS, ATTENTION_HEADS, DK) / GATE_TEMPER
    log_decay_rows = log_decay_rows + extra_log_decay.reshape(block_count, BLOCK_POSITIONS, ATTENTION_HEADS)[..., None]
    inside = jnp.cumsum(log_decay_rows, axis=1)
    block_total = inside[:, -1]
    query_decay = query_block * jnp.exp(inside)
    key_decay = key_block * jnp.exp(-inside)
    causal = jnp.tril(jnp.ones((BLOCK_POSITIONS, BLOCK_POSITIONS), dtype=bool))
    scores = jnp.where(causal, jnp.einsum('nthd,nshd->nhts', query_decay, key_decay, precision=HIGHEST), 0.0)
    within = jnp.einsum('nhts,nshv->nthv', scores, value_block, precision=HIGHEST)
    key_end = key_block * jnp.exp(block_total[:, None] - inside)

    def advance(carried, inputs):
        decay_sum, keys_end, values, queries_dec = inputs
        readout = jnp.einsum('thd,hdv->thv', queries_dec, carried, precision=HIGHEST)
        fresh_term = jnp.einsum('shd,shv->hdv', keys_end, values, precision=HIGHEST)
        return (jnp.exp(decay_sum)[..., None] * carried + fresh_term, readout)
    start_state = jnp.zeros((ATTENTION_HEADS, DK, DV), jnp.float32)
    _, passed = lax.scan(advance, start_state, (block_total, key_end, value_block, query_decay))
    return (within + passed).reshape(SEQUENCE_LENGTH, ATTENTION_HEADS, DV)

def reference(queries, key_matrix, value_matrix, output_gate_preactivation, decay_preactivation, extra_log_decay, head_norm_gain, output_projection, residual, feedforward_gain, routing, router_score, expert_gate_weight, expert_up_weight, expert_down_weight, shared_expert_gate, shared_expert_up, shared_expert_down):
    attention_output = attention_check(queries, key_matrix, value_matrix, decay_preactivation, extra_log_decay)
    inverse_rms = lax.rsqrt(lax.optimization_barrier(jnp.mean(attention_output * attention_output, axis=-1, keepdims=True)) + EPSILON)
    gate_act = jax.nn.silu(output_gate_preactivation.astype(jnp.float32).reshape(SEQUENCE_LENGTH, ATTENTION_HEADS, DV))
    head_rows = (attention_output * inverse_rms * head_norm_gain.astype(jnp.float32) * gate_act).reshape(SEQUENCE_LENGTH, ATTENTION_HEADS * DV).astype(jnp.bfloat16)
    mid_rows = (residual.astype(jnp.float32) + jnp.dot(head_rows, output_projection, preferred_element_type=jnp.float32)).astype(jnp.bfloat16)
    mid_float = mid_rows.astype(jnp.float32)
    normed = (mid_float * lax.rsqrt(lax.optimization_barrier(jnp.mean(mid_float * mid_float, axis=-1, keepdims=True)) + EPSILON) * feedforward_gain.astype(jnp.float32)).astype(jnp.bfloat16)
    route_weight = ROUTE_SCALE * router_score / lax.optimization_barrier(jnp.sum(router_score, axis=1, keepdims=True))
    flat_expert = routing.reshape(N_SP, TOK_DEV * K)
    one_hot = (flat_expert[..., None] == jnp.arange(E, dtype=jnp.int32)).astype(jnp.int32)
    rank_before = lax.optimization_barrier(jnp.sum((jnp.cumsum(one_hot, axis=1) - one_hot) * one_hot, axis=2))
    block_index = jnp.arange(N_SP, dtype=jnp.int32)[:, None]
    table_index = (flat_expert * (N_SP * MOST) + block_index * MOST + rank_before).reshape(-1).astype(jnp.int32)
    assign_token = jnp.arange(SEQUENCE_LENGTH * K, dtype=jnp.int32) // K
    slot_token = jnp.full((E * N_SP * MOST,), SEQUENCE_LENGTH, jnp.int32).at[table_index].set(assign_token)
    slot_weight = jnp.zeros((E * N_SP * MOST,), jnp.float32).at[table_index].set(route_weight.reshape(-1))
    padded = jnp.concatenate([normed, jnp.zeros((1, D), jnp.bfloat16)], axis=0)

    def expert_rows(inputs):
        token_ids, expert_id = inputs
        first = expert_id * FF
        gate_cols = lax.dynamic_slice_in_dim(expert_gate_weight, first, FF, 1)
        up_cols = lax.dynamic_slice_in_dim(expert_up_weight, first, FF, 1)
        down_rows = lax.dynamic_slice_in_dim(expert_down_weight, first, FF, 0)
        rows_in = padded[token_ids]
        hidden = (jax.nn.silu(jnp.dot(rows_in, gate_cols, preferred_element_type=jnp.float32)) * jnp.dot(rows_in, up_cols, preferred_element_type=jnp.float32)).astype(jnp.bfloat16)
        return jnp.dot(hidden, down_rows, preferred_element_type=jnp.float32).astype(jnp.bfloat16)
    expert_out = lax.map(expert_rows, (slot_token.reshape(E, N_SP * MOST), jnp.arange(E, dtype=jnp.int32)))
    weighted = expert_out.reshape(-1, D).astype(jnp.float32) * slot_weight[:, None]
    routed = jax.ops.segment_sum(weighted, slot_token, num_segments=SEQUENCE_LENGTH + 1)[:SEQUENCE_LENGTH]
    shared_hidden = (jax.nn.silu(jnp.dot(normed, shared_expert_gate, preferred_element_type=jnp.float32)) * jnp.dot(normed, shared_expert_up, preferred_element_type=jnp.float32)).astype(jnp.bfloat16)
    shared = jnp.dot(shared_hidden, shared_expert_down, preferred_element_type=jnp.float32)
    return (mid_float + routed + shared).astype(jnp.bfloat16)
```

```python
import functools

import jax
import jax.numpy as jnp
from jax import lax
from jax.experimental import pallas as pl
from jax.experimental.pallas import tpu as pltpu
from jax.sharding import PartitionSpec as P

DK = 128
DV = 256
BLOCK_POSITIONS = 64
FF_PARTS = 4
CHUNKS = 4


HIGHEST = lax.Precision.HIGHEST
EPSILON = 1e-06
ROUTE_SCALE = 2.5
GATE_TEMPER = 16.0


def from_partner(value, axis, bit, upward=False):
    mask = 2**bit
    pairs = [(source, source ^ mask) for source in range(lax.axis_size(axis))]
    if upward:
        pairs = [(source, target) for source, target in pairs if source < target]
    return lax.ppermute(value, axis, pairs)


def as_sent(value):
    return jax.tree.map(lambda a: a.astype(jnp.bfloat16) if a.dtype == jnp.float32 else a, value)


def carry_combine(first_part, second_part):
    return (
        first_part[0] * second_part[0],
        second_part[0][..., None] * first_part[1] + second_part[1],
    )


def choose(flag, yes, no):
    return jax.tree.map(lambda a, b: jnp.where(flag, a, b), yes, no)


def prefix(value, axis, join, neutral):
    place = lax.axis_index(axis)
    bits = lax.axis_size(axis).bit_length() - 1
    total, state = value, neutral
    for bit in range(bits):
        upper = (place >> bit) % 2 == 1
        last = bit == bits - 1
        arrived = jax.tree.map(
            lambda a: from_partner(a.astype(jnp.bfloat16), axis, bit, last).astype(a.dtype), total
        )
        state = choose(upper, join(arrived, state), state)
        if not last:
            total = choose(upper, join(arrived, total), join(total, arrived))
    return state


def relative_rows(matrix, place, masks):
    height = matrix.shape[0] // len(masks)
    return jnp.concatenate(
        [lax.dynamic_slice_in_dim(matrix, (place ^ mask) * height, height, 0) for mask in masks], 0
    )


def relative_columns(matrix, place, masks):
    width = matrix.shape[1] // len(masks)
    return jnp.concatenate(
        [lax.dynamic_slice_in_dim(matrix, (place ^ mask) * width, width, 1) for mask in masks], 1
    )


def masks_of(steps, axis):
    masks = [0]
    for step_axis, bit in steps:
        if step_axis == axis:
            masks = masks + [mask ^ (2**bit) for mask in masks]
    return masks


def spread(value, steps):
    for axis, bit in steps:
        arrived = from_partner(value, axis, bit)
        value = jnp.concatenate([value, arrived], 0 if axis == "sp" else 1)
    return value


def collect(value, steps):
    for axis, bit in reversed(steps):
        own, given = jnp.split(value, 2, 0 if axis == "sp" else 1)
        value = (
            own.astype(jnp.float32) + from_partner(given, axis, bit).astype(jnp.float32)
        ).astype(jnp.bfloat16)
    return value


def dot_halves(halves, matrix):
    parts = jnp.split(matrix, 2, 0)
    return sum(
        jnp.dot(half, part, preferred_element_type=jnp.float32)
        for half, part in zip(halves, parts)
    )


def dense_experts(
    mid_local,
    feedforward_gain,
    routing,
    router_score,
    expert_gate_weight,
    expert_up_weight,
    expert_down_weight,
    shared_expert_gate,
    shared_expert_up,
    shared_expert_down,
):
    tokens = mid_local.shape[0]
    hidden_width = expert_gate_weight.shape[1]
    sp_index, tp_index = lax.axis_index("sp"), lax.axis_index("tp")
    sp_steps = [("sp", bit) for bit in range(lax.axis_size("sp").bit_length() - 1)][::-1]
    tp_steps = [("tp", bit) for bit in range(lax.axis_size("tp").bit_length() - 1)][::-1]
    plans = (
        sp_steps + tp_steps,
        sp_steps[:-1] + tp_steps[:-1] + sp_steps[-1:] + tp_steps[-1:],
    )
    column_masks = masks_of(tp_steps, "tp")
    slab = mid_local.shape[1]
    gain = lax.dynamic_slice_in_dim(feedforward_gain, tp_index * slab, slab, 0)
    mid_float = mid_local.astype(jnp.float32)
    scaled = (mid_float * gain.astype(jnp.float32)).astype(jnp.bfloat16)
    squares = jnp.sum(mid_float * mid_float, axis=-1)
    for axis, bit in tp_steps:
        squares = squares + from_partner(squares, axis, bit)
    inverse_own = lax.rsqrt(squares / (slab * lax.axis_size("tp")) + EPSILON)
    inverse_here = spread(inverse_own[None], sp_steps)
    gate = relative_rows(expert_gate_weight, tp_index, column_masks)
    up = relative_rows(expert_up_weight, tp_index, column_masks)
    down = relative_columns(expert_down_weight, tp_index, column_masks)
    shared_gate = relative_rows(shared_expert_gate, tp_index, column_masks)
    shared_up = relative_rows(shared_expert_up, tp_index, column_masks)
    shared_down = relative_rows(shared_expert_down, tp_index, column_masks)
    route_weight = ROUTE_SCALE * router_score / jnp.sum(router_score, axis=1, keepdims=True)
    expert_ids = jnp.arange(lax.axis_size("sp"), dtype=jnp.int32)
    weight_table = jnp.sum(
        jnp.where(routing[:, :, None] == expert_ids, route_weight[:, :, None], 0.0), axis=1
    )
    weight_all = spread(weight_table.T[None], sp_steps)
    weight_here = lax.dynamic_index_in_dim(weight_all, sp_index, 1, False)
    rows = tokens // CHUNKS
    own_halves, routed = [], []
    for chunk in range(CHUNKS):
        steps = plans[chunk % 2]
        axis, bit = steps[-1]
        span = slice(chunk * rows, (chunk + 1) * rows)
        near = spread(scaled[span], steps[:-1])
        halves = (near, from_partner(near, axis, bit))
        own_halves.append([half[:rows] for half in halves])
        row_inverse = inverse_here[:, span].reshape(-1, 1)
        row_weight = weight_here[:, span].reshape(-1, 1)
        hidden = (
            jax.nn.silu(dot_halves(halves, gate) * row_inverse)
            * (dot_halves(halves, up) * row_inverse)
            * row_weight
        ).astype(jnp.bfloat16)
        kept_down, given_down = jnp.split(down, 2, 1)
        given = jnp.dot(hidden, given_down, preferred_element_type=jnp.float32).astype(jnp.bfloat16)
        kept = jnp.dot(hidden, kept_down, preferred_element_type=jnp.float32)
        summed = (kept + from_partner(given, axis, bit).astype(jnp.float32)).astype(jnp.bfloat16)
        routed.append(collect(summed, steps[:-1]))
    own_halves = [jnp.concatenate(parts, 0) for parts in zip(*own_halves)]
    shared_hidden = (
        jax.nn.silu(dot_halves(own_halves, shared_gate) * inverse_own[:, None])
        * (dot_halves(own_halves, shared_up) * inverse_own[:, None])
    ).astype(jnp.bfloat16)
    shared_out = jnp.dot(
        spread(shared_hidden, tp_steps), shared_down, preferred_element_type=jnp.float32
    )
    routed = jnp.concatenate(routed, 0).astype(jnp.float32)
    return (mid_float + routed + shared_out).astype(jnp.bfloat16)


SLAB_HALF = 256
EXPERT_PARTS = 3


def remote(source, target, send_sem, recv_sem, device):
    return pltpu.make_async_remote_copy(
        src_ref=source,
        dst_ref=target,
        send_sem=send_sem,
        recv_sem=recv_sem,
        device_id=device,
        device_id_type=pl.DeviceIdType.MESH,
    )


def swish(value):
    return value / (1.0 + jnp.exp(-value))


def exchange_kernel(
    most,
    mid_ref,
    gain_ref,
    table_ref,
    gate_hbm,
    up_hbm,
    down_hbm,
    shared_gate_hbm,
    shared_up_hbm,
    shared_down_hbm,
    out_ref,
    gate_ref,
    up_ref,
    down_ref,
    shared_gate_ref,
    shared_up_ref,
    shared_down_ref,
    tables,
    ranks,
    slot_weights,
    picks,
    own_rows,
    partner_high,
    core_rows,
    line_rows,
    side_out,
    expert_rows,
    hidden_rows,
    core_out,
    core_in,
    kept_rows,
    y_out,
    y_in,
    results,
    side_in,
    line_out,
    left_in,
    right_in,
    last_out,
    last_in,
    shared_hidden,
    routed,
    base,
    weight_sem,
    table_send,
    table_recv,
    own_send,
    own_recv,
    core_send,
    core_recv,
    left_send,
    right_send,
    line_recv,
    side_send,
    side_recv,
    y_send,
    y_recv,
    pair_send,
    pair_recv,
    back_core_send,
    back_core_recv,
    back_y_send,
    back_y_recv,
    back_side_send,
    back_side_recv,
    back_line_send,
    left_recv,
    right_recv,
    shared_send,
    shared_recv,
    last_send,
    last_recv,
):
    bf16, f32 = jnp.bfloat16, jnp.float32
    sp_count, tp_count = lax.axis_size("sp"), lax.axis_size("tp")
    depth = sp_count // 2
    tokens = mid_ref.shape[0]
    half = mid_ref.shape[1] // 2
    parts = 2 * tp_count
    width = half * parts
    sp, tp = lax.axis_index("sp"), lax.axis_index("tp")
    z, x = sp // 2, sp % 2
    y, core = tp // 2, tp % 2
    tp_y = (1 - y) * 2 + core
    tp_core = y * 2 + (1 - core)
    side = (z * 2 + 1 - x, tp)
    over_y = (sp, tp_y)
    over_core = (sp, tp_core)
    left, right = (sp - 2, tp), (sp + 2, tp)
    has_left, has_right = z > 0, z < depth - 1
    pending = []

    def begin(copy, when=None):
        if when is None:
            copy.start()
        else:
            pl.when(when)(copy.start)
        pending.append((copy, when))

    def arrive(target, sem):
        remote(target, target, weight_sem.at[0], sem, (sp, tp)).wait_recv()

    order = [
        z,
        jnp.where(z == 0, 1, jnp.where(z == 1, 0, jnp.where(z == 2, 3, 2))),
        jnp.where(z == 0, 2, jnp.where(z == 1, 2, jnp.where(z == 2, 1, 1))),
        jnp.where(z == 0, 3, jnp.where(z == 1, 3, 0)),
    ]
    back_order = [
        jnp.where(z == 0, 1, jnp.where(z == 1, 2, jnp.where(z == 2, 1, 2))),
        jnp.where(z == 0, 2, jnp.where(z == 1, 3, jnp.where(z == 2, 0, 1))),
        jnp.where(z == 0, 3, jnp.where(z == 1, 0, jnp.where(z == 2, 3, 0))),
        z,
    ]

    barrier = pltpu.get_barrier_semaphore()
    peers = [(lax.rem(sp + step, sp_count), tp) for step in range(1, sp_count)]
    peers += [(sp, lax.rem(tp + step, tp_count)) for step in range(1, tp_count)]
    for peer in peers:
        pl.semaphore_signal(barrier, inc=1, device_id=peer, device_id_type=pl.DeviceIdType.MESH)
    weights = [
        (gate_hbm, gate_ref),
        (up_hbm, up_ref),
        (down_hbm, down_ref),
        (shared_gate_hbm, shared_gate_ref),
        (shared_up_hbm, shared_up_ref),
        (shared_down_hbm, shared_down_ref),
    ]
    loads = [
        pltpu.make_async_copy(hbm, vmem, weight_sem.at[number + 1])
        for number, (hbm, vmem) in enumerate(weights)
    ]
    for load in loads:
        load.start()
    pl.semaphore_wait(barrier, len(peers))

    low, high = mid_ref.at[:, pl.ds(0, half)], mid_ref.at[:, pl.ds(half, half)]
    for step in range(1, sp_count):
        peer = lax.rem(sp + step, sp_count)
        begin(
            remote(table_ref, tables.at[sp], table_send.at[step], table_recv.at[sp], (peer, tp))
        )
    begin(remote(low, line_rows.at[z, 2], own_send.at[0], own_recv.at[0], over_y))
    for part, source in ((0, high), (1, low)):
        target = line_rows.at[z, part]
        begin(remote(source, target, left_send.at[z, part], line_recv.at[z, part], left), has_left)
        begin(
            remote(source, target, right_send.at[z, part], line_recv.at[z, part], right), has_right
        )
    begin(remote(high, partner_high, own_send.at[1], own_recv.at[1], over_y))
    begin(remote(low, core_rows.at[0], core_send.at[0], core_recv.at[0], over_core))
    begin(remote(high, core_rows.at[1], core_send.at[1], core_recv.at[1], over_core))
    own_rows[0] = mid_ref[:, half:]
    own_rows[1] = mid_ref[:, :half]
    tables[sp] = table_ref[...]

    earlier = (
        lax.broadcasted_iota(jnp.int32, (tokens, tokens), 0)
        < lax.broadcasted_iota(jnp.int32, (tokens, tokens), 1)
    ).astype(f32).astype(bf16)
    slots = lax.broadcasted_iota(jnp.int32, (most, tokens), 0).astype(f32)

    def rank_block(source):
        chosen = tables[source] > 0.0
        counts = jnp.dot(
            jnp.where(chosen, 1.0, 0.0).astype(bf16), earlier, preferred_element_type=f32
        )
        ranks[source] = jnp.where(chosen, counts, -1.0)

    def pick(source, expert):
        return slots == ranks[source, pl.ds(expert, 1), :]

    def slot_block(source):
        weight = jnp.where(pick(source, sp), tables[source, pl.ds(sp, 1), :], 0.0)
        slot_weights[source] = jnp.broadcast_to(
            jnp.sum(weight, axis=1, keepdims=True), (most, 128)
        )

    def pick_block(depth_at):
        source = depth_at * 2 + x
        for number, expert in ((0, sp), (1, z * 2 + 1 - x)):
            picks[depth_at, pl.ds(number * most, most), :] = (
                jnp.where(pick(source, expert), 1.0, 0.0).astype(bf16)
            )

    def prepare(depth_at, first):
        for source in (depth_at * 2 + x, depth_at * 2 + 1 - x):
            if first:
                @pl.when(source != sp)
                def _():
                    arrive(tables.at[source], table_recv.at[source])
            else:
                arrive(tables.at[source], table_recv.at[source])
            rank_block(source)
            slot_block(source)
        pick_block(depth_at)

    prepare(order[0], True)
    arrive(line_rows.at[z, 2], own_recv.at[0])
    target = line_rows.at[z, 2]
    begin(remote(target, target, left_send.at[z, 2], line_recv.at[z, 2], left), has_left)
    begin(remote(target, target, right_send.at[z, 2], line_recv.at[z, 2], right), has_right)
    begin(remote(target, core_rows.at[2], core_send.at[2], core_recv.at[2], over_core))

    held = (tp * 2 + 1, tp * 2, tp_y * 2)
    late = tp_y * 2 + 1

    def to_core(number, source):
        ref = expert_rows.at[number, source]
        begin(
            remote(ref, ref, pair_send.at[number, source], pair_recv.at[number, source], over_core)
        )

    def to_y(source):
        ref = expert_rows.at[held[0], source]
        begin(remote(ref, ref, y_send.at[source], y_recv.at[source], over_y))

    def lines(k):
        at = order[k]
        source = at * 2 + x
        for part in range(EXPERT_PARTS):
            if k > 0:
                ref = line_rows.at[at, part]
                arrive(ref, line_recv.at[at, part])
                begin(
                    remote(ref, ref, left_send.at[at, part], line_recv.at[at, part], left),
                    jnp.logical_and(at > z, has_left),
                )
                begin(
                    remote(ref, ref, right_send.at[at, part], line_recv.at[at, part], right),
                    jnp.logical_and(at < z, has_right),
                )
                rows = line_rows[at, part]
            else:
                rows = line_rows[z, 2] if part == 2 else own_rows[part]
            chosen = jnp.dot(picks[at], rows, preferred_element_type=f32).astype(bf16)
            side_out[at, part] = chosen[most:]
            begin(
                remote(
                    side_out.at[at, part],
                    expert_rows.at[held[part], source],
                    side_send.at[at, part],
                    side_recv.at[at, part],
                    side,
                )
            )
            expert_rows[held[part], source] = chosen[:most]
            if part == 0 and k > 0:
                to_y(source)
            to_core(held[part], source)
        if k == 0:
            arrive(partner_high, own_recv.at[1])
            begin(remote(partner_high, core_rows.at[3], core_send.at[3], core_recv.at[3], over_core))
            expert_rows[late, source] = jnp.dot(
                picks[at, pl.ds(0, most), :], partner_high[...], preferred_element_type=f32
            ).astype(bf16)
            to_core(late, source)

    def sides(k):
        at = order[k]
        source = at * 2 + 1 - x
        for part in range(EXPERT_PARTS):
            arrive(expert_rows.at[held[part], source], side_recv.at[at, part])
            if part == 0:
                to_y(source)
            to_core(held[part], source)

    def lates(k, which):
        at = order[k]
        source = at * 2 + (x if which == 0 else 1 - x)
        arrive(expert_rows.at[late, source], y_recv.at[source])
        to_core(late, source)

    other_held = (tp_core * 2 + 1, tp_core * 2, ((1 - y) * 2 + 1 - core) * 2)
    other_late = ((1 - y) * 2 + 1 - core) * 2 + 1

    def experts(k):
        for which in range(2):
            source = order[k] * 2 + (x if which == 0 else 1 - x)
            for number in (*other_held, other_late):
                arrive(expert_rows.at[number, source], pair_recv.at[number, source])
            pieces, squares = [], None
            for number in range(parts):
                rows = expert_rows[number, source]
                pieces.append(rows * gain_ref[pl.ds(number, 1), :].astype(bf16))
                wide = rows.astype(f32)
                squares = wide * wide if squares is None else squares + wide * wide
            inverse = lax.rsqrt(jnp.sum(squares, axis=1, keepdims=True) / width + EPSILON)
            joined = jnp.concatenate(pieces, axis=1)
            gate = jnp.dot(joined, gate_ref[...], preferred_element_type=f32) * inverse
            up = jnp.dot(joined, up_ref[...], preferred_element_type=f32) * inverse
            hidden = (swish(gate) * up * slot_weights[source][:, :1]).astype(bf16)
            hidden_rows[source] = hidden
            for number, row in ((0, y), (1, 1 - y)):
                slab = (row * 2 + 1 - core) * (2 * half)
                block = down_ref[:, pl.ds(pl.multiple_of(slab, 2 * half), 2 * half)]
                core_out[source, number] = jnp.dot(
                    hidden, block, preferred_element_type=f32
                ).astype(bf16)
            begin(
                remote(
                    core_out.at[source],
                    core_in.at[source],
                    back_core_send.at[source],
                    back_core_recv.at[source],
                    over_core,
                )
            )

    def pairs(k):
        for which in range(2):
            source = order[k] * 2 + (x if which == 0 else 1 - x)
            arrive(core_in.at[source], back_core_recv.at[source])
            hidden = hidden_rows[source]

            def summed(number, row):
                slab = (row * 2 + core) * (2 * half)
                block = down_ref[:, pl.ds(pl.multiple_of(slab, 2 * half), 2 * half)]
                return jnp.dot(hidden, block, preferred_element_type=f32) + core_in[
                    source, number
                ].astype(f32)

            other = summed(1, 1 - y)
            y_out[source] = other[:, half:].astype(bf16)
            begin(
                remote(
                    y_out.at[source],
                    y_in.at[source],
                    back_y_send.at[source],
                    back_y_recv.at[source],
                    over_y,
                )
            )
            results[source, 2] = other[:, :half].astype(bf16)
            mine = summed(0, y)
            results[source, 1] = mine[:, :half].astype(bf16)
            kept_rows[source] = mine[:, half:]

    def ready(k):
        at = order[k]
        for which in (1, 0):
            source = at * 2 + (x if which == 0 else 1 - x)
            if which == 1:
                for part in (2, 1):
                    give_side(at, source, part)
            arrive(y_in.at[source], back_y_recv.at[source])
            results[source, 0] = (kept_rows[source] + y_in[source].astype(f32)).astype(bf16)
            if which == 1:
                give_side(at, source, 0)

    def give_side(at, source, part):
        begin(
            remote(
                results.at[source, part],
                side_in.at[at, part],
                back_side_send.at[at, part],
                back_side_recv.at[at, part],
                side,
            )
        )

    def spread_back(at, part):
        arrive(side_in.at[at, part], back_side_recv.at[at, part])
        rows = jnp.concatenate([results[at * 2 + x, part], side_in[at, part]], axis=0)
        return lax.dot_general(
            picks[at], rows, (((0,), (0,)), ((), ())), preferred_element_type=f32
        )

    def arrived(at, part):
        from_right = jnp.logical_and(at <= z, has_right)
        from_left = jnp.logical_and(at >= z, has_left)

        @pl.when(from_right)
        def _():
            arrive(right_in.at[at, part], right_recv.at[at, part])

        @pl.when(from_left)
        def _():
            arrive(left_in.at[at, part], left_recv.at[at, part])

        return jnp.where(from_right, right_in[at, part].astype(f32), 0.0) + jnp.where(
            from_left, left_in[at, part].astype(f32), 0.0
        )

    def back_lines(k):
        at = back_order[k]
        for part in (2, 1, 0):
            routed[part] = spread_back(at, part) + arrived(at, part)
            line_out[at, part] = routed[part].astype(bf16)
            source = line_out.at[at, part]
            begin(
                remote(
                    source,
                    right_in.at[at, part],
                    back_line_send.at[at, part],
                    right_recv.at[at, part],
                    left,
                ),
                at < z,
            )
            begin(
                remote(
                    source,
                    left_in.at[at, part],
                    back_line_send.at[at, part],
                    left_recv.at[at, part],
                    right,
                ),
                at > z,
            )

    def own_lines(part):
        routed[part] = spread_back(z, part) + arrived(z, part)

    def shared_first():
        for number in range(4):
            arrive(core_rows.at[number], core_recv.at[number])
        blocks = [
            (own_rows[1], tp * 2),
            (own_rows[0], tp * 2 + 1),
            (line_rows[z, 2], tp_y * 2),
            (partner_high[...], tp_y * 2 + 1),
            (core_rows[0], tp_core * 2),
            (core_rows[1], tp_core * 2 + 1),
            (core_rows[2], other_held[2]),
            (core_rows[3], other_late),
        ]
        squares = gate = up = 0.0
        for rows, number in blocks:
            wide = rows.astype(f32)
            squares = squares + wide * wide
            scaled = rows * gain_ref[pl.ds(number, 1), :].astype(bf16)
            span = pl.ds(pl.multiple_of(number * half, half), half)
            gate = gate + jnp.dot(scaled, shared_gate_ref[span, :], preferred_element_type=f32)
            up = up + jnp.dot(scaled, shared_up_ref[span, :], preferred_element_type=f32)
        inverse = lax.rsqrt(jnp.sum(squares, axis=1, keepdims=True) / width + EPSILON)
        shared_hidden[tp] = (swish(gate * inverse) * (up * inverse)).astype(bf16)
        for step in range(1, tp_count):
            peer = lax.rem(tp + step, tp_count)
            begin(
                remote(
                    shared_hidden.at[tp],
                    shared_hidden.at[tp],
                    shared_send.at[step],
                    shared_recv.at[tp],
                    (sp, peer),
                )
            )

    def shared_second():
        for step in range(1, tp_count):
            peer = lax.rem(tp + step, tp_count)
            arrive(shared_hidden.at[peer], shared_recv.at[peer])
        joined = jnp.concatenate([shared_hidden[number] for number in range(tp_count)], axis=1)
        base[...] = mid_ref[...].astype(f32) + jnp.dot(
            joined, shared_down_ref[...], preferred_element_type=f32
        )

    lines(0)
    for k in range(1, depth):
        prepare(order[k], False)
    for load in loads:
        load.wait()
    sides(0)
    shared_first()
    lines(1)
    lates(0, 1)
    experts(0)
    sides(1)
    lines(2)
    lates(1, 0)
    lates(1, 1)
    experts(1)
    pairs(0)
    sides(2)
    lines(3)
    lates(2, 0)
    lates(2, 1)
    experts(2)
    pairs(1)
    ready(0)
    sides(3)
    lates(3, 0)
    lates(3, 1)
    experts(3)
    pairs(2)
    ready(1)
    pairs(3)
    ready(2)
    back_lines(0)
    ready(3)
    back_lines(1)
    back_lines(2)
    shared_second()
    own_lines(2)
    last_out[...] = routed[2].astype(bf16)
    begin(remote(last_out, last_in, last_send, last_recv, over_y))
    own_lines(1)
    own_lines(0)
    out_ref[:, half:] = (base[:, half:] + routed[0]).astype(bf16)
    arrive(last_in, last_recv)
    out_ref[:, :half] = (base[:, :half] + routed[1] + last_in[...].astype(f32)).astype(bf16)
    for copy, when in pending:
        if when is None:
            copy.wait_send()
        else:
            pl.when(when)(copy.wait_send)


def exchange_experts(
    mid_local,
    feedforward_gain,
    routing,
    router_score,
    expert_gate_weight,
    expert_up_weight,
    expert_down_weight,
    shared_expert_gate,
    shared_expert_up,
    shared_expert_down,
):
    sp_count, tp_count = lax.axis_size("sp"), lax.axis_size("tp")
    depth = sp_count // 2
    tokens, slab = mid_local.shape
    half = slab // 2
    parts = 2 * tp_count
    picked = routing.shape[1]
    most = 3 * tokens * picked // (2 * sp_count)
    route_weight = ROUTE_SCALE * router_score / jnp.sum(router_score, axis=1, keepdims=True)
    expert_ids = jnp.arange(sp_count, dtype=jnp.int32)
    table = jnp.sum(
        jnp.where(
            routing.T[None, :, :] == expert_ids[:, None, None], route_weight.T[None, :, :], 0.0
        ),
        axis=1,
    )
    gain = feedforward_gain.astype(jnp.float32).reshape(parts, half)
    bf16, f32 = jnp.bfloat16, jnp.float32
    vmem = pltpu.VMEM
    dma = pltpu.SemaphoreType.DMA
    hidden_width = expert_gate_weight.shape[1]
    in_vmem = pl.BlockSpec(memory_space=pltpu.VMEM)
    in_any = pl.BlockSpec(memory_space=pl.ANY)
    weights = (
        expert_gate_weight,
        expert_up_weight,
        expert_down_weight,
        shared_expert_gate,
        shared_expert_up,
        shared_expert_down,
    )
    return pl.pallas_call(
        functools.partial(exchange_kernel, most),
        name="exchange_experts",
        out_shape=jax.ShapeDtypeStruct(mid_local.shape, bf16),
        in_specs=[in_vmem] * 3 + [in_any] * len(weights),
        out_specs=in_vmem,
        scratch_shapes=[vmem(weight.shape, bf16) for weight in weights]
        + [
            vmem((sp_count, sp_count, tokens), f32),
            vmem((sp_count, sp_count, tokens), f32),
            vmem((sp_count, most, 128), f32),
            vmem((depth, 2 * most, tokens), bf16),
            vmem((2, tokens, half), bf16),
            vmem((tokens, half), bf16),
            vmem((4, tokens, half), bf16),
            vmem((depth, EXPERT_PARTS, tokens, half), bf16),
            vmem((depth, EXPERT_PARTS, most, half), bf16),
            vmem((parts, sp_count, most, half), bf16),
            vmem((sp_count, most, hidden_width), bf16),
            vmem((sp_count, 2, most, slab), bf16),
            vmem((sp_count, 2, most, slab), bf16),
            vmem((sp_count, most, half), f32),
            vmem((sp_count, most, half), bf16),
            vmem((sp_count, most, half), bf16),
            vmem((sp_count, EXPERT_PARTS, most, half), bf16),
            vmem((depth, EXPERT_PARTS, most, half), bf16),
            vmem((depth, EXPERT_PARTS, tokens, half), bf16),
            vmem((depth, EXPERT_PARTS, tokens, half), bf16),
            vmem((depth, EXPERT_PARTS, tokens, half), bf16),
            vmem((tokens, half), bf16),
            vmem((tokens, half), bf16),
            vmem((tp_count, tokens, shared_expert_gate.shape[1]), bf16),
            vmem((EXPERT_PARTS, tokens, half), f32),
            vmem((tokens, slab), f32),
            dma((len(weights) + 1,)),
            dma((sp_count,)),
            dma((sp_count,)),
            dma((2,)),
            dma((2,)),
            dma((4,)),
            dma((4,)),
            dma((depth, EXPERT_PARTS)),
            dma((depth, EXPERT_PARTS)),
            dma((depth, EXPERT_PARTS)),
            dma((depth, EXPERT_PARTS)),
            dma((depth, EXPERT_PARTS)),
            dma((sp_count,)),
            dma((sp_count,)),
            dma((parts, sp_count)),
            dma((parts, sp_count)),
            dma((sp_count,)),
            dma((sp_count,)),
            dma((sp_count,)),
            dma((sp_count,)),
            dma((depth, EXPERT_PARTS)),
            dma((depth, EXPERT_PARTS)),
            dma((depth, EXPERT_PARTS)),
            dma((depth, EXPERT_PARTS)),
            dma((depth, EXPERT_PARTS)),
            dma((tp_count,)),
            dma((tp_count,)),
            dma,
            dma,
        ],
        compiler_params=pltpu.CompilerParams(
            collective_id=1, has_side_effects=True, vmem_limit_bytes=60 * 1024 * 1024
        ),
    )(mid_local, gain, table, *weights)


def attention_heads(queries, key_matrix, value_matrix, decay_preactivation, extra_log_decay):
    tokens = queries.shape[0]
    local_head_count = extra_log_decay.shape[1]
    block_count = tokens // BLOCK_POSITIONS
    query_block = queries.astype(jnp.float32).reshape(
        block_count, BLOCK_POSITIONS, local_head_count, DK
    ) * DK ** (-0.5)
    key_block = key_matrix.astype(jnp.float32).reshape(
        block_count, BLOCK_POSITIONS, local_head_count, DK
    )
    value_block = value_matrix.astype(jnp.float32).reshape(
        block_count, BLOCK_POSITIONS, local_head_count, DV
    )
    log_decay_rows = (
        jax.nn.log_sigmoid(decay_preactivation.astype(jnp.float32)).reshape(
            block_count, BLOCK_POSITIONS, local_head_count, DK
        )
        / GATE_TEMPER
    )
    log_decay_rows = (
        log_decay_rows
        + extra_log_decay.reshape(block_count, BLOCK_POSITIONS, local_head_count)[..., None]
    )
    inside = jnp.cumsum(log_decay_rows, axis=1)
    block_total = inside[:, -1]
    query_decay = query_block * jnp.exp(inside)
    key_decay = key_block * jnp.exp(-inside)
    causal = jnp.tril(jnp.ones((BLOCK_POSITIONS, BLOCK_POSITIONS), dtype=bool))
    scores = jnp.where(
        causal, jnp.einsum("nthd,nshd->nhts", query_decay, key_decay, precision=HIGHEST), 0.0
    )
    within = jnp.einsum("nhts,nshv->nthv", scores, value_block, precision=HIGHEST)
    key_end = key_block * jnp.exp(block_total[:, None] - inside)
    update = jnp.einsum("nshd,nshv->nhdv", key_end, value_block, precision=HIGHEST)
    before = jnp.cumsum(block_total, axis=0) - block_total
    ending = jnp.concatenate([before, (before[-1] + block_total[-1])[None]], axis=0)
    after_block = before + block_total
    earlier_mask = jnp.arange(block_count + 1)[:, None] > jnp.arange(block_count)[None, :]
    span_logs = jnp.where(
        earlier_mask[:, :, None, None], ending[:, None] - after_block[None], -1e30
    )
    states = jnp.einsum("nmhd,mhdv->nhdv", jnp.exp(span_logs), update, precision=HIGHEST)
    passed = jnp.einsum("nthd,nhdv->nthv", query_decay, states[:block_count], precision=HIGHEST)
    query_start = query_block * jnp.exp(inside + before[:, None])
    return (within + passed, query_start, jnp.exp(ending[block_count]), states[block_count])


def body(
    queries,
    key_matrix,
    value_matrix,
    output_gate_preactivation,
    decay_preactivation,
    extra_log_decay,
    head_norm_gain,
    output_projection,
    residual,
    feedforward_gain,
    routing,
    router_score,
    expert_gate_weight,
    expert_up_weight,
    expert_down_weight,
    shared_expert_gate,
    shared_expert_up,
    shared_expert_down,
):
    tokens = queries.shape[0]
    local_head_count = extra_log_decay.shape[1]
    local_part, query_start, dev_decay, dev_update = attention_heads(
        queries, key_matrix, value_matrix, decay_preactivation, extra_log_decay
    )
    _, entering = prefix(
        (dev_decay, dev_update),
        "sp",
        carry_combine,
        (jnp.ones_like(dev_decay), jnp.zeros_like(dev_update)),
    )
    attention_output = local_part + jnp.einsum(
        "nthd,hdv->nthv", query_start, entering, precision=HIGHEST
    )
    attention_output = attention_output.reshape(tokens, local_head_count, DV)
    inverse_rms = lax.rsqrt(
        jnp.mean(attention_output * attention_output, axis=-1, keepdims=True) + EPSILON
    )
    gate_act = jax.nn.silu(
        output_gate_preactivation.astype(jnp.float32).reshape(tokens, local_head_count, DV)
    )
    head_rows = (
        (attention_output * inverse_rms * head_norm_gain.astype(jnp.float32) * gate_act)
        .reshape(tokens, local_head_count * DV)
        .astype(jnp.bfloat16)
    )
    tp_steps = [("tp", bit) for bit in range(lax.axis_size("tp").bit_length() - 1)][::-1]
    projected = jnp.dot(
        spread(head_rows, tp_steps),
        relative_rows(output_projection, lax.axis_index("tp"), masks_of(tp_steps, "tp")),
        preferred_element_type=jnp.float32,
    )
    mid_local = (residual.astype(jnp.float32) + projected).astype(jnp.bfloat16)
    most = 3 * tokens * routing.shape[1] // (2 * lax.axis_size("sp"))
    if lax.axis_size("tp") == FF_PARTS and lax.axis_size("sp") == 8:
        return exchange_experts(
            mid_local,
            feedforward_gain,
            routing,
            router_score,
            expert_gate_weight,
            expert_up_weight,
            expert_down_weight,
            shared_expert_gate,
            shared_expert_up,
            shared_expert_down,
        )
    mid_rows = lax.all_gather(mid_local, "tp", axis=1, tiled=True).astype(jnp.float32)
    normed = (
        mid_rows
        * lax.rsqrt(jnp.mean(mid_rows * mid_rows, axis=-1, keepdims=True) + EPSILON)
        * feedforward_gain.astype(jnp.float32)
    ).astype(jnp.bfloat16)
    shared_pre = jnp.dot(normed, shared_expert_gate, preferred_element_type=jnp.float32)
    shared_lin = jnp.dot(normed, shared_expert_up, preferred_element_type=jnp.float32)
    shared_hidden = (jax.nn.silu(shared_pre) * shared_lin).astype(jnp.bfloat16)
    senders = lax.axis_size("sp")
    tp_count = lax.axis_size("tp")
    tp_bits = tp_count.bit_length() - 1
    tp_index = lax.axis_index("tp")
    groups = tp_count // FF_PARTS
    group_here = tp_index // FF_PARTS
    part_here = tp_index % FF_PARTS
    model_width = normed.shape[1]
    picks = routing.shape[1]
    expert_total = senders * groups
    rows_most = max(2, 3 * tokens * picks // (2 * expert_total))
    slot_count = senders * rows_most
    flat_expert = routing.reshape(-1)
    one_hot = (flat_expert[:, None] == jnp.arange(expert_total, dtype=jnp.int32)[None, :]).astype(
        jnp.int32
    )
    rank_before = jnp.sum((jnp.cumsum(one_hot, axis=0) - one_hot) * one_hot, axis=1)
    owned = flat_expert % groups == group_here
    slot_index = jnp.where(owned, flat_expert // groups * rows_most + rank_before, slot_count)
    token_index = jnp.arange(flat_expert.shape[0], dtype=jnp.int32) // picks
    part_width = model_width // FF_PARTS
    normed_part = lax.dynamic_slice_in_dim(normed, part_here * part_width, part_width, 1)
    outgoing = (
        jnp.zeros((slot_count, part_width), jnp.bfloat16)
        .at[slot_index]
        .set(normed_part[token_index], mode="drop")
    )
    arrived = lax.all_to_all(
        outgoing.reshape(senders, rows_most, part_width),
        "sp",
        split_axis=0,
        concat_axis=0,
        tiled=True,
    )
    for bit in range(2):
        partner_cols = from_partner(arrived, "tp", bit)
        upper = (tp_index >> bit) % 2
        arrived = jnp.where(
            upper == 1,
            jnp.concatenate([partner_cols, arrived], axis=2),
            jnp.concatenate([arrived, partner_cols], axis=2),
        )
    rows_in = arrived.reshape(slot_count, model_width)
    gate_pre = jnp.dot(rows_in, expert_gate_weight, preferred_element_type=jnp.float32)
    up_pre = jnp.dot(rows_in, expert_up_weight, preferred_element_type=jnp.float32)
    routed_hidden = (jax.nn.silu(gate_pre) * up_pre).astype(jnp.bfloat16)
    partial_out = jnp.dot(routed_hidden, expert_down_weight, preferred_element_type=jnp.float32)
    slab_width = model_width // tp_count
    partial_out = partial_out.reshape(slot_count, groups, FF_PARTS, slab_width)
    for bit in (1, 0):
        paired = partial_out.reshape(slot_count, groups, 2, 2**bit, slab_width)
        upper = (tp_index >> bit) % 2
        kept = lax.dynamic_index_in_dim(paired, upper, 2, keepdims=False)
        given = lax.dynamic_index_in_dim(paired, 1 - upper, 2, keepdims=False)
        partial_out = kept + from_partner(given.astype(jnp.bfloat16), "tp", bit).astype(given.dtype)
    expert_out = partial_out.reshape(senders, rows_most, groups, slab_width).astype(jnp.bfloat16)
    shared_out = jnp.dot(
        lax.all_gather(shared_hidden, "tp", axis=1, tiled=True),
        shared_expert_down,
        preferred_element_type=jnp.float32,
    )
    returned = lax.all_to_all(expert_out, "sp", split_axis=0, concat_axis=0, tiled=True).reshape(
        slot_count, groups, slab_width
    )
    safe_slot = jnp.minimum(slot_index, slot_count - 1)
    route_weight = ROUTE_SCALE * router_score / jnp.sum(router_score, axis=1, keepdims=True)
    pair_weight = jnp.where(owned, route_weight.reshape(-1), 0.0)
    picked = returned[safe_slot].astype(jnp.float32) * pair_weight[:, None, None]
    routed_part = jnp.sum(picked.reshape(tokens, picks, groups, slab_width), axis=1)
    for bit in range(tp_bits - 1, 1, -1):
        paired = routed_part.reshape(tokens, 2, 2 ** (bit - 2), slab_width)
        upper = (tp_index >> bit) % 2
        kept = lax.dynamic_index_in_dim(paired, upper, 1, keepdims=False)
        given = lax.dynamic_index_in_dim(paired, 1 - upper, 1, keepdims=False)
        routed_part = kept + from_partner(as_sent(given), "tp", bit).astype(given.dtype)
    routed = routed_part.reshape(tokens, slab_width)
    return (mid_local.astype(jnp.float32) + routed + shared_out).astype(jnp.bfloat16)


def solution(mesh):
    return jax.shard_map(
        body,
        mesh=mesh,
        in_specs=(
            P("sp", "tp"),
            P("sp", "tp"),
            P("sp", "tp"),
            P("sp", "tp"),
            P("sp", "tp"),
            P("sp", "tp"),
            P(),
            P(None, "tp"),
            P("sp", "tp"),
            P(),
            P("sp", None),
            P("sp", None),
            P(None, ("sp", "tp")),
            P(None, ("sp", "tp")),
            P(("sp", "tp"), None),
            P(None, "tp"),
            P(None, "tp"),
            P(None, "tp"),
        ),
        out_specs=P("sp", "tp"),
        check_vma=False,
    )
```

```python
import functools

import jax
import jax.numpy as jnp
from jax import lax
from jax.experimental import pallas as pl
from jax.experimental.pallas import tpu as pltpu
from jax.sharding import PartitionSpec as P

DK = 128
DV = 256
BLOCK_POSITIONS = 64
FF_PARTS = 4

HIGHEST = lax.Precision.HIGHEST
EPSILON = 1e-06
ROUTE_SCALE = 2.5
GATE_TEMPER = 16.0


def from_partner(value, axis, bit, upward=False):
    mask = 2**bit
    pairs = [(source, source ^ mask) for source in range(lax.axis_size(axis))]
    if upward:
        pairs = [(source, target) for source, target in pairs if source < target]
    return lax.ppermute(value, axis, pairs)


def as_sent(value):
    return jax.tree.map(lambda a: a.astype(jnp.bfloat16) if a.dtype == jnp.float32 else a, value)


def carry_combine(first_part, second_part):
    return (
        first_part[0] * second_part[0],
        second_part[0][..., None] * first_part[1] + second_part[1],
    )


def choose(flag, yes, no):
    return jax.tree.map(lambda a, b: jnp.where(flag, a, b), yes, no)


def prefix(value, axis, join, neutral):
    place = lax.axis_index(axis)
    bits = lax.axis_size(axis).bit_length() - 1
    total, state = value, neutral
    for bit in range(bits):
        upper = (place >> bit) % 2 == 1
        last = bit == bits - 1
        arrived = jax.tree.map(
            lambda a: from_partner(a.astype(jnp.bfloat16), axis, bit, last).astype(a.dtype), total
        )
        state = choose(upper, join(arrived, state), state)
        if not last:
            total = choose(upper, join(arrived, total), join(total, arrived))
    return state


def relative_rows(matrix, place, masks):
    height = matrix.shape[0] // len(masks)
    return jnp.concatenate(
        [lax.dynamic_slice_in_dim(matrix, (place ^ mask) * height, height, 0) for mask in masks], 0
    )


def relative_columns(matrix, place, masks):
    width = matrix.shape[1] // len(masks)
    return jnp.concatenate(
        [lax.dynamic_slice_in_dim(matrix, (place ^ mask) * width, width, 1) for mask in masks], 1
    )


def masks_of(steps, axis):
    masks = [0]
    for step_axis, bit in steps:
        if step_axis == axis:
            masks = masks + [mask ^ (2**bit) for mask in masks]
    return masks


def spread(value, steps):
    for axis, bit in steps:
        arrived = from_partner(value, axis, bit)
        value = jnp.concatenate([value, arrived], 0 if axis == "sp" else 1)
    return value


def collect(value, steps):
    for axis, bit in reversed(steps):
        own, given = jnp.split(value, 2, 0 if axis == "sp" else 1)
        value = (
            own.astype(jnp.float32) + from_partner(given, axis, bit).astype(jnp.float32)
        ).astype(jnp.bfloat16)
    return value


EXPERT_PARTS = 3


def remote(source, target, send_sem, recv_sem, device):
    return pltpu.make_async_remote_copy(
        src_ref=source,
        dst_ref=target,
        send_sem=send_sem,
        recv_sem=recv_sem,
        device_id=device,
        device_id_type=pl.DeviceIdType.MESH,
    )


def swish(value):
    return value / (1.0 + jnp.exp(-value))


def exchange_kernel(
    most,
    mid_ref,
    gain_ref,
    routing_ref,
    score_ref,
    gate_hbm,
    up_hbm,
    down_hbm,
    shared_gate_hbm,
    shared_up_hbm,
    shared_down_hbm,
    out_ref,
    gate_ref,
    up_ref,
    down_ref,
    shared_gate_ref,
    shared_up_ref,
    shared_down_ref,
    table_ref,
    tables,
    ranks,
    slot_weights,
    picks,
    own_rows,
    partner_high,
    core_rows,
    line_rows,
    side_out,
    expert_rows,
    hidden_rows,
    core_out,
    core_in,
    kept_rows,
    y_out,
    y_in,
    results,
    side_in,
    line_out,
    left_in,
    right_in,
    last_out,
    last_in,
    shared_hidden,
    routed,
    base,
    weight_sem,
    table_send,
    table_recv,
    own_send,
    own_recv,
    core_send,
    core_recv,
    left_send,
    right_send,
    line_recv,
    side_send,
    side_recv,
    y_send,
    y_recv,
    pair_send,
    pair_recv,
    back_core_send,
    back_core_recv,
    back_y_send,
    back_y_recv,
    back_side_send,
    back_side_recv,
    back_line_send,
    left_recv,
    right_recv,
    shared_send,
    shared_recv,
    last_send,
    last_recv,
):
    bf16, f32 = jnp.bfloat16, jnp.float32
    sp_count, tp_count = lax.axis_size("sp"), lax.axis_size("tp")
    depth = sp_count // 2
    tokens = mid_ref.shape[0]
    half = mid_ref.shape[1] // 2
    parts = 2 * tp_count
    width = half * parts
    sp, tp = lax.axis_index("sp"), lax.axis_index("tp")
    z, x = sp // 2, sp % 2
    y, core = tp // 2, tp % 2
    tp_y = (1 - y) * 2 + core
    tp_core = y * 2 + (1 - core)
    side = (z * 2 + 1 - x, tp)
    over_y = (sp, tp_y)
    over_core = (sp, tp_core)
    left, right = (sp - 2, tp), (sp + 2, tp)
    has_left, has_right = z > 0, z < depth - 1
    pending = []

    def begin(copy, when=None):
        if when is None:
            copy.start()
        else:
            pl.when(when)(copy.start)
        pending.append((copy, when))

    def arrive(target, sem):
        remote(target, target, weight_sem.at[0], sem, (sp, tp)).wait_recv()

    order = [
        z,
        jnp.where(z == 0, 1, jnp.where(z == 1, 0, jnp.where(z == 2, 3, 2))),
        jnp.where(z == 0, 2, jnp.where(z == 1, 2, jnp.where(z == 2, 1, 1))),
        jnp.where(z == 0, 3, jnp.where(z == 1, 3, 0)),
    ]
    back_order = [
        jnp.where(z == 0, 1, jnp.where(z == 1, 2, jnp.where(z == 2, 1, 2))),
        jnp.where(z == 0, 2, jnp.where(z == 1, 3, jnp.where(z == 2, 0, 1))),
        jnp.where(z == 0, 3, jnp.where(z == 1, 0, jnp.where(z == 2, 3, 0))),
        z,
    ]

    barrier = pltpu.get_barrier_semaphore()
    peers = [(lax.rem(sp + step, sp_count), tp) for step in range(1, sp_count)]
    peers += [(sp, lax.rem(tp + step, tp_count)) for step in range(1, tp_count)]
    for peer in peers:
        pl.semaphore_signal(barrier, inc=1, device_id=peer, device_id_type=pl.DeviceIdType.MESH)
    weights = [
        (gate_hbm, gate_ref),
        (up_hbm, up_ref),
        (down_hbm, down_ref),
        (shared_gate_hbm, shared_gate_ref),
        (shared_up_hbm, shared_up_ref),
        (shared_down_hbm, shared_down_ref),
    ]
    loads = [
        pltpu.make_async_copy(hbm, vmem, weight_sem.at[number + 1])
        for number, (hbm, vmem) in enumerate(weights)
    ]
    for load in loads:
        load.start()
    score = score_ref[...]
    route_weight = ROUTE_SCALE * score / jnp.sum(score, axis=0, keepdims=True)
    experts_here = lax.broadcasted_iota(jnp.int32, table_ref.shape, 0)
    table = jnp.zeros(table_ref.shape, f32)
    for pick_at in range(score.shape[0]):
        table = table + jnp.where(
            routing_ref[pick_at : pick_at + 1, :] == experts_here,
            route_weight[pick_at : pick_at + 1, :],
            0.0,
        )
    table_ref[...] = table
    pl.semaphore_wait(barrier, len(peers))

    low, high = mid_ref.at[:, pl.ds(0, half)], mid_ref.at[:, pl.ds(half, half)]
    for step in range(1, sp_count):
        peer = lax.rem(sp + step, sp_count)
        begin(
            remote(table_ref, tables.at[sp], table_send.at[step], table_recv.at[sp], (peer, tp))
        )
    begin(remote(low, line_rows.at[z, 2], own_send.at[0], own_recv.at[0], over_y))
    for part, source in ((0, high), (1, low)):
        target = line_rows.at[z, part]
        begin(remote(source, target, left_send.at[z, part], line_recv.at[z, part], left), has_left)
        begin(
            remote(source, target, right_send.at[z, part], line_recv.at[z, part], right), has_right
        )
    begin(remote(high, partner_high, own_send.at[1], own_recv.at[1], over_y))
    begin(remote(low, core_rows.at[0], core_send.at[0], core_recv.at[0], over_core))
    begin(remote(high, core_rows.at[1], core_send.at[1], core_recv.at[1], over_core))
    own_rows[0] = mid_ref[:, half:]
    own_rows[1] = mid_ref[:, :half]
    tables[sp] = table_ref[...]

    earlier = (
        lax.broadcasted_iota(jnp.int32, (tokens, tokens), 0)
        < lax.broadcasted_iota(jnp.int32, (tokens, tokens), 1)
    ).astype(f32).astype(bf16)
    slots = lax.broadcasted_iota(jnp.int32, (most, tokens), 0).astype(f32)

    def rank_block(source):
        chosen = tables[source] > 0.0
        counts = jnp.dot(
            jnp.where(chosen, 1.0, 0.0).astype(bf16), earlier, preferred_element_type=f32
        )
        ranks[source] = jnp.where(chosen, counts, -1.0)

    def pick(source, expert):
        return slots == ranks[source, pl.ds(expert, 1), :]

    def slot_block(source):
        weight = jnp.where(pick(source, sp), tables[source, pl.ds(sp, 1), :], 0.0)
        slot_weights[source] = jnp.broadcast_to(
            jnp.sum(weight, axis=1, keepdims=True), (most, 128)
        )

    def pick_block(depth_at):
        source = depth_at * 2 + x
        for number, expert in ((0, sp), (1, z * 2 + 1 - x)):
            picks[depth_at, pl.ds(number * most, most), :] = (
                jnp.where(pick(source, expert), 1.0, 0.0).astype(bf16)
            )

    def prepare(depth_at, first):
        for source in (depth_at * 2 + x, depth_at * 2 + 1 - x):
            if first:
                @pl.when(source != sp)
                def _():
                    arrive(tables.at[source], table_recv.at[source])
            else:
                arrive(tables.at[source], table_recv.at[source])
            rank_block(source)
            slot_block(source)
        pick_block(depth_at)

    prepare(order[0], True)
    arrive(line_rows.at[z, 2], own_recv.at[0])
    target = line_rows.at[z, 2]
    begin(remote(target, target, left_send.at[z, 2], line_recv.at[z, 2], left), has_left)
    begin(remote(target, target, right_send.at[z, 2], line_recv.at[z, 2], right), has_right)
    begin(remote(target, core_rows.at[2], core_send.at[2], core_recv.at[2], over_core))

    held = (tp * 2 + 1, tp * 2, tp_y * 2)
    late = tp_y * 2 + 1

    def to_core(number, source):
        ref = expert_rows.at[number, source]
        begin(
            remote(ref, ref, pair_send.at[number, source], pair_recv.at[number, source], over_core)
        )

    def to_y(source):
        ref = expert_rows.at[held[0], source]
        begin(remote(ref, ref, y_send.at[source], y_recv.at[source], over_y))

    def lines(k):
        at = order[k]
        source = at * 2 + x
        for part in range(EXPERT_PARTS):
            if k > 0:
                ref = line_rows.at[at, part]
                arrive(ref, line_recv.at[at, part])
                begin(
                    remote(ref, ref, left_send.at[at, part], line_recv.at[at, part], left),
                    jnp.logical_and(at > z, has_left),
                )
                begin(
                    remote(ref, ref, right_send.at[at, part], line_recv.at[at, part], right),
                    jnp.logical_and(at < z, has_right),
                )
                rows = line_rows[at, part]
            else:
                rows = line_rows[z, 2] if part == 2 else own_rows[part]
            chosen = jnp.dot(picks[at], rows, preferred_element_type=f32).astype(bf16)
            side_out[at, part] = chosen[most:]
            begin(
                remote(
                    side_out.at[at, part],
                    expert_rows.at[held[part], source],
                    side_send.at[at, part],
                    side_recv.at[at, part],
                    side,
                )
            )
            expert_rows[held[part], source] = chosen[:most]
            if part == 0 and k > 0:
                to_y(source)
            to_core(held[part], source)
        if k == 0:
            arrive(partner_high, own_recv.at[1])
            begin(remote(partner_high, core_rows.at[3], core_send.at[3], core_recv.at[3], over_core))
            expert_rows[late, source] = jnp.dot(
                picks[at, pl.ds(0, most), :], partner_high[...], preferred_element_type=f32
            ).astype(bf16)
            to_core(late, source)

    def sides(k):
        at = order[k]
        source = at * 2 + 1 - x
        for part in range(EXPERT_PARTS):
            arrive(expert_rows.at[held[part], source], side_recv.at[at, part])
            if part == 0:
                to_y(source)
            to_core(held[part], source)

    def lates(k, which):
        at = order[k]
        source = at * 2 + (x if which == 0 else 1 - x)
        arrive(expert_rows.at[late, source], y_recv.at[source])
        to_core(late, source)

    other_held = (tp_core * 2 + 1, tp_core * 2, ((1 - y) * 2 + 1 - core) * 2)
    other_late = ((1 - y) * 2 + 1 - core) * 2 + 1

    def experts(k):
        for which in range(2):
            source = order[k] * 2 + (x if which == 0 else 1 - x)
            for number in (*other_held, other_late):
                arrive(expert_rows.at[number, source], pair_recv.at[number, source])
            pieces, squares = [], None
            for number in range(parts):
                rows = expert_rows[number, source]
                pieces.append(rows * gain_ref[:, number * half : (number + 1) * half])
                wide = rows.astype(f32)
                squares = wide * wide if squares is None else squares + wide * wide
            inverse = lax.rsqrt(jnp.sum(squares, axis=1, keepdims=True) / width + EPSILON)
            joined = jnp.concatenate(pieces, axis=1)
            gate = jnp.dot(joined, gate_ref[...], preferred_element_type=f32) * inverse
            up = jnp.dot(joined, up_ref[...], preferred_element_type=f32) * inverse
            hidden = (swish(gate) * up * slot_weights[source][:, :1]).astype(bf16)
            hidden_rows[source] = hidden
            for number, row in ((0, y), (1, 1 - y)):
                slab = (row * 2 + 1 - core) * (2 * half)
                block = down_ref[:, pl.ds(pl.multiple_of(slab, 2 * half), 2 * half)]
                core_out[source, number] = jnp.dot(
                    hidden, block, preferred_element_type=f32
                ).astype(bf16)
            begin(
                remote(
                    core_out.at[source],
                    core_in.at[source],
                    back_core_send.at[source],
                    back_core_recv.at[source],
                    over_core,
                )
            )

    def pairs(k):
        for which in range(2):
            source = order[k] * 2 + (x if which == 0 else 1 - x)
            arrive(core_in.at[source], back_core_recv.at[source])
            hidden = hidden_rows[source]

            def summed(number, row):
                slab = (row * 2 + core) * (2 * half)
                block = down_ref[:, pl.ds(pl.multiple_of(slab, 2 * half), 2 * half)]
                return jnp.dot(hidden, block, preferred_element_type=f32) + core_in[
                    source, number
                ].astype(f32)

            other = summed(1, 1 - y)
            y_out[source] = other[:, half:].astype(bf16)
            begin(
                remote(
                    y_out.at[source],
                    y_in.at[source],
                    back_y_send.at[source],
                    back_y_recv.at[source],
                    over_y,
                )
            )
            results[source, 2] = other[:, :half].astype(bf16)
            mine = summed(0, y)
            results[source, 1] = mine[:, :half].astype(bf16)
            kept_rows[source] = mine[:, half:]

    def ready(k):
        at = order[k]
        for which in (1, 0):
            source = at * 2 + (x if which == 0 else 1 - x)
            if which == 1:
                for part in (2, 1):
                    give_side(at, source, part)
            arrive(y_in.at[source], back_y_recv.at[source])
            results[source, 0] = (kept_rows[source] + y_in[source].astype(f32)).astype(bf16)
            if which == 1:
                give_side(at, source, 0)

    def give_side(at, source, part):
        begin(
            remote(
                results.at[source, part],
                side_in.at[at, part],
                back_side_send.at[at, part],
                back_side_recv.at[at, part],
                side,
            )
        )

    def spread_back(at, part):
        arrive(side_in.at[at, part], back_side_recv.at[at, part])
        rows = jnp.concatenate([results[at * 2 + x, part], side_in[at, part]], axis=0)
        return lax.dot_general(
            picks[at], rows, (((0,), (0,)), ((), ())), preferred_element_type=f32
        )

    def arrived(at, part):
        from_right = jnp.logical_and(at <= z, has_right)
        from_left = jnp.logical_and(at >= z, has_left)

        @pl.when(from_right)
        def _():
            arrive(right_in.at[at, part], right_recv.at[at, part])

        @pl.when(from_left)
        def _():
            arrive(left_in.at[at, part], left_recv.at[at, part])

        return jnp.where(from_right, right_in[at, part].astype(f32), 0.0) + jnp.where(
            from_left, left_in[at, part].astype(f32), 0.0
        )

    def back_lines(k):
        at = back_order[k]
        for part in (2, 1, 0):
            routed[part] = spread_back(at, part) + arrived(at, part)
            line_out[at, part] = routed[part].astype(bf16)
            source = line_out.at[at, part]
            begin(
                remote(
                    source,
                    right_in.at[at, part],
                    back_line_send.at[at, part],
                    right_recv.at[at, part],
                    left,
                ),
                at < z,
            )
            begin(
                remote(
                    source,
                    left_in.at[at, part],
                    back_line_send.at[at, part],
                    left_recv.at[at, part],
                    right,
                ),
                at > z,
            )

    def own_lines(part):
        routed[part] = spread_back(z, part) + arrived(z, part)

    def shared_first():
        for number in range(4):
            arrive(core_rows.at[number], core_recv.at[number])
        blocks = [
            (own_rows[1], tp * 2),
            (own_rows[0], tp * 2 + 1),
            (line_rows[z, 2], tp_y * 2),
            (partner_high[...], tp_y * 2 + 1),
            (core_rows[0], tp_core * 2),
            (core_rows[1], tp_core * 2 + 1),
            (core_rows[2], other_held[2]),
            (core_rows[3], other_late),
        ]
        squares = gate = up = 0.0
        for rows, number in blocks:
            wide = rows.astype(f32)
            squares = squares + wide * wide
            span = pl.ds(pl.multiple_of(number * half, half), half)
            scaled = rows * gain_ref[:, span]
            gate = gate + jnp.dot(scaled, shared_gate_ref[span, :], preferred_element_type=f32)
            up = up + jnp.dot(scaled, shared_up_ref[span, :], preferred_element_type=f32)
        inverse = lax.rsqrt(jnp.sum(squares, axis=1, keepdims=True) / width + EPSILON)
        shared_hidden[tp] = (swish(gate * inverse) * (up * inverse)).astype(bf16)
        for step in range(1, tp_count):
            peer = lax.rem(tp + step, tp_count)
            begin(
                remote(
                    shared_hidden.at[tp],
                    shared_hidden.at[tp],
                    shared_send.at[step],
                    shared_recv.at[tp],
                    (sp, peer),
                )
            )

    def shared_second():
        for step in range(1, tp_count):
            peer = lax.rem(tp + step, tp_count)
            arrive(shared_hidden.at[peer], shared_recv.at[peer])
        joined = jnp.concatenate([shared_hidden[number] for number in range(tp_count)], axis=1)
        base[...] = mid_ref[...].astype(f32) + jnp.dot(
            joined, shared_down_ref[...], preferred_element_type=f32
        )

    lines(0)
    for k in range(1, depth):
        prepare(order[k], False)
    for load in loads:
        load.wait()
    sides(0)
    shared_first()
    lines(1)
    lates(0, 1)
    experts(0)
    sides(1)
    lines(2)
    lates(1, 0)
    lates(1, 1)
    experts(1)
    pairs(0)
    sides(2)
    lines(3)
    lates(2, 0)
    lates(2, 1)
    experts(2)
    pairs(1)
    ready(0)
    sides(3)
    lates(3, 0)
    lates(3, 1)
    experts(3)
    pairs(2)
    ready(1)
    pairs(3)
    ready(2)
    back_lines(0)
    ready(3)
    back_lines(1)
    back_lines(2)
    shared_second()
    own_lines(2)
    last_out[...] = routed[2].astype(bf16)
    begin(remote(last_out, last_in, last_send, last_recv, over_y))
    own_lines(1)
    own_lines(0)
    out_ref[:, half:] = (base[:, half:] + routed[0]).astype(bf16)
    arrive(last_in, last_recv)
    out_ref[:, :half] = (base[:, :half] + routed[1] + last_in[...].astype(f32)).astype(bf16)
    for copy, when in pending:
        if when is None:
            copy.wait_send()
        else:
            pl.when(when)(copy.wait_send)


def exchange_experts(
    mid_local,
    feedforward_gain,
    routing,
    router_score,
    expert_gate_weight,
    expert_up_weight,
    expert_down_weight,
    shared_expert_gate,
    shared_expert_up,
    shared_expert_down,
):
    sp_count, tp_count = lax.axis_size("sp"), lax.axis_size("tp")
    depth = sp_count // 2
    tokens, slab = mid_local.shape
    half = slab // 2
    parts = 2 * tp_count
    picked = routing.shape[1]
    most = 3 * tokens * picked // (2 * sp_count)
    gain = feedforward_gain.reshape(1, parts * half)
    bf16, f32 = jnp.bfloat16, jnp.float32
    vmem = pltpu.VMEM
    dma = pltpu.SemaphoreType.DMA
    hidden_width = expert_gate_weight.shape[1]
    in_vmem = pl.BlockSpec(memory_space=pltpu.VMEM)
    in_any = pl.BlockSpec(memory_space=pl.ANY)
    weights = (
        expert_gate_weight,
        expert_up_weight,
        expert_down_weight,
        shared_expert_gate,
        shared_expert_up,
        shared_expert_down,
    )
    return pl.pallas_call(
        functools.partial(exchange_kernel, most),
        name="exchange_experts",
        out_shape=jax.ShapeDtypeStruct(mid_local.shape, bf16),
        in_specs=[in_vmem] * 4 + [in_any] * len(weights),
        out_specs=in_vmem,
        scratch_shapes=[vmem(weight.shape, bf16) for weight in weights]
        + [
            vmem((sp_count, tokens), f32),
            vmem((sp_count, sp_count, tokens), f32),
            vmem((sp_count, sp_count, tokens), f32),
            vmem((sp_count, most, 128), f32),
            vmem((depth, 2 * most, tokens), bf16),
            vmem((2, tokens, half), bf16),
            vmem((tokens, half), bf16),
            vmem((4, tokens, half), bf16),
            vmem((depth, EXPERT_PARTS, tokens, half), bf16),
            vmem((depth, EXPERT_PARTS, most, half), bf16),
            vmem((parts, sp_count, most, half), bf16),
            vmem((sp_count, most, hidden_width), bf16),
            vmem((sp_count, 2, most, slab), bf16),
            vmem((sp_count, 2, most, slab), bf16),
            vmem((sp_count, most, half), f32),
            vmem((sp_count, most, half), bf16),
            vmem((sp_count, most, half), bf16),
            vmem((sp_count, EXPERT_PARTS, most, half), bf16),
            vmem((depth, EXPERT_PARTS, most, half), bf16),
            vmem((depth, EXPERT_PARTS, tokens, half), bf16),
            vmem((depth, EXPERT_PARTS, tokens, half), bf16),
            vmem((depth, EXPERT_PARTS, tokens, half), bf16),
            vmem((tokens, half), bf16),
            vmem((tokens, half), bf16),
            vmem((tp_count, tokens, shared_expert_gate.shape[1]), bf16),
            vmem((EXPERT_PARTS, tokens, half), f32),
            vmem((tokens, slab), f32),
            dma((len(weights) + 1,)),
            dma((sp_count,)),
            dma((sp_count,)),
            dma((2,)),
            dma((2,)),
            dma((4,)),
            dma((4,)),
            dma((depth, EXPERT_PARTS)),
            dma((depth, EXPERT_PARTS)),
            dma((depth, EXPERT_PARTS)),
            dma((depth, EXPERT_PARTS)),
            dma((depth, EXPERT_PARTS)),
            dma((sp_count,)),
            dma((sp_count,)),
            dma((parts, sp_count)),
            dma((parts, sp_count)),
            dma((sp_count,)),
            dma((sp_count,)),
            dma((sp_count,)),
            dma((sp_count,)),
            dma((depth, EXPERT_PARTS)),
            dma((depth, EXPERT_PARTS)),
            dma((depth, EXPERT_PARTS)),
            dma((depth, EXPERT_PARTS)),
            dma((depth, EXPERT_PARTS)),
            dma((tp_count,)),
            dma((tp_count,)),
            dma,
            dma,
        ],
        compiler_params=pltpu.CompilerParams(
            collective_id=1, has_side_effects=True, vmem_limit_bytes=60 * 1024 * 1024
        ),
    )(mid_local, gain, routing.T, router_score.T, *weights)


def attend_kernel(
    extra_ref,
    norm_gain_ref,
    decay_hbm,
    key_hbm,
    value_hbm,
    query_hbm,
    gate_hbm,
    residual_hbm,
    projection_hbm,
    out_ref,
    decay_ref,
    key_ref,
    value_ref,
    query_ref,
    gate_ref,
    residual_ref,
    projection_ref,
    inside,
    query_start,
    decays,
    decays_in,
    state_out,
    state_in,
    carry_out,
    carry_in,
    local_mixed,
    head_rows,
    total,
    load_sem,
    decay_sems,
    state_send,
    state_recv,
    carry_send,
    carry_recv,
    y_send,
    y_recv,
    core_send,
    core_recv,
    pass_send,
    pass_recv,
):
    bf16, f32 = jnp.bfloat16, jnp.float32
    sp_count, tp_count = lax.axis_size("sp"), lax.axis_size("tp")
    depth = sp_count // 2
    head_count, tokens = extra_ref.shape
    blocks = tokens // BLOCK_POSITIONS
    sp, tp = lax.axis_index("sp"), lax.axis_index("tp")
    z, x = sp // 2, sp % 2
    y, core = tp // 2, tp % 2
    tp_y = (1 - y) * 2 + core
    tp_core = y * 2 + (1 - core)
    tp_far = (1 - y) * 2 + (1 - core)
    side, right = (z * 2 + 1 - x, tp), (sp + 2, tp)
    over_y, over_core = (sp, tp_y), (sp, tp_core)
    has_left, has_right = z > 0, z < depth - 1
    pending = []

    def begin(copy, when=None):
        if when is None:
            copy.start()
        else:
            pl.when(when)(copy.start)
        pending.append((copy, when))

    def arrive(target, sem):
        remote(target, target, decay_sems.at[0], sem, (sp, tp)).wait_recv()

    arrays = [
        (decay_hbm, decay_ref),
        (key_hbm, key_ref),
        (value_hbm, value_ref),
        (query_hbm, query_ref),
        (gate_hbm, gate_ref),
        (residual_hbm, residual_ref),
        (projection_hbm, projection_ref),
    ]
    loads = [
        pltpu.make_async_copy(hbm, ref, load_sem.at[number])
        for number, (hbm, ref) in enumerate(arrays)
    ]
    for load in loads:
        load.start()
    barrier = pltpu.get_barrier_semaphore()
    for peer in (side, over_y, over_core):
        pl.semaphore_signal(barrier, inc=1, device_id=peer, device_id_type=pl.DeviceIdType.MESH)
    for peer, exists in (((sp - 2, tp), has_left), (right, has_right)):
        @pl.when(exists)
        def _():
            pl.semaphore_signal(
                barrier, inc=1, device_id=peer, device_id_type=pl.DeviceIdType.MESH
            )

    row = lax.broadcasted_iota(jnp.int32, (tokens, tokens), 0)
    column = lax.broadcasted_iota(jnp.int32, (tokens, tokens), 1)
    causal = jnp.logical_and(
        column <= row, row // BLOCK_POSITIONS == column // BLOCK_POSITIONS
    )
    triangle = jnp.where(causal, 1.0, 0.0).astype(f32)
    over_first, over_rows = (((0,), (0,)), ((), ())), (((1,), (1,)), ((), ()))
    owner = (
        lax.broadcasted_iota(jnp.int32, (head_count, head_count * DK), 1) // DK
        == lax.broadcasted_iota(jnp.int32, (head_count, head_count * DK), 0)
    )
    extra = lax.dot_general(
        extra_ref[...],
        jnp.where(owner, 1.0, 0.0),
        over_first,
        precision=HIGHEST,
        preferred_element_type=f32,
    )
    loads[0].wait()
    preactivation = decay_ref[...].astype(f32)
    logs = jnp.minimum(preactivation, 0.0) - jnp.log1p(jnp.exp(-jnp.abs(preactivation)))
    logs = logs / GATE_TEMPER + extra
    inside[...] = jnp.dot(triangle, logs, precision=HIGHEST, preferred_element_type=f32)
    ends = [
        inside[(block + 1) * BLOCK_POSITIONS - 1 : (block + 1) * BLOCK_POSITIONS, :]
        for block in range(blocks)
    ]
    before = [jnp.zeros_like(ends[0])]
    for end in ends:
        before.append(before[-1] + end)
    decays[...] = jnp.broadcast_to(jnp.exp(before[blocks]), decays.shape)

    def span(block):
        return slice(block * BLOCK_POSITIONS, (block + 1) * BLOCK_POSITIONS)

    def columns(head, width):
        return slice(head * width, (head + 1) * width)

    loads[1].wait()
    loads[2].wait()
    pl.semaphore_wait(
        barrier, 3 + jnp.where(has_left, 1, 0) + jnp.where(has_right, 1, 0)
    )
    begin(remote(decays, decays_in, decay_sems.at[1], decay_sems.at[2], side))
    for head in range(head_count):
        wide = columns(head, DK)
        tail = jnp.concatenate(
            [
                before[blocks][:, wide] - before[block][:, wide] - inside[span(block), wide]
                for block in range(blocks)
            ],
            axis=0,
        )
        faded = (key_ref[:, wide].astype(f32) * jnp.exp(tail)).astype(bf16)
        state_out[head] = lax.dot_general(
            value_ref[:, columns(head, DV)], faded, over_first, preferred_element_type=f32
        ).astype(bf16)
        begin(
            remote(
                state_out.at[head],
                state_in.at[head],
                state_send.at[head],
                state_recv.at[head],
                side,
            )
        )

    def local(head):
        wide = columns(head, DK)
        values = value_ref[:, columns(head, DV)]
        keys = key_ref[:, wide].astype(f32)
        logs_inside = inside[:, wide]
        queries = query_ref[:, wide].astype(f32) * (DK**-0.5) * jnp.exp(logs_inside)
        query_decay = queries.astype(bf16)
        key_decay = (keys * jnp.exp(-logs_inside)).astype(bf16)
        scores = lax.dot_general(
            query_decay, key_decay, over_rows, preferred_element_type=f32
        )
        scores = jnp.where(causal, scores, 0.0).astype(bf16)
        mixed = jnp.dot(scores, values, preferred_element_type=f32)
        state, pieces, starts = None, [mixed[span(0)]], []
        for block in range(blocks):
            starts.append(queries[span(block)] * jnp.exp(before[block][:, wide]))
            if block == blocks - 1:
                break
            end = ends[block][:, wide]
            key_end = (keys[span(block)] * jnp.exp(end - logs_inside[span(block)])).astype(bf16)
            fresh = lax.dot_general(
                values[span(block)], key_end, over_first, preferred_element_type=f32
            )
            state = fresh if state is None else state * jnp.exp(end) + fresh
            passed = lax.dot_general(
                query_decay[span(block + 1)],
                state.astype(bf16),
                over_rows,
                preferred_element_type=f32,
            )
            pieces.append(mixed[span(block + 1)] + passed)
        local_mixed[head] = jnp.concatenate(pieces, axis=0)
        query_start[head] = jnp.concatenate(starts, axis=0).astype(bf16)

    def chain(head):
        wide = columns(head, DK)
        arrive(state_in.at[head], state_recv.at[head])
        own, other = state_out[head].astype(f32), state_in[head].astype(f32)
        decay_own, decay_other = decays[0:1, wide], decays_in[0:1, wide]
        first = jnp.where(x == 0, own, other)
        second = jnp.where(x == 0, other, own)
        decay_second = jnp.where(x == 0, decay_other, decay_own)

        @pl.when(has_left)
        def _():
            arrive(carry_in.at[head], carry_recv.at[head])

        entering = jnp.where(has_left, carry_in[head].astype(f32), 0.0)
        carry_out[head] = (
            decay_own * decay_other * entering + decay_second * first + second
        ).astype(bf16)
        begin(
            remote(
                carry_out.at[head],
                carry_in.at[head],
                carry_send.at[head],
                carry_recv.at[head],
                right,
            ),
            has_right,
        )
        return jnp.where(x == 0, entering, decay_other * entering + other).astype(bf16)

    def finish(head, entering):
        mixed = local_mixed[head] + lax.dot_general(
            query_start[head], entering, over_rows, preferred_element_type=f32
        )
        inverse = lax.rsqrt(jnp.mean(mixed * mixed, axis=1, keepdims=True) + EPSILON)
        opened = swish(gate_ref[:, columns(head, DV)].astype(f32))
        head_rows[tp, head] = (
            mixed * inverse * norm_gain_ref[...].astype(f32) * opened
        ).astype(bf16)
        source = head_rows.at[tp, head]
        begin(remote(source, source, y_send.at[head], y_recv.at[head], over_y))
        begin(remote(source, source, core_send.at[head], core_recv.at[head], over_core))

    def project(owner, head):
        start = (owner * head_count + head) * DV
        return jnp.dot(
            head_rows[owner, head],
            projection_ref[pl.ds(pl.multiple_of(start, DV), DV), :],
            preferred_element_type=f32,
        )

    def relay(head):
        target = head_rows.at[tp_y, head]
        arrive(target, y_recv.at[head])
        begin(remote(target, target, pass_send.at[head], pass_recv.at[head], over_core))

    loads[3].wait()
    for head in range(head_count):
        local(head)
    loads[4].wait()
    arrive(decays_in, decay_sems.at[2])
    for head in range(head_count):
        entering = chain(head)
        finish(head, entering)
        if head >= 2:
            relay(head - 2)
    loads[5].wait()
    loads[6].wait()
    total[...] = residual_ref[...].astype(f32) + sum(
        project(tp, head) for head in range(head_count)
    )
    for head in range(head_count):
        arrive(head_rows.at[tp_core, head], core_recv.at[head])
    total[...] = total[...] + sum(project(tp_core, head) for head in range(head_count))
    for head in range(head_count):
        if head >= 2:
            relay(head)
    for head in range(head_count):
        total[...] = total[...] + project(tp_y, head)
        arrive(head_rows.at[tp_far, head], pass_recv.at[head])
        total[...] = total[...] + project(tp_far, head)
    out_ref[...] = total[...].astype(bf16)
    for copy, when in pending:
        if when is None:
            copy.wait_send()
        else:
            pl.when(when)(copy.wait_send)


def attend_project(
    queries,
    key_matrix,
    value_matrix,
    output_gate_preactivation,
    decay_preactivation,
    extra_log_decay,
    head_norm_gain,
    residual,
    output_projection,
):
    bf16, f32 = jnp.bfloat16, jnp.float32
    arrays = (
        decay_preactivation,
        key_matrix,
        value_matrix,
        queries,
        output_gate_preactivation,
        residual,
        output_projection,
    )
    tokens, head_count = extra_log_decay.shape
    tp_count = lax.axis_size("tp")
    vmem, dma = pltpu.VMEM, pltpu.SemaphoreType.DMA
    in_vmem = pl.BlockSpec(memory_space=pltpu.VMEM)
    in_any = pl.BlockSpec(memory_space=pl.ANY)
    return pl.pallas_call(
        attend_kernel,
        name="attend_project",
        out_shape=jax.ShapeDtypeStruct(residual.shape, bf16),
        in_specs=[in_vmem] * 2 + [in_any] * len(arrays),
        out_specs=in_vmem,
        scratch_shapes=[vmem(array.shape, bf16) for array in arrays]
        + [
            vmem((tokens, head_count * DK), f32),
            vmem((head_count, tokens, DK), bf16),
            vmem((8, head_count * DK), f32),
            vmem((8, head_count * DK), f32),
            vmem((head_count, DV, DK), bf16),
            vmem((head_count, DV, DK), bf16),
            vmem((head_count, DV, DK), bf16),
            vmem((head_count, DV, DK), bf16),
            vmem((head_count, tokens, DV), f32),
            vmem((tp_count, head_count, tokens, DV), bf16),
            vmem(residual.shape, f32),
            dma((len(arrays),)),
            dma((3,)),
            dma((head_count,)),
            dma((head_count,)),
            dma((head_count,)),
            dma((head_count,)),
            dma((head_count,)),
            dma((head_count,)),
            dma((head_count,)),
            dma((head_count,)),
            dma((head_count,)),
            dma((head_count,)),
        ],
        compiler_params=pltpu.CompilerParams(
            collective_id=2, has_side_effects=True, vmem_limit_bytes=62 * 1024 * 1024
        ),
    )(extra_log_decay.T, head_norm_gain.reshape(1, DV), *arrays)


def attention_heads(queries, key_matrix, value_matrix, decay_preactivation, extra_log_decay):
    tokens = queries.shape[0]
    local_head_count = extra_log_decay.shape[1]
    block_count = tokens // BLOCK_POSITIONS
    query_block = queries.astype(jnp.float32).reshape(
        block_count, BLOCK_POSITIONS, local_head_count, DK
    ) * DK ** (-0.5)
    key_block = key_matrix.astype(jnp.float32).reshape(
        block_count, BLOCK_POSITIONS, local_head_count, DK
    )
    value_block = value_matrix.astype(jnp.float32).reshape(
        block_count, BLOCK_POSITIONS, local_head_count, DV
    )
    log_decay_rows = (
        jax.nn.log_sigmoid(decay_preactivation.astype(jnp.float32)).reshape(
            block_count, BLOCK_POSITIONS, local_head_count, DK
        )
        / GATE_TEMPER
    )
    log_decay_rows = (
        log_decay_rows
        + extra_log_decay.reshape(block_count, BLOCK_POSITIONS, local_head_count)[..., None]
    )
    inside = jnp.cumsum(log_decay_rows, axis=1)
    block_total = inside[:, -1]
    query_decay = query_block * jnp.exp(inside)
    key_decay = key_block * jnp.exp(-inside)
    causal = jnp.tril(jnp.ones((BLOCK_POSITIONS, BLOCK_POSITIONS), dtype=bool))
    scores = jnp.where(
        causal, jnp.einsum("nthd,nshd->nhts", query_decay, key_decay, precision=HIGHEST), 0.0
    )
    within = jnp.einsum("nhts,nshv->nthv", scores, value_block, precision=HIGHEST)
    key_end = key_block * jnp.exp(block_total[:, None] - inside)
    update = jnp.einsum("nshd,nshv->nhdv", key_end, value_block, precision=HIGHEST)
    before = jnp.cumsum(block_total, axis=0) - block_total
    ending = jnp.concatenate([before, (before[-1] + block_total[-1])[None]], axis=0)
    after_block = before + block_total
    earlier_mask = jnp.arange(block_count + 1)[:, None] > jnp.arange(block_count)[None, :]
    span_logs = jnp.where(
        earlier_mask[:, :, None, None], ending[:, None] - after_block[None], -1e30
    )
    states = jnp.einsum("nmhd,mhdv->nhdv", jnp.exp(span_logs), update, precision=HIGHEST)
    passed = jnp.einsum("nthd,nhdv->nthv", query_decay, states[:block_count], precision=HIGHEST)
    query_start = query_block * jnp.exp(inside + before[:, None])
    return (within + passed, query_start, jnp.exp(ending[block_count]), states[block_count])


def body(
    queries,
    key_matrix,
    value_matrix,
    output_gate_preactivation,
    decay_preactivation,
    extra_log_decay,
    head_norm_gain,
    output_projection,
    residual,
    feedforward_gain,
    routing,
    router_score,
    expert_gate_weight,
    expert_up_weight,
    expert_down_weight,
    shared_expert_gate,
    shared_expert_up,
    shared_expert_down,
):
    tokens = queries.shape[0]
    local_head_count = extra_log_decay.shape[1]
    if lax.axis_size("tp") == FF_PARTS and lax.axis_size("sp") == 8:
        mid_local = attend_project(
            queries,
            key_matrix,
            value_matrix,
            output_gate_preactivation,
            decay_preactivation,
            extra_log_decay,
            head_norm_gain,
            residual,
            output_projection,
        )
        return exchange_experts(
            mid_local,
            feedforward_gain,
            routing,
            router_score,
            expert_gate_weight,
            expert_up_weight,
            expert_down_weight,
            shared_expert_gate,
            shared_expert_up,
            shared_expert_down,
        )
    local_part, query_start, dev_decay, dev_update = attention_heads(
        queries, key_matrix, value_matrix, decay_preactivation, extra_log_decay
    )
    _, entering = prefix(
        (dev_decay, dev_update),
        "sp",
        carry_combine,
        (jnp.ones_like(dev_decay), jnp.zeros_like(dev_update)),
    )
    attention_output = local_part + jnp.einsum(
        "nthd,hdv->nthv", query_start, entering, precision=HIGHEST
    )
    attention_output = attention_output.reshape(tokens, local_head_count, DV)
    inverse_rms = lax.rsqrt(
        jnp.mean(attention_output * attention_output, axis=-1, keepdims=True) + EPSILON
    )
    gate_act = jax.nn.silu(
        output_gate_preactivation.astype(jnp.float32).reshape(tokens, local_head_count, DV)
    )
    head_rows = (
        (attention_output * inverse_rms * head_norm_gain.astype(jnp.float32) * gate_act)
        .reshape(tokens, local_head_count * DV)
        .astype(jnp.bfloat16)
    )
    tp_steps = [("tp", bit) for bit in range(lax.axis_size("tp").bit_length() - 1)][::-1]
    projected = jnp.dot(
        spread(head_rows, tp_steps),
        relative_rows(output_projection, lax.axis_index("tp"), masks_of(tp_steps, "tp")),
        preferred_element_type=jnp.float32,
    )
    mid_local = (residual.astype(jnp.float32) + projected).astype(jnp.bfloat16)
    mid_rows = lax.all_gather(mid_local, "tp", axis=1, tiled=True).astype(jnp.float32)
    normed = (
        mid_rows
        * lax.rsqrt(jnp.mean(mid_rows * mid_rows, axis=-1, keepdims=True) + EPSILON)
        * feedforward_gain.astype(jnp.float32)
    ).astype(jnp.bfloat16)
    shared_pre = jnp.dot(normed, shared_expert_gate, preferred_element_type=jnp.float32)
    shared_lin = jnp.dot(normed, shared_expert_up, preferred_element_type=jnp.float32)
    shared_hidden = (jax.nn.silu(shared_pre) * shared_lin).astype(jnp.bfloat16)
    senders = lax.axis_size("sp")
    tp_count = lax.axis_size("tp")
    tp_bits = tp_count.bit_length() - 1
    tp_index = lax.axis_index("tp")
    groups = tp_count // FF_PARTS
    group_here = tp_index // FF_PARTS
    part_here = tp_index % FF_PARTS
    model_width = normed.shape[1]
    picks = routing.shape[1]
    expert_total = senders * groups
    rows_most = max(2, 3 * tokens * picks // (2 * expert_total))
    slot_count = senders * rows_most
    flat_expert = routing.reshape(-1)
    one_hot = (flat_expert[:, None] == jnp.arange(expert_total, dtype=jnp.int32)[None, :]).astype(
        jnp.int32
    )
    rank_before = jnp.sum((jnp.cumsum(one_hot, axis=0) - one_hot) * one_hot, axis=1)
    owned = flat_expert % groups == group_here
    slot_index = jnp.where(owned, flat_expert // groups * rows_most + rank_before, slot_count)
    token_index = jnp.arange(flat_expert.shape[0], dtype=jnp.int32) // picks
    part_width = model_width // FF_PARTS
    normed_part = lax.dynamic_slice_in_dim(normed, part_here * part_width, part_width, 1)
    outgoing = (
        jnp.zeros((slot_count, part_width), jnp.bfloat16)
        .at[slot_index]
        .set(normed_part[token_index], mode="drop")
    )
    arrived = lax.all_to_all(
        outgoing.reshape(senders, rows_most, part_width),
        "sp",
        split_axis=0,
        concat_axis=0,
        tiled=True,
    )
    for bit in range(2):
        partner_cols = from_partner(arrived, "tp", bit)
        upper = (tp_index >> bit) % 2
        arrived = jnp.where(
            upper == 1,
            jnp.concatenate([partner_cols, arrived], axis=2),
            jnp.concatenate([arrived, partner_cols], axis=2),
        )
    rows_in = arrived.reshape(slot_count, model_width)
    gate_pre = jnp.dot(rows_in, expert_gate_weight, preferred_element_type=jnp.float32)
    up_pre = jnp.dot(rows_in, expert_up_weight, preferred_element_type=jnp.float32)
    routed_hidden = (jax.nn.silu(gate_pre) * up_pre).astype(jnp.bfloat16)
    partial_out = jnp.dot(routed_hidden, expert_down_weight, preferred_element_type=jnp.float32)
    slab_width = model_width // tp_count
    partial_out = partial_out.reshape(slot_count, groups, FF_PARTS, slab_width)
    for bit in (1, 0):
        paired = partial_out.reshape(slot_count, groups, 2, 2**bit, slab_width)
        upper = (tp_index >> bit) % 2
        kept = lax.dynamic_index_in_dim(paired, upper, 2, keepdims=False)
        given = lax.dynamic_index_in_dim(paired, 1 - upper, 2, keepdims=False)
        partial_out = kept + from_partner(given.astype(jnp.bfloat16), "tp", bit).astype(given.dtype)
    expert_out = partial_out.reshape(senders, rows_most, groups, slab_width).astype(jnp.bfloat16)
    shared_out = jnp.dot(
        lax.all_gather(shared_hidden, "tp", axis=1, tiled=True),
        shared_expert_down,
        preferred_element_type=jnp.float32,
    )
    returned = lax.all_to_all(expert_out, "sp", split_axis=0, concat_axis=0, tiled=True).reshape(
        slot_count, groups, slab_width
    )
    safe_slot = jnp.minimum(slot_index, slot_count - 1)
    route_weight = ROUTE_SCALE * router_score / jnp.sum(router_score, axis=1, keepdims=True)
    pair_weight = jnp.where(owned, route_weight.reshape(-1), 0.0)
    picked = returned[safe_slot].astype(jnp.float32) * pair_weight[:, None, None]
    routed_part = jnp.sum(picked.reshape(tokens, picks, groups, slab_width), axis=1)
    for bit in range(tp_bits - 1, 1, -1):
        paired = routed_part.reshape(tokens, 2, 2 ** (bit - 2), slab_width)
        upper = (tp_index >> bit) % 2
        kept = lax.dynamic_index_in_dim(paired, upper, 1, keepdims=False)
        given = lax.dynamic_index_in_dim(paired, 1 - upper, 1, keepdims=False)
        routed_part = kept + from_partner(as_sent(given), "tp", bit).astype(given.dtype)
    routed = routed_part.reshape(tokens, slab_width)
    return (mid_local.astype(jnp.float32) + routed + shared_out).astype(jnp.bfloat16)


def solution(mesh):
    return jax.shard_map(
        body,
        mesh=mesh,
        in_specs=(
            P("sp", "tp"),
            P("sp", "tp"),
            P("sp", "tp"),
            P("sp", "tp"),
            P("sp", "tp"),
            P("sp", "tp"),
            P(),
            P(None, "tp"),
            P("sp", "tp"),
            P(),
            P("sp", None),
            P("sp", None),
            P(None, ("sp", "tp")),
            P(None, ("sp", "tp")),
            P(("sp", "tp"), None),
            P(None, "tp"),
            P(None, "tp"),
            P(None, "tp"),
        ),
        out_specs=P("sp", "tp"),
        check_vma=False,
    )
```

```python
import functools

import jax
import jax.numpy as jnp
from jax import lax
from jax.experimental import pallas as pl
from jax.experimental.pallas import tpu as pltpu
from jax.sharding import PartitionSpec as P

DK = 128
DV = 256
BLOCK_POSITIONS = 64
FF_PARTS = 4

HIGHEST = lax.Precision.HIGHEST
EPSILON = 1e-06
ROUTE_SCALE = 2.5
GATE_TEMPER = 16.0


def from_partner(value, axis, bit, upward=False):
    mask = 2**bit
    pairs = [(source, source ^ mask) for source in range(lax.axis_size(axis))]
    if upward:
        pairs = [(source, target) for source, target in pairs if source < target]
    return lax.ppermute(value, axis, pairs)


def as_sent(value):
    return jax.tree.map(lambda a: a.astype(jnp.bfloat16) if a.dtype == jnp.float32 else a, value)


def carry_combine(first_part, second_part):
    return (
        first_part[0] * second_part[0],
        second_part[0][..., None] * first_part[1] + second_part[1],
    )


def choose(flag, yes, no):
    return jax.tree.map(lambda a, b: jnp.where(flag, a, b), yes, no)


def prefix(value, axis, join, neutral):
    place = lax.axis_index(axis)
    bits = lax.axis_size(axis).bit_length() - 1
    total, state = value, neutral
    for bit in range(bits):
        upper = (place >> bit) % 2 == 1
        last = bit == bits - 1
        arrived = jax.tree.map(
            lambda a: from_partner(a.astype(jnp.bfloat16), axis, bit, last).astype(a.dtype), total
        )
        state = choose(upper, join(arrived, state), state)
        if not last:
            total = choose(upper, join(arrived, total), join(total, arrived))
    return state


def relative_rows(matrix, place, masks):
    height = matrix.shape[0] // len(masks)
    return jnp.concatenate(
        [lax.dynamic_slice_in_dim(matrix, (place ^ mask) * height, height, 0) for mask in masks], 0
    )


def relative_columns(matrix, place, masks):
    width = matrix.shape[1] // len(masks)
    return jnp.concatenate(
        [lax.dynamic_slice_in_dim(matrix, (place ^ mask) * width, width, 1) for mask in masks], 1
    )


def masks_of(steps, axis):
    masks = [0]
    for step_axis, bit in steps:
        if step_axis == axis:
            masks = masks + [mask ^ (2**bit) for mask in masks]
    return masks


def spread(value, steps):
    for axis, bit in steps:
        arrived = from_partner(value, axis, bit)
        value = jnp.concatenate([value, arrived], 0 if axis == "sp" else 1)
    return value


def collect(value, steps):
    for axis, bit in reversed(steps):
        own, given = jnp.split(value, 2, 0 if axis == "sp" else 1)
        value = (
            own.astype(jnp.float32) + from_partner(given, axis, bit).astype(jnp.float32)
        ).astype(jnp.bfloat16)
    return value


EXPERT_PARTS = 3


def remote(source, target, send_sem, recv_sem, device):
    return pltpu.make_async_remote_copy(
        src_ref=source,
        dst_ref=target,
        send_sem=send_sem,
        recv_sem=recv_sem,
        device_id=device,
        device_id_type=pl.DeviceIdType.MESH,
    )


def swish(value):
    return value / (1.0 + jnp.exp(-value))


def exchange_kernel(
    most,
    mid_ref,
    gain_ref,
    routing_ref,
    score_ref,
    gate_hbm,
    up_hbm,
    down_hbm,
    shared_gate_hbm,
    shared_up_hbm,
    shared_down_hbm,
    out_ref,
    gate_ref,
    up_ref,
    down_ref,
    shared_gate_ref,
    shared_up_ref,
    shared_down_ref,
    table_ref,
    tables,
    ranks,
    slot_weights,
    picks,
    turned,
    own_rows,
    partner_high,
    core_rows,
    line_rows,
    side_out,
    expert_rows,
    hidden_rows,
    core_out,
    core_in,
    kept_rows,
    y_out,
    y_in,
    results,
    side_in,
    line_out,
    left_in,
    right_in,
    last_out,
    last_in,
    shared_hidden,
    routed,
    base,
    weight_sem,
    table_send,
    table_recv,
    own_send,
    own_recv,
    core_send,
    core_recv,
    left_send,
    right_send,
    line_recv,
    side_send,
    side_recv,
    y_send,
    y_recv,
    pair_send,
    pair_recv,
    back_core_send,
    back_core_recv,
    back_y_send,
    back_y_recv,
    back_side_send,
    back_side_recv,
    back_line_send,
    left_recv,
    right_recv,
    shared_send,
    shared_recv,
    last_send,
    last_recv,
):
    bf16, f32 = jnp.bfloat16, jnp.float32
    sp_count, tp_count = lax.axis_size("sp"), lax.axis_size("tp")
    depth = sp_count // 2
    tokens = mid_ref.shape[0]
    half = mid_ref.shape[1] // 2
    parts = 2 * tp_count
    width = half * parts
    sp, tp = lax.axis_index("sp"), lax.axis_index("tp")
    z, x = sp // 2, sp % 2
    y, core = tp // 2, tp % 2
    tp_y = (1 - y) * 2 + core
    tp_core = y * 2 + (1 - core)
    side = (z * 2 + 1 - x, tp)
    over_y = (sp, tp_y)
    over_core = (sp, tp_core)
    left, right = (sp - 2, tp), (sp + 2, tp)
    has_left, has_right = z > 0, z < depth - 1
    pending = []

    def begin(copy, when=None):
        if when is None:
            copy.start()
        else:
            pl.when(when)(copy.start)
        pending.append((copy, when))

    def arrive(target, sem):
        remote(target, target, weight_sem.at[0], sem, (sp, tp)).wait_recv()

    order = [
        z,
        jnp.where(z == 0, 1, jnp.where(z == 1, 0, jnp.where(z == 2, 3, 2))),
        jnp.where(z == 0, 2, jnp.where(z == 1, 2, jnp.where(z == 2, 1, 1))),
        jnp.where(z == 0, 3, jnp.where(z == 1, 3, 0)),
    ]
    back_order = [
        jnp.where(z == 0, 1, jnp.where(z == 1, 2, jnp.where(z == 2, 1, 2))),
        jnp.where(z == 0, 2, jnp.where(z == 1, 3, jnp.where(z == 2, 0, 1))),
        jnp.where(z == 0, 3, jnp.where(z == 1, 0, jnp.where(z == 2, 3, 0))),
        z,
    ]

    barrier = pltpu.get_barrier_semaphore()
    peers = [(lax.rem(sp + step, sp_count), tp) for step in range(1, sp_count)]
    peers += [(sp, lax.rem(tp + step, tp_count)) for step in range(1, tp_count)]
    for peer in peers:
        pl.semaphore_signal(barrier, inc=1, device_id=peer, device_id_type=pl.DeviceIdType.MESH)
    weights = [
        (gate_hbm, gate_ref),
        (up_hbm, up_ref),
        (down_hbm, down_ref),
        (shared_gate_hbm, shared_gate_ref),
        (shared_up_hbm, shared_up_ref),
        (shared_down_hbm, shared_down_ref),
    ]
    loads = [
        pltpu.make_async_copy(hbm, vmem, weight_sem.at[number + 1])
        for number, (hbm, vmem) in enumerate(weights)
    ]
    for load in loads:
        load.start()
    score = score_ref[...]
    route_weight = ROUTE_SCALE * score / jnp.sum(score, axis=0, keepdims=True)
    experts_here = lax.broadcasted_iota(jnp.int32, table_ref.shape, 0)
    table = jnp.zeros(table_ref.shape, f32)
    for pick_at in range(score.shape[0]):
        table = table + jnp.where(
            routing_ref[pick_at : pick_at + 1, :] == experts_here,
            route_weight[pick_at : pick_at + 1, :],
            0.0,
        )
    table_ref[...] = table
    pl.semaphore_wait(barrier, len(peers))

    low, high = mid_ref.at[:, pl.ds(0, half)], mid_ref.at[:, pl.ds(half, half)]
    for step in range(1, sp_count):
        peer = lax.rem(sp + step, sp_count)
        begin(
            remote(table_ref, tables.at[sp], table_send.at[step], table_recv.at[sp], (peer, tp))
        )
    begin(remote(low, line_rows.at[z, 2], own_send.at[0], own_recv.at[0], over_y))
    for part, source in ((0, high), (1, low)):
        target = line_rows.at[z, part]
        begin(remote(source, target, left_send.at[z, part], line_recv.at[z, part], left), has_left)
        begin(
            remote(source, target, right_send.at[z, part], line_recv.at[z, part], right), has_right
        )
    begin(remote(high, partner_high, own_send.at[1], own_recv.at[1], over_y))
    begin(remote(low, core_rows.at[0], core_send.at[0], core_recv.at[0], over_core))
    begin(remote(high, core_rows.at[1], core_send.at[1], core_recv.at[1], over_core))
    own_rows[0] = mid_ref[:, half:]
    own_rows[1] = mid_ref[:, :half]
    tables[sp] = table_ref[...]

    earlier = (
        lax.broadcasted_iota(jnp.int32, (tokens, tokens), 0)
        < lax.broadcasted_iota(jnp.int32, (tokens, tokens), 1)
    ).astype(f32).astype(bf16)
    slots = lax.broadcasted_iota(jnp.int32, (most, tokens), 0).astype(f32)

    def rank_block(source):
        chosen = tables[source] > 0.0
        counts = jnp.dot(
            jnp.where(chosen, 1.0, 0.0).astype(bf16), earlier, preferred_element_type=f32
        )
        ranks[source] = jnp.where(chosen, counts, -1.0)

    def pick(source, expert):
        return slots == ranks[source, pl.ds(expert, 1), :]

    def slot_block(source):
        weight = jnp.where(pick(source, sp), tables[source, pl.ds(sp, 1), :], 0.0)
        slot_weights[source] = jnp.broadcast_to(
            jnp.sum(weight, axis=1, keepdims=True), (most, 128)
        )

    def pick_block(depth_at):
        source = depth_at * 2 + x
        chosen = jnp.concatenate(
            [
                jnp.where(pick(source, expert), 1.0, 0.0)
                for expert in (sp, z * 2 + 1 - x)
            ],
            axis=0,
        )
        picks[depth_at] = chosen.astype(bf16)

    def turn():
        for depth_at in range(depth):
            turned[depth_at] = picks[depth_at].astype(f32).T.astype(bf16)

    def prepare(depth_at, first):
        for source in (depth_at * 2 + x, depth_at * 2 + 1 - x):
            if first:
                @pl.when(source != sp)
                def _():
                    arrive(tables.at[source], table_recv.at[source])
            else:
                arrive(tables.at[source], table_recv.at[source])
            rank_block(source)
            slot_block(source)
        pick_block(depth_at)

    prepare(order[0], True)
    arrive(line_rows.at[z, 2], own_recv.at[0])
    target = line_rows.at[z, 2]
    begin(remote(target, target, left_send.at[z, 2], line_recv.at[z, 2], left), has_left)
    begin(remote(target, target, right_send.at[z, 2], line_recv.at[z, 2], right), has_right)
    begin(remote(target, core_rows.at[2], core_send.at[2], core_recv.at[2], over_core))

    held = (tp * 2 + 1, tp * 2, tp_y * 2)
    late = tp_y * 2 + 1

    def to_core(number, source):
        ref = expert_rows.at[number, source]
        begin(
            remote(ref, ref, pair_send.at[number, source], pair_recv.at[number, source], over_core)
        )

    def to_y(source):
        ref = expert_rows.at[held[0], source]
        begin(remote(ref, ref, y_send.at[source], y_recv.at[source], over_y))

    def compact(at, part, number, rows):
        source = at * 2 + x
        chosen = jnp.dot(picks[at], rows, preferred_element_type=f32).astype(bf16)
        side_out[at, part] = chosen[most:]
        begin(
            remote(
                side_out.at[at, part],
                expert_rows.at[number, source],
                side_send.at[at, part],
                side_recv.at[at, part],
                side,
            )
        )
        expert_rows[number, source] = chosen[:most]

    def own_block():
        source = sp
        for part in range(EXPERT_PARTS):
            rows = line_rows[z, 2] if part == 2 else own_rows[part]
            compact(z, part, held[part], rows)
            to_core(held[part], source)
        arrive(partner_high, own_recv.at[1])
        begin(remote(partner_high, core_rows.at[3], core_send.at[3], core_recv.at[3], over_core))
        expert_rows[late, source] = jnp.dot(
            picks[z, pl.ds(0, most), :], partner_high[...], preferred_element_type=f32
        ).astype(bf16)
        to_core(late, source)

    inner = jnp.logical_and(has_left, has_right)
    turns = [(1, 0), (2, 0), (1, 1), (2, 1), (1, 2), (2, 2), (3, 0), (3, 1), (3, 2)]

    def line(number):
        (k, part), (plain_k, plain_part) = turns[number], divmod(number, EXPERT_PARTS)
        at = jnp.where(inner, order[k], order[plain_k + 1])
        part = jnp.where(inner, part, plain_part)
        ref = line_rows.at[at, part]
        arrive(ref, line_recv.at[at, part])
        begin(
            remote(ref, ref, left_send.at[at, part], line_recv.at[at, part], left),
            jnp.logical_and(at > z, has_left),
        )
        begin(
            remote(ref, ref, right_send.at[at, part], line_recv.at[at, part], right),
            jnp.logical_and(at < z, has_right),
        )
        part_number = jnp.where(part == 0, held[0], jnp.where(part == 1, held[1], held[2]))
        compact(at, part, part_number, line_rows[at, part])
        source = at * 2 + x
        ref = expert_rows.at[part_number, source]
        begin(
            remote(ref, ref, y_send.at[source], y_recv.at[source], over_y),
            part == 0,
        )
        to_core(part_number, source)

    def sides(k):
        at = order[k]
        source = at * 2 + 1 - x
        for part in range(EXPERT_PARTS):
            arrive(expert_rows.at[held[part], source], side_recv.at[at, part])
            if part == 0:
                to_y(source)
            to_core(held[part], source)

    def lates(k, which):
        at = order[k]
        source = at * 2 + (x if which == 0 else 1 - x)
        arrive(expert_rows.at[late, source], y_recv.at[source])
        to_core(late, source)

    other_held = (tp_core * 2 + 1, tp_core * 2, ((1 - y) * 2 + 1 - core) * 2)
    other_late = ((1 - y) * 2 + 1 - core) * 2 + 1

    def experts(k):
        for which in range(2):
            source = order[k] * 2 + (x if which == 0 else 1 - x)
            for number in (*other_held, other_late):
                arrive(expert_rows.at[number, source], pair_recv.at[number, source])
            pieces, squares = [], None
            for number in range(parts):
                rows = expert_rows[number, source]
                pieces.append(rows * gain_ref[:, number * half : (number + 1) * half])
                wide = rows.astype(f32)
                squares = wide * wide if squares is None else squares + wide * wide
            inverse = lax.rsqrt(jnp.sum(squares, axis=1, keepdims=True) / width + EPSILON)
            joined = jnp.concatenate(pieces, axis=1)
            gate = jnp.dot(joined, gate_ref[...], preferred_element_type=f32) * inverse
            up = jnp.dot(joined, up_ref[...], preferred_element_type=f32) * inverse
            hidden = (swish(gate) * up * slot_weights[source][:, :1]).astype(bf16)
            hidden_rows[source] = hidden
            for number, row in ((0, y), (1, 1 - y)):
                slab = (row * 2 + 1 - core) * (2 * half)
                block = down_ref[:, pl.ds(pl.multiple_of(slab, 2 * half), 2 * half)]
                core_out[source, number] = jnp.dot(
                    hidden, block, preferred_element_type=f32
                ).astype(bf16)
            begin(
                remote(
                    core_out.at[source],
                    core_in.at[source],
                    back_core_send.at[source],
                    back_core_recv.at[source],
                    over_core,
                )
            )

    def pairs(k):
        for which in range(2):
            source = order[k] * 2 + (x if which == 0 else 1 - x)
            arrive(core_in.at[source], back_core_recv.at[source])
            hidden = hidden_rows[source]

            def summed(number, row):
                slab = (row * 2 + core) * (2 * half)
                block = down_ref[:, pl.ds(pl.multiple_of(slab, 2 * half), 2 * half)]
                return jnp.dot(hidden, block, preferred_element_type=f32) + core_in[
                    source, number
                ].astype(f32)

            other = summed(1, 1 - y)
            y_out[source] = other[:, half:].astype(bf16)
            begin(
                remote(
                    y_out.at[source],
                    y_in.at[source],
                    back_y_send.at[source],
                    back_y_recv.at[source],
                    over_y,
                )
            )
            results[source, 2] = other[:, :half].astype(bf16)
            mine = summed(0, y)
            results[source, 1] = mine[:, :half].astype(bf16)
            kept_rows[source] = mine[:, half:]

    def ready(k):
        at = order[k]
        for which in (1, 0):
            source = at * 2 + (x if which == 0 else 1 - x)
            if which == 1:
                for part in (2, 1):
                    give_side(at, source, part)
            arrive(y_in.at[source], back_y_recv.at[source])
            results[source, 0] = (kept_rows[source] + y_in[source].astype(f32)).astype(bf16)
            if which == 1:
                give_side(at, source, 0)

    def give_side(at, source, part):
        begin(
            remote(
                results.at[source, part],
                side_in.at[at, part],
                back_side_send.at[at, part],
                back_side_recv.at[at, part],
                side,
            )
        )

    def spread_back(at, part):
        arrive(side_in.at[at, part], back_side_recv.at[at, part])
        rows = jnp.concatenate([results[at * 2 + x, part], side_in[at, part]], axis=0)
        return jnp.dot(turned[at], rows, preferred_element_type=f32)

    def arrived(at, part):
        from_right = jnp.logical_and(at <= z, has_right)
        from_left = jnp.logical_and(at >= z, has_left)

        @pl.when(from_right)
        def _():
            arrive(right_in.at[at, part], right_recv.at[at, part])

        @pl.when(from_left)
        def _():
            arrive(left_in.at[at, part], left_recv.at[at, part])

        return jnp.where(from_right, right_in[at, part].astype(f32), 0.0) + jnp.where(
            from_left, left_in[at, part].astype(f32), 0.0
        )

    def back_lines(k):
        at = back_order[k]
        for part in (2, 1, 0):
            routed[part] = spread_back(at, part) + arrived(at, part)
            line_out[at, part] = routed[part].astype(bf16)
            source = line_out.at[at, part]
            begin(
                remote(
                    source,
                    right_in.at[at, part],
                    back_line_send.at[at, part],
                    right_recv.at[at, part],
                    left,
                ),
                at < z,
            )
            begin(
                remote(
                    source,
                    left_in.at[at, part],
                    back_line_send.at[at, part],
                    left_recv.at[at, part],
                    right,
                ),
                at > z,
            )

    def own_lines(part):
        routed[part] = spread_back(z, part) + arrived(z, part)

    def shared_first():
        for number in range(4):
            arrive(core_rows.at[number], core_recv.at[number])
        blocks = [
            (own_rows[1], tp * 2),
            (own_rows[0], tp * 2 + 1),
            (line_rows[z, 2], tp_y * 2),
            (partner_high[...], tp_y * 2 + 1),
            (core_rows[0], tp_core * 2),
            (core_rows[1], tp_core * 2 + 1),
            (core_rows[2], other_held[2]),
            (core_rows[3], other_late),
        ]
        squares = gate = up = 0.0
        for rows, number in blocks:
            wide = rows.astype(f32)
            squares = squares + wide * wide
            span = pl.ds(pl.multiple_of(number * half, half), half)
            scaled = rows * gain_ref[:, span]
            gate = gate + jnp.dot(scaled, shared_gate_ref[span, :], preferred_element_type=f32)
            up = up + jnp.dot(scaled, shared_up_ref[span, :], preferred_element_type=f32)
        inverse = lax.rsqrt(jnp.sum(squares, axis=1, keepdims=True) / width + EPSILON)
        shared_hidden[tp] = (swish(gate * inverse) * (up * inverse)).astype(bf16)
        for step in range(1, tp_count):
            peer = lax.rem(tp + step, tp_count)
            begin(
                remote(
                    shared_hidden.at[tp],
                    shared_hidden.at[tp],
                    shared_send.at[step],
                    shared_recv.at[tp],
                    (sp, peer),
                )
            )

    def shared_second():
        for step in range(1, tp_count):
            peer = lax.rem(tp + step, tp_count)
            arrive(shared_hidden.at[peer], shared_recv.at[peer])
        joined = jnp.concatenate([shared_hidden[number] for number in range(tp_count)], axis=1)
        base[...] = mid_ref[...].astype(f32) + jnp.dot(
            joined, shared_down_ref[...], preferred_element_type=f32
        )

    own_block()
    prepare(order[1], False)
    line(0)
    prepare(order[2], False)
    line(1)
    line(2)
    line(3)
    sides(0)
    prepare(order[3], False)
    line(4)
    lates(0, 1)
    for load in loads:
        load.wait()
    line(5)
    experts(0)
    line(6)
    sides(1)
    line(7)
    pairs(0)
    line(8)
    shared_first()
    sides(2)
    lates(1, 0)
    lates(1, 1)
    experts(1)
    ready(0)
    pairs(1)
    turn()
    lates(2, 0)
    lates(2, 1)
    experts(2)
    sides(3)
    ready(1)
    pairs(2)
    lates(3, 0)
    lates(3, 1)
    experts(3)
    pairs(3)
    ready(2)
    back_lines(0)
    ready(3)
    back_lines(1)
    back_lines(2)
    shared_second()
    own_lines(2)
    last_out[...] = routed[2].astype(bf16)
    begin(remote(last_out, last_in, last_send, last_recv, over_y))
    own_lines(1)
    own_lines(0)
    out_ref[:, half:] = (base[:, half:] + routed[0]).astype(bf16)
    arrive(last_in, last_recv)
    out_ref[:, :half] = (base[:, :half] + routed[1] + last_in[...].astype(f32)).astype(bf16)
    for copy, when in pending:
        if when is None:
            copy.wait_send()
        else:
            pl.when(when)(copy.wait_send)


def exchange_experts(
    mid_local,
    feedforward_gain,
    routing,
    router_score,
    expert_gate_weight,
    expert_up_weight,
    expert_down_weight,
    shared_expert_gate,
    shared_expert_up,
    shared_expert_down,
):
    sp_count, tp_count = lax.axis_size("sp"), lax.axis_size("tp")
    depth = sp_count // 2
    tokens, slab = mid_local.shape
    half = slab // 2
    parts = 2 * tp_count
    picked = routing.shape[1]
    most = 3 * tokens * picked // (2 * sp_count)
    gain = feedforward_gain.reshape(1, parts * half)
    bf16, f32 = jnp.bfloat16, jnp.float32
    vmem = pltpu.VMEM
    dma = pltpu.SemaphoreType.DMA
    hidden_width = expert_gate_weight.shape[1]
    in_vmem = pl.BlockSpec(memory_space=pltpu.VMEM)
    in_any = pl.BlockSpec(memory_space=pl.ANY)
    weights = (
        expert_gate_weight,
        expert_up_weight,
        expert_down_weight,
        shared_expert_gate,
        shared_expert_up,
        shared_expert_down,
    )
    return pl.pallas_call(
        functools.partial(exchange_kernel, most),
        name="exchange_experts",
        out_shape=jax.ShapeDtypeStruct(mid_local.shape, bf16),
        in_specs=[in_vmem] * 4 + [in_any] * len(weights),
        out_specs=in_vmem,
        scratch_shapes=[vmem(weight.shape, bf16) for weight in weights]
        + [
            vmem((sp_count, tokens), f32),
            vmem((sp_count, sp_count, tokens), f32),
            vmem((sp_count, sp_count, tokens), f32),
            vmem((sp_count, most, 128), f32),
            vmem((depth, 2 * most, tokens), bf16),
            vmem((depth, tokens, 2 * most), bf16),
            vmem((2, tokens, half), bf16),
            vmem((tokens, half), bf16),
            vmem((4, tokens, half), bf16),
            vmem((depth, EXPERT_PARTS, tokens, half), bf16),
            vmem((depth, EXPERT_PARTS, most, half), bf16),
            vmem((parts, sp_count, most, half), bf16),
            vmem((sp_count, most, hidden_width), bf16),
            vmem((sp_count, 2, most, slab), bf16),
            vmem((sp_count, 2, most, slab), bf16),
            vmem((sp_count, most, half), f32),
            vmem((sp_count, most, half), bf16),
            vmem((sp_count, most, half), bf16),
            vmem((sp_count, EXPERT_PARTS, most, half), bf16),
            vmem((depth, EXPERT_PARTS, most, half), bf16),
            vmem((depth, EXPERT_PARTS, tokens, half), bf16),
            vmem((depth, EXPERT_PARTS, tokens, half), bf16),
            vmem((depth, EXPERT_PARTS, tokens, half), bf16),
            vmem((tokens, half), bf16),
            vmem((tokens, half), bf16),
            vmem((tp_count, tokens, shared_expert_gate.shape[1]), bf16),
            vmem((EXPERT_PARTS, tokens, half), f32),
            vmem((tokens, slab), f32),
            dma((len(weights) + 1,)),
            dma((sp_count,)),
            dma((sp_count,)),
            dma((2,)),
            dma((2,)),
            dma((4,)),
            dma((4,)),
            dma((depth, EXPERT_PARTS)),
            dma((depth, EXPERT_PARTS)),
            dma((depth, EXPERT_PARTS)),
            dma((depth, EXPERT_PARTS)),
            dma((depth, EXPERT_PARTS)),
            dma((sp_count,)),
            dma((sp_count,)),
            dma((parts, sp_count)),
            dma((parts, sp_count)),
            dma((sp_count,)),
            dma((sp_count,)),
            dma((sp_count,)),
            dma((sp_count,)),
            dma((depth, EXPERT_PARTS)),
            dma((depth, EXPERT_PARTS)),
            dma((depth, EXPERT_PARTS)),
            dma((depth, EXPERT_PARTS)),
            dma((depth, EXPERT_PARTS)),
            dma((tp_count,)),
            dma((tp_count,)),
            dma,
            dma,
        ],
        compiler_params=pltpu.CompilerParams(
            collective_id=1, has_side_effects=True, vmem_limit_bytes=60 * 1024 * 1024
        ),
    )(mid_local, gain, routing.T, router_score.T, *weights)


def attend_kernel(
    extra_ref,
    norm_gain_ref,
    decay_hbm,
    key_hbm,
    value_hbm,
    query_hbm,
    gate_hbm,
    residual_hbm,
    projection_hbm,
    out_ref,
    decay_ref,
    key_ref,
    value_ref,
    query_ref,
    gate_ref,
    residual_ref,
    projection_ref,
    inside,
    query_start,
    decays,
    decays_in,
    state_out,
    state_in,
    carry_out,
    carry_in,
    local_mixed,
    head_rows,
    total,
    load_sem,
    decay_sems,
    state_send,
    state_recv,
    carry_send,
    carry_recv,
    y_send,
    y_recv,
    core_send,
    core_recv,
    pass_send,
    pass_recv,
):
    bf16, f32 = jnp.bfloat16, jnp.float32
    sp_count, tp_count = lax.axis_size("sp"), lax.axis_size("tp")
    depth = sp_count // 2
    head_count, tokens = extra_ref.shape
    blocks = tokens // BLOCK_POSITIONS
    sp, tp = lax.axis_index("sp"), lax.axis_index("tp")
    z, x = sp // 2, sp % 2
    y, core = tp // 2, tp % 2
    tp_y = (1 - y) * 2 + core
    tp_core = y * 2 + (1 - core)
    tp_far = (1 - y) * 2 + (1 - core)
    side, right = (z * 2 + 1 - x, tp), (sp + 2, tp)
    over_y, over_core = (sp, tp_y), (sp, tp_core)
    has_left, has_right = z > 0, z < depth - 1
    pending = []

    def begin(copy, when=None):
        if when is None:
            copy.start()
        else:
            pl.when(when)(copy.start)
        pending.append((copy, when))

    def arrive(target, sem):
        remote(target, target, decay_sems.at[0], sem, (sp, tp)).wait_recv()

    arrays = [
        (decay_hbm, decay_ref),
        (key_hbm, key_ref),
        (value_hbm, value_ref),
        (query_hbm, query_ref),
        (gate_hbm, gate_ref),
        (residual_hbm, residual_ref),
        (projection_hbm, projection_ref),
    ]
    loads = [
        pltpu.make_async_copy(hbm, ref, load_sem.at[number])
        for number, (hbm, ref) in enumerate(arrays)
    ]
    for load in loads:
        load.start()
    barrier = pltpu.get_barrier_semaphore()
    for peer in (side, over_y, over_core):
        pl.semaphore_signal(barrier, inc=1, device_id=peer, device_id_type=pl.DeviceIdType.MESH)
    for peer, exists in (((sp - 2, tp), has_left), (right, has_right)):
        @pl.when(exists)
        def _():
            pl.semaphore_signal(
                barrier, inc=1, device_id=peer, device_id_type=pl.DeviceIdType.MESH
            )

    row = lax.broadcasted_iota(jnp.int32, (tokens, tokens), 0)
    column = lax.broadcasted_iota(jnp.int32, (tokens, tokens), 1)
    causal = jnp.logical_and(
        column <= row, row // BLOCK_POSITIONS == column // BLOCK_POSITIONS
    )
    triangle = jnp.where(causal, 1.0, 0.0).astype(f32)
    over_first, over_rows = (((0,), (0,)), ((), ())), (((1,), (1,)), ((), ()))
    owner = (
        lax.broadcasted_iota(jnp.int32, (head_count, head_count * DK), 1) // DK
        == lax.broadcasted_iota(jnp.int32, (head_count, head_count * DK), 0)
    )
    extra = lax.dot_general(
        extra_ref[...],
        jnp.where(owner, 1.0, 0.0),
        over_first,
        precision=HIGHEST,
        preferred_element_type=f32,
    )
    loads[0].wait()
    preactivation = decay_ref[...].astype(f32)
    logs = jnp.minimum(preactivation, 0.0) - jnp.log1p(jnp.exp(-jnp.abs(preactivation)))
    logs = logs / GATE_TEMPER + extra
    inside[...] = jnp.dot(triangle, logs, precision=HIGHEST, preferred_element_type=f32)
    ends = [
        inside[(block + 1) * BLOCK_POSITIONS - 1 : (block + 1) * BLOCK_POSITIONS, :]
        for block in range(blocks)
    ]
    before = [jnp.zeros_like(ends[0])]
    for end in ends:
        before.append(before[-1] + end)
    decays[...] = jnp.broadcast_to(jnp.exp(before[blocks]), decays.shape)

    def span(block):
        return slice(block * BLOCK_POSITIONS, (block + 1) * BLOCK_POSITIONS)

    def columns(head, width):
        return slice(head * width, (head + 1) * width)

    loads[1].wait()
    loads[2].wait()
    pl.semaphore_wait(
        barrier, 3 + jnp.where(has_left, 1, 0) + jnp.where(has_right, 1, 0)
    )
    begin(remote(decays, decays_in, decay_sems.at[1], decay_sems.at[2], side))
    for head in range(head_count):
        wide = columns(head, DK)
        tail = jnp.concatenate(
            [
                before[blocks][:, wide] - before[block][:, wide] - inside[span(block), wide]
                for block in range(blocks)
            ],
            axis=0,
        )
        faded = (key_ref[:, wide].astype(f32) * jnp.exp(tail)).astype(bf16)
        state_out[head] = lax.dot_general(
            value_ref[:, columns(head, DV)], faded, over_first, preferred_element_type=f32
        ).astype(bf16)
        begin(
            remote(
                state_out.at[head],
                state_in.at[head],
                state_send.at[head],
                state_recv.at[head],
                side,
            )
        )

    def local(head):
        wide = columns(head, DK)
        values = value_ref[:, columns(head, DV)]
        keys = key_ref[:, wide].astype(f32)
        logs_inside = inside[:, wide]
        queries = query_ref[:, wide].astype(f32) * (DK**-0.5) * jnp.exp(logs_inside)
        query_decay = queries.astype(bf16)
        key_decay = (keys * jnp.exp(-logs_inside)).astype(bf16)
        scores = lax.dot_general(
            query_decay, key_decay, over_rows, preferred_element_type=f32
        )
        scores = jnp.where(causal, scores, 0.0).astype(bf16)
        mixed = jnp.dot(scores, values, preferred_element_type=f32)
        state, pieces, starts = None, [mixed[span(0)]], []
        for block in range(blocks):
            starts.append(queries[span(block)] * jnp.exp(before[block][:, wide]))
            if block == blocks - 1:
                break
            end = ends[block][:, wide]
            key_end = (keys[span(block)] * jnp.exp(end - logs_inside[span(block)])).astype(bf16)
            fresh = lax.dot_general(
                values[span(block)], key_end, over_first, preferred_element_type=f32
            )
            state = fresh if state is None else state * jnp.exp(end) + fresh
            passed = lax.dot_general(
                query_decay[span(block + 1)],
                state.astype(bf16),
                over_rows,
                preferred_element_type=f32,
            )
            pieces.append(mixed[span(block + 1)] + passed)
        local_mixed[head] = jnp.concatenate(pieces, axis=0)
        query_start[head] = jnp.concatenate(starts, axis=0).astype(bf16)

    def chain(head):
        wide = columns(head, DK)
        arrive(state_in.at[head], state_recv.at[head])
        own, other = state_out[head].astype(f32), state_in[head].astype(f32)
        decay_own, decay_other = decays[0:1, wide], decays_in[0:1, wide]
        first = jnp.where(x == 0, own, other)
        second = jnp.where(x == 0, other, own)
        decay_second = jnp.where(x == 0, decay_other, decay_own)

        @pl.when(has_left)
        def _():
            arrive(carry_in.at[head], carry_recv.at[head])

        entering = jnp.where(has_left, carry_in[head].astype(f32), 0.0)
        carry_out[head] = (
            decay_own * decay_other * entering + decay_second * first + second
        ).astype(bf16)
        begin(
            remote(
                carry_out.at[head],
                carry_in.at[head],
                carry_send.at[head],
                carry_recv.at[head],
                right,
            ),
            has_right,
        )
        return jnp.where(x == 0, entering, decay_other * entering + other).astype(bf16)

    def finish(head, entering):
        mixed = local_mixed[head] + lax.dot_general(
            query_start[head], entering, over_rows, preferred_element_type=f32
        )
        inverse = lax.rsqrt(jnp.mean(mixed * mixed, axis=1, keepdims=True) + EPSILON)
        opened = swish(gate_ref[:, columns(head, DV)].astype(f32))
        head_rows[tp, head] = (
            mixed * inverse * norm_gain_ref[...].astype(f32) * opened
        ).astype(bf16)
        source = head_rows.at[tp, head]
        begin(remote(source, source, y_send.at[head], y_recv.at[head], over_y))
        begin(remote(source, source, core_send.at[head], core_recv.at[head], over_core))

    def project(owner, head):
        start = (owner * head_count + head) * DV
        return jnp.dot(
            head_rows[owner, head],
            projection_ref[pl.ds(pl.multiple_of(start, DV), DV), :],
            preferred_element_type=f32,
        )

    def relay(head):
        target = head_rows.at[tp_y, head]
        arrive(target, y_recv.at[head])
        begin(remote(target, target, pass_send.at[head], pass_recv.at[head], over_core))

    loads[3].wait()
    for head in range(head_count):
        local(head)
    loads[4].wait()
    arrive(decays_in, decay_sems.at[2])
    for head in range(head_count):
        entering = chain(head)
        finish(head, entering)
        if head >= 2:
            relay(head - 2)
    loads[5].wait()
    loads[6].wait()
    total[...] = residual_ref[...].astype(f32) + sum(
        project(tp, head) for head in range(head_count)
    )
    for head in range(head_count):
        arrive(head_rows.at[tp_core, head], core_recv.at[head])
    total[...] = total[...] + sum(project(tp_core, head) for head in range(head_count))
    for head in range(head_count):
        if head >= 2:
            relay(head)
    for head in range(head_count):
        total[...] = total[...] + project(tp_y, head)
        arrive(head_rows.at[tp_far, head], pass_recv.at[head])
        total[...] = total[...] + project(tp_far, head)
    out_ref[...] = total[...].astype(bf16)
    for copy, when in pending:
        if when is None:
            copy.wait_send()
        else:
            pl.when(when)(copy.wait_send)


def attend_project(
    queries,
    key_matrix,
    value_matrix,
    output_gate_preactivation,
    decay_preactivation,
    extra_log_decay,
    head_norm_gain,
    residual,
    output_projection,
):
    bf16, f32 = jnp.bfloat16, jnp.float32
    arrays = (
        decay_preactivation,
        key_matrix,
        value_matrix,
        queries,
        output_gate_preactivation,
        residual,
        output_projection,
    )
    tokens, head_count = extra_log_decay.shape
    tp_count = lax.axis_size("tp")
    vmem, dma = pltpu.VMEM, pltpu.SemaphoreType.DMA
    in_vmem = pl.BlockSpec(memory_space=pltpu.VMEM)
    in_any = pl.BlockSpec(memory_space=pl.ANY)
    return pl.pallas_call(
        attend_kernel,
        name="attend_project",
        out_shape=jax.ShapeDtypeStruct(residual.shape, bf16),
        in_specs=[in_vmem] * 2 + [in_any] * len(arrays),
        out_specs=in_vmem,
        scratch_shapes=[vmem(array.shape, bf16) for array in arrays]
        + [
            vmem((tokens, head_count * DK), f32),
            vmem((head_count, tokens, DK), bf16),
            vmem((8, head_count * DK), f32),
            vmem((8, head_count * DK), f32),
            vmem((head_count, DV, DK), bf16),
            vmem((head_count, DV, DK), bf16),
            vmem((head_count, DV, DK), bf16),
            vmem((head_count, DV, DK), bf16),
            vmem((head_count, tokens, DV), f32),
            vmem((tp_count, head_count, tokens, DV), bf16),
            vmem(residual.shape, f32),
            dma((len(arrays),)),
            dma((3,)),
            dma((head_count,)),
            dma((head_count,)),
            dma((head_count,)),
            dma((head_count,)),
            dma((head_count,)),
            dma((head_count,)),
            dma((head_count,)),
            dma((head_count,)),
            dma((head_count,)),
            dma((head_count,)),
        ],
        compiler_params=pltpu.CompilerParams(
            collective_id=2, has_side_effects=True, vmem_limit_bytes=62 * 1024 * 1024
        ),
    )(extra_log_decay.T, head_norm_gain.reshape(1, DV), *arrays)


def attention_heads(queries, key_matrix, value_matrix, decay_preactivation, extra_log_decay):
    tokens = queries.shape[0]
    local_head_count = extra_log_decay.shape[1]
    block_count = tokens // BLOCK_POSITIONS
    query_block = queries.astype(jnp.float32).reshape(
        block_count, BLOCK_POSITIONS, local_head_count, DK
    ) * DK ** (-0.5)
    key_block = key_matrix.astype(jnp.float32).reshape(
        block_count, BLOCK_POSITIONS, local_head_count, DK
    )
    value_block = value_matrix.astype(jnp.float32).reshape(
        block_count, BLOCK_POSITIONS, local_head_count, DV
    )
    log_decay_rows = (
        jax.nn.log_sigmoid(decay_preactivation.astype(jnp.float32)).reshape(
            block_count, BLOCK_POSITIONS, local_head_count, DK
        )
        / GATE_TEMPER
    )
    log_decay_rows = (
        log_decay_rows
        + extra_log_decay.reshape(block_count, BLOCK_POSITIONS, local_head_count)[..., None]
    )
    inside = jnp.cumsum(log_decay_rows, axis=1)
    block_total = inside[:, -1]
    query_decay = query_block * jnp.exp(inside)
    key_decay = key_block * jnp.exp(-inside)
    causal = jnp.tril(jnp.ones((BLOCK_POSITIONS, BLOCK_POSITIONS), dtype=bool))
    scores = jnp.where(
        causal, jnp.einsum("nthd,nshd->nhts", query_decay, key_decay, precision=HIGHEST), 0.0
    )
    within = jnp.einsum("nhts,nshv->nthv", scores, value_block, precision=HIGHEST)
    key_end = key_block * jnp.exp(block_total[:, None] - inside)
    update = jnp.einsum("nshd,nshv->nhdv", key_end, value_block, precision=HIGHEST)
    before = jnp.cumsum(block_total, axis=0) - block_total
    ending = jnp.concatenate([before, (before[-1] + block_total[-1])[None]], axis=0)
    after_block = before + block_total
    earlier_mask = jnp.arange(block_count + 1)[:, None] > jnp.arange(block_count)[None, :]
    span_logs = jnp.where(
        earlier_mask[:, :, None, None], ending[:, None] - after_block[None], -1e30
    )
    states = jnp.einsum("nmhd,mhdv->nhdv", jnp.exp(span_logs), update, precision=HIGHEST)
    passed = jnp.einsum("nthd,nhdv->nthv", query_decay, states[:block_count], precision=HIGHEST)
    query_start = query_block * jnp.exp(inside + before[:, None])
    return (within + passed, query_start, jnp.exp(ending[block_count]), states[block_count])


def body(
    queries,
    key_matrix,
    value_matrix,
    output_gate_preactivation,
    decay_preactivation,
    extra_log_decay,
    head_norm_gain,
    output_projection,
    residual,
    feedforward_gain,
    routing,
    router_score,
    expert_gate_weight,
    expert_up_weight,
    expert_down_weight,
    shared_expert_gate,
    shared_expert_up,
    shared_expert_down,
):
    tokens = queries.shape[0]
    local_head_count = extra_log_decay.shape[1]
    if lax.axis_size("tp") == FF_PARTS and lax.axis_size("sp") == 8:
        mid_local = attend_project(
            queries,
            key_matrix,
            value_matrix,
            output_gate_preactivation,
            decay_preactivation,
            extra_log_decay,
            head_norm_gain,
            residual,
            output_projection,
        )
        return exchange_experts(
            mid_local,
            feedforward_gain,
            routing,
            router_score,
            expert_gate_weight,
            expert_up_weight,
            expert_down_weight,
            shared_expert_gate,
            shared_expert_up,
            shared_expert_down,
        )
    local_part, query_start, dev_decay, dev_update = attention_heads(
        queries, key_matrix, value_matrix, decay_preactivation, extra_log_decay
    )
    _, entering = prefix(
        (dev_decay, dev_update),
        "sp",
        carry_combine,
        (jnp.ones_like(dev_decay), jnp.zeros_like(dev_update)),
    )
    attention_output = local_part + jnp.einsum(
        "nthd,hdv->nthv", query_start, entering, precision=HIGHEST
    )
    attention_output = attention_output.reshape(tokens, local_head_count, DV)
    inverse_rms = lax.rsqrt(
        jnp.mean(attention_output * attention_output, axis=-1, keepdims=True) + EPSILON
    )
    gate_act = jax.nn.silu(
        output_gate_preactivation.astype(jnp.float32).reshape(tokens, local_head_count, DV)
    )
    head_rows = (
        (attention_output * inverse_rms * head_norm_gain.astype(jnp.float32) * gate_act)
        .reshape(tokens, local_head_count * DV)
        .astype(jnp.bfloat16)
    )
    tp_steps = [("tp", bit) for bit in range(lax.axis_size("tp").bit_length() - 1)][::-1]
    projected = jnp.dot(
        spread(head_rows, tp_steps),
        relative_rows(output_projection, lax.axis_index("tp"), masks_of(tp_steps, "tp")),
        preferred_element_type=jnp.float32,
    )
    mid_local = (residual.astype(jnp.float32) + projected).astype(jnp.bfloat16)
    mid_rows = lax.all_gather(mid_local, "tp", axis=1, tiled=True).astype(jnp.float32)
    normed = (
        mid_rows
        * lax.rsqrt(jnp.mean(mid_rows * mid_rows, axis=-1, keepdims=True) + EPSILON)
        * feedforward_gain.astype(jnp.float32)
    ).astype(jnp.bfloat16)
    shared_pre = jnp.dot(normed, shared_expert_gate, preferred_element_type=jnp.float32)
    shared_lin = jnp.dot(normed, shared_expert_up, preferred_element_type=jnp.float32)
    shared_hidden = (jax.nn.silu(shared_pre) * shared_lin).astype(jnp.bfloat16)
    senders = lax.axis_size("sp")
    tp_count = lax.axis_size("tp")
    tp_bits = tp_count.bit_length() - 1
    tp_index = lax.axis_index("tp")
    groups = tp_count // FF_PARTS
    group_here = tp_index // FF_PARTS
    part_here = tp_index % FF_PARTS
    model_width = normed.shape[1]
    picks = routing.shape[1]
    expert_total = senders * groups
    rows_most = max(2, 3 * tokens * picks // (2 * expert_total))
    slot_count = senders * rows_most
    flat_expert = routing.reshape(-1)
    one_hot = (flat_expert[:, None] == jnp.arange(expert_total, dtype=jnp.int32)[None, :]).astype(
        jnp.int32
    )
    rank_before = jnp.sum((jnp.cumsum(one_hot, axis=0) - one_hot) * one_hot, axis=1)
    owned = flat_expert % groups == group_here
    slot_index = jnp.where(owned, flat_expert // groups * rows_most + rank_before, slot_count)
    token_index = jnp.arange(flat_expert.shape[0], dtype=jnp.int32) // picks
    part_width = model_width // FF_PARTS
    normed_part = lax.dynamic_slice_in_dim(normed, part_here * part_width, part_width, 1)
    outgoing = (
        jnp.zeros((slot_count, part_width), jnp.bfloat16)
        .at[slot_index]
        .set(normed_part[token_index], mode="drop")
    )
    arrived = lax.all_to_all(
        outgoing.reshape(senders, rows_most, part_width),
        "sp",
        split_axis=0,
        concat_axis=0,
        tiled=True,
    )
    for bit in range(2):
        partner_cols = from_partner(arrived, "tp", bit)
        upper = (tp_index >> bit) % 2
        arrived = jnp.where(
            upper == 1,
            jnp.concatenate([partner_cols, arrived], axis=2),
            jnp.concatenate([arrived, partner_cols], axis=2),
        )
    rows_in = arrived.reshape(slot_count, model_width)
    gate_pre = jnp.dot(rows_in, expert_gate_weight, preferred_element_type=jnp.float32)
    up_pre = jnp.dot(rows_in, expert_up_weight, preferred_element_type=jnp.float32)
    routed_hidden = (jax.nn.silu(gate_pre) * up_pre).astype(jnp.bfloat16)
    partial_out = jnp.dot(routed_hidden, expert_down_weight, preferred_element_type=jnp.float32)
    slab_width = model_width // tp_count
    partial_out = partial_out.reshape(slot_count, groups, FF_PARTS, slab_width)
    for bit in (1, 0):
        paired = partial_out.reshape(slot_count, groups, 2, 2**bit, slab_width)
        upper = (tp_index >> bit) % 2
        kept = lax.dynamic_index_in_dim(paired, upper, 2, keepdims=False)
        given = lax.dynamic_index_in_dim(paired, 1 - upper, 2, keepdims=False)
        partial_out = kept + from_partner(given.astype(jnp.bfloat16), "tp", bit).astype(given.dtype)
    expert_out = partial_out.reshape(senders, rows_most, groups, slab_width).astype(jnp.bfloat16)
    shared_out = jnp.dot(
        lax.all_gather(shared_hidden, "tp", axis=1, tiled=True),
        shared_expert_down,
        preferred_element_type=jnp.float32,
    )
    returned = lax.all_to_all(expert_out, "sp", split_axis=0, concat_axis=0, tiled=True).reshape(
        slot_count, groups, slab_width
    )
    safe_slot = jnp.minimum(slot_index, slot_count - 1)
    route_weight = ROUTE_SCALE * router_score / jnp.sum(router_score, axis=1, keepdims=True)
    pair_weight = jnp.where(owned, route_weight.reshape(-1), 0.0)
    picked = returned[safe_slot].astype(jnp.float32) * pair_weight[:, None, None]
    routed_part = jnp.sum(picked.reshape(tokens, picks, groups, slab_width), axis=1)
    for bit in range(tp_bits - 1, 1, -1):
        paired = routed_part.reshape(tokens, 2, 2 ** (bit - 2), slab_width)
        upper = (tp_index >> bit) % 2
        kept = lax.dynamic_index_in_dim(paired, upper, 1, keepdims=False)
        given = lax.dynamic_index_in_dim(paired, 1 - upper, 1, keepdims=False)
        routed_part = kept + from_partner(as_sent(given), "tp", bit).astype(given.dtype)
    routed = routed_part.reshape(tokens, slab_width)
    return (mid_local.astype(jnp.float32) + routed + shared_out).astype(jnp.bfloat16)


def solution(mesh):
    return jax.shard_map(
        body,
        mesh=mesh,
        in_specs=(
            P("sp", "tp"),
            P("sp", "tp"),
            P("sp", "tp"),
            P("sp", "tp"),
            P("sp", "tp"),
            P("sp", "tp"),
            P(),
            P(None, "tp"),
            P("sp", "tp"),
            P(),
            P("sp", None),
            P("sp", None),
            P(None, ("sp", "tp")),
            P(None, ("sp", "tp")),
            P(("sp", "tp"), None),
            P(None, "tp"),
            P(None, "tp"),
            P(None, "tp"),
        ),
        out_specs=P("sp", "tp"),
        check_vma=False,
    )
```

```python
import functools

import jax
import jax.numpy as jnp
from jax import lax
from jax.experimental import pallas as pl
from jax.experimental.pallas import tpu as pltpu
from jax.sharding import PartitionSpec as P

DK = 128
DV = 256
BLOCK_POSITIONS = 64
FF_PARTS = 4

HIGHEST = lax.Precision.HIGHEST
EPSILON = 1e-06
ROUTE_SCALE = 2.5
GATE_TEMPER = 16.0


def from_partner(value, axis, bit, upward=False):
    mask = 2**bit
    pairs = [(source, source ^ mask) for source in range(lax.axis_size(axis))]
    if upward:
        pairs = [(source, target) for source, target in pairs if source < target]
    return lax.ppermute(value, axis, pairs)


def as_sent(value):
    return jax.tree.map(lambda a: a.astype(jnp.bfloat16) if a.dtype == jnp.float32 else a, value)


def carry_combine(first_part, second_part):
    return (
        first_part[0] * second_part[0],
        second_part[0][..., None] * first_part[1] + second_part[1],
    )


def choose(flag, yes, no):
    return jax.tree.map(lambda a, b: jnp.where(flag, a, b), yes, no)


def prefix(value, axis, join, neutral):
    place = lax.axis_index(axis)
    bits = lax.axis_size(axis).bit_length() - 1
    total, state = value, neutral
    for bit in range(bits):
        upper = (place >> bit) % 2 == 1
        last = bit == bits - 1
        arrived = jax.tree.map(
            lambda a: from_partner(a.astype(jnp.bfloat16), axis, bit, last).astype(a.dtype), total
        )
        state = choose(upper, join(arrived, state), state)
        if not last:
            total = choose(upper, join(arrived, total), join(total, arrived))
    return state


def relative_rows(matrix, place, masks):
    height = matrix.shape[0] // len(masks)
    return jnp.concatenate(
        [lax.dynamic_slice_in_dim(matrix, (place ^ mask) * height, height, 0) for mask in masks], 0
    )


def relative_columns(matrix, place, masks):
    width = matrix.shape[1] // len(masks)
    return jnp.concatenate(
        [lax.dynamic_slice_in_dim(matrix, (place ^ mask) * width, width, 1) for mask in masks], 1
    )


def masks_of(steps, axis):
    masks = [0]
    for step_axis, bit in steps:
        if step_axis == axis:
            masks = masks + [mask ^ (2**bit) for mask in masks]
    return masks


def spread(value, steps):
    for axis, bit in steps:
        arrived = from_partner(value, axis, bit)
        value = jnp.concatenate([value, arrived], 0 if axis == "sp" else 1)
    return value


def collect(value, steps):
    for axis, bit in reversed(steps):
        own, given = jnp.split(value, 2, 0 if axis == "sp" else 1)
        value = (
            own.astype(jnp.float32) + from_partner(given, axis, bit).astype(jnp.float32)
        ).astype(jnp.bfloat16)
    return value


EXPERT_PARTS = 3


def remote(source, target, send_sem, recv_sem, device):
    return pltpu.make_async_remote_copy(
        src_ref=source,
        dst_ref=target,
        send_sem=send_sem,
        recv_sem=recv_sem,
        device_id=device,
        device_id_type=pl.DeviceIdType.MESH,
    )


def swish(value):
    return value / (1.0 + jnp.exp(-value))


def exchange_kernel(
    most,
    mid_ref,
    gain_ref,
    routing_ref,
    score_ref,
    gate_hbm,
    up_hbm,
    down_hbm,
    shared_gate_hbm,
    shared_up_hbm,
    shared_down_hbm,
    out_ref,
    gate_ref,
    up_ref,
    down_ref,
    shared_gate_ref,
    shared_up_ref,
    shared_down_ref,
    table_ref,
    tables,
    ranks,
    slot_weights,
    picks,
    turned,
    own_rows,
    partner_high,
    core_rows,
    line_rows,
    side_out,
    expert_rows,
    hidden_rows,
    core_out,
    core_in,
    kept_rows,
    y_out,
    y_in,
    results,
    side_in,
    line_out,
    left_in,
    right_in,
    last_out,
    last_in,
    shared_hidden,
    routed,
    base,
    weight_sem,
    table_send,
    table_recv,
    own_send,
    own_recv,
    core_send,
    core_recv,
    left_send,
    right_send,
    line_recv,
    side_send,
    side_recv,
    y_send,
    y_recv,
    pair_send,
    pair_recv,
    back_core_send,
    back_core_recv,
    back_y_send,
    back_y_recv,
    back_side_send,
    back_side_recv,
    back_line_send,
    left_recv,
    right_recv,
    shared_send,
    shared_recv,
    last_send,
    last_recv,
):
    bf16, f32 = jnp.bfloat16, jnp.float32
    sp_count, tp_count = lax.axis_size("sp"), lax.axis_size("tp")
    depth = sp_count // 2
    tokens = mid_ref.shape[0]
    half = mid_ref.shape[1] // 2
    parts = 2 * tp_count
    width = half * parts
    sp, tp = lax.axis_index("sp"), lax.axis_index("tp")
    z, x = sp // 2, sp % 2
    y, core = tp // 2, tp % 2
    tp_y = (1 - y) * 2 + core
    tp_core = y * 2 + (1 - core)
    side = (z * 2 + 1 - x, tp)
    over_y = (sp, tp_y)
    over_core = (sp, tp_core)
    left, right = (sp - 2, tp), (sp + 2, tp)
    has_left, has_right = z > 0, z < depth - 1
    pending = []

    def begin(copy, when=None):
        if when is None:
            copy.start()
        else:
            pl.when(when)(copy.start)
        pending.append((copy, when))

    def arrive(target, sem):
        remote(target, target, weight_sem.at[0], sem, (sp, tp)).wait_recv()

    order = [
        z,
        jnp.where(z == 0, 1, jnp.where(z == 1, 0, jnp.where(z == 2, 3, 2))),
        jnp.where(z == 0, 2, jnp.where(z == 1, 2, jnp.where(z == 2, 1, 1))),
        jnp.where(z == 0, 3, jnp.where(z == 1, 3, 0)),
    ]
    back_order = [
        jnp.where(z == 0, 1, jnp.where(z == 1, 2, jnp.where(z == 2, 1, 2))),
        jnp.where(z == 0, 2, jnp.where(z == 1, 3, jnp.where(z == 2, 0, 1))),
        jnp.where(z == 0, 3, jnp.where(z == 1, 0, jnp.where(z == 2, 3, 0))),
        z,
    ]

    barrier = pltpu.get_barrier_semaphore()
    peers = [(lax.rem(sp + step, sp_count), tp) for step in range(1, sp_count)]
    peers += [(sp, lax.rem(tp + step, tp_count)) for step in range(1, tp_count)]
    for peer in peers:
        pl.semaphore_signal(barrier, inc=1, device_id=peer, device_id_type=pl.DeviceIdType.MESH)
    weights = [
        (gate_hbm, gate_ref),
        (up_hbm, up_ref),
        (down_hbm, down_ref),
        (shared_gate_hbm, shared_gate_ref),
        (shared_up_hbm, shared_up_ref),
        (shared_down_hbm, shared_down_ref),
    ]
    loads = [
        pltpu.make_async_copy(hbm, vmem, weight_sem.at[number + 1])
        for number, (hbm, vmem) in enumerate(weights)
    ]
    for load in loads:
        load.start()
    score = score_ref[...]
    route_weight = ROUTE_SCALE * score / jnp.sum(score, axis=0, keepdims=True)
    experts_here = lax.broadcasted_iota(jnp.int32, table_ref.shape, 0)
    table = jnp.zeros(table_ref.shape, f32)
    for pick_at in range(score.shape[0]):
        table = table + jnp.where(
            routing_ref[pick_at : pick_at + 1, :] == experts_here,
            route_weight[pick_at : pick_at + 1, :],
            0.0,
        )
    table_ref[...] = table
    pl.semaphore_wait(barrier, len(peers))

    low, high = mid_ref.at[:, pl.ds(0, half)], mid_ref.at[:, pl.ds(half, half)]
    for step in range(1, sp_count):
        peer = lax.rem(sp + step, sp_count)
        begin(
            remote(table_ref, tables.at[sp], table_send.at[step], table_recv.at[sp], (peer, tp))
        )
    begin(remote(low, line_rows.at[z, 2], own_send.at[0], own_recv.at[0], over_y))
    for part, source in ((0, high), (1, low)):
        target = line_rows.at[z, part]
        begin(remote(source, target, left_send.at[z, part], line_recv.at[z, part], left), has_left)
        begin(
            remote(source, target, right_send.at[z, part], line_recv.at[z, part], right), has_right
        )
    begin(remote(high, partner_high, own_send.at[1], own_recv.at[1], over_y))
    begin(remote(low, core_rows.at[0], core_send.at[0], core_recv.at[0], over_core))
    begin(remote(high, core_rows.at[1], core_send.at[1], core_recv.at[1], over_core))
    own_rows[0] = mid_ref[:, half:]
    own_rows[1] = mid_ref[:, :half]
    tables[sp] = table_ref[...]

    earlier = (
        lax.broadcasted_iota(jnp.int32, (tokens, tokens), 0)
        < lax.broadcasted_iota(jnp.int32, (tokens, tokens), 1)
    ).astype(f32).astype(bf16)
    slots = lax.broadcasted_iota(jnp.int32, (most, tokens), 0).astype(f32)

    def rank_block(source):
        chosen = tables[source] > 0.0
        counts = jnp.dot(
            jnp.where(chosen, 1.0, 0.0).astype(bf16), earlier, preferred_element_type=f32
        )
        ranks[source] = jnp.where(chosen, counts, -1.0)

    def pick(source, expert):
        return slots == ranks[source, pl.ds(expert, 1), :]

    def slot_block(source):
        weight = jnp.where(pick(source, sp), tables[source, pl.ds(sp, 1), :], 0.0)
        slot_weights[source] = jnp.broadcast_to(
            jnp.sum(weight, axis=1, keepdims=True), (most, 128)
        )

    def pick_block(depth_at):
        source = depth_at * 2 + x
        chosen = jnp.concatenate(
            [
                jnp.where(pick(source, expert), 1.0, 0.0)
                for expert in (sp, z * 2 + 1 - x)
            ],
            axis=0,
        )
        picks[depth_at] = chosen.astype(bf16)

    def turn():
        for depth_at in range(depth):
            turned[depth_at] = picks[depth_at].astype(f32).T.astype(bf16)

    def prepare(depth_at, first):
        for source in (depth_at * 2 + x, depth_at * 2 + 1 - x):
            if first:
                @pl.when(source != sp)
                def _():
                    arrive(tables.at[source], table_recv.at[source])
            else:
                arrive(tables.at[source], table_recv.at[source])
            rank_block(source)
            slot_block(source)
        pick_block(depth_at)

    prepare(order[0], True)
    arrive(line_rows.at[z, 2], own_recv.at[0])
    target = line_rows.at[z, 2]
    begin(remote(target, target, left_send.at[z, 2], line_recv.at[z, 2], left), has_left)
    begin(remote(target, target, right_send.at[z, 2], line_recv.at[z, 2], right), has_right)
    begin(remote(target, core_rows.at[2], core_send.at[2], core_recv.at[2], over_core))

    held = (tp * 2 + 1, tp * 2, tp_y * 2)
    late = tp_y * 2 + 1

    def to_core(number, source):
        ref = expert_rows.at[number, source]
        begin(
            remote(ref, ref, pair_send.at[number, source], pair_recv.at[number, source], over_core)
        )

    def to_y(source):
        ref = expert_rows.at[held[0], source]
        begin(remote(ref, ref, y_send.at[source], y_recv.at[source], over_y))

    def compact(at, part, number, rows):
        source = at * 2 + x
        chosen = jnp.dot(picks[at], rows, preferred_element_type=f32).astype(bf16)
        side_out[at, part] = chosen[most:]
        begin(
            remote(
                side_out.at[at, part],
                expert_rows.at[number, source],
                side_send.at[at, part],
                side_recv.at[at, part],
                side,
            )
        )
        expert_rows[number, source] = chosen[:most]

    def own_block():
        source = sp
        for part in range(EXPERT_PARTS):
            rows = line_rows[z, 2] if part == 2 else own_rows[part]
            compact(z, part, held[part], rows)
            to_core(held[part], source)
        arrive(partner_high, own_recv.at[1])
        begin(remote(partner_high, core_rows.at[3], core_send.at[3], core_recv.at[3], over_core))
        expert_rows[late, source] = jnp.dot(
            picks[z, pl.ds(0, most), :], partner_high[...], preferred_element_type=f32
        ).astype(bf16)
        to_core(late, source)

    inner = jnp.logical_and(has_left, has_right)
    turns = [(1, 0), (2, 0), (1, 1), (2, 1), (1, 2), (2, 2), (3, 0), (3, 1), (3, 2)]

    def line(number):
        (k, part), (plain_k, plain_part) = turns[number], divmod(number, EXPERT_PARTS)
        at = jnp.where(inner, order[k], order[plain_k + 1])
        part = jnp.where(inner, part, plain_part)
        ref = line_rows.at[at, part]
        arrive(ref, line_recv.at[at, part])
        begin(
            remote(ref, ref, left_send.at[at, part], line_recv.at[at, part], left),
            jnp.logical_and(at > z, has_left),
        )
        begin(
            remote(ref, ref, right_send.at[at, part], line_recv.at[at, part], right),
            jnp.logical_and(at < z, has_right),
        )
        part_number = jnp.where(part == 0, held[0], jnp.where(part == 1, held[1], held[2]))
        compact(at, part, part_number, line_rows[at, part])
        source = at * 2 + x
        ref = expert_rows.at[part_number, source]
        begin(
            remote(ref, ref, y_send.at[source], y_recv.at[source], over_y),
            part == 0,
        )
        to_core(part_number, source)

    def sides(k):
        at = order[k]
        source = at * 2 + 1 - x
        for part in range(EXPERT_PARTS):
            arrive(expert_rows.at[held[part], source], side_recv.at[at, part])
            if part == 0:
                to_y(source)
            to_core(held[part], source)

    def lates(k, which):
        at = order[k]
        source = at * 2 + (x if which == 0 else 1 - x)
        arrive(expert_rows.at[late, source], y_recv.at[source])
        to_core(late, source)

    other_held = (tp_core * 2 + 1, tp_core * 2, ((1 - y) * 2 + 1 - core) * 2)
    other_late = ((1 - y) * 2 + 1 - core) * 2 + 1

    def experts(k):
        for which in range(2):
            source = order[k] * 2 + (x if which == 0 else 1 - x)
            for number in (*other_held, other_late):
                arrive(expert_rows.at[number, source], pair_recv.at[number, source])
            pieces, squares = [], None
            for number in range(parts):
                rows = expert_rows[number, source]
                pieces.append(rows * gain_ref[:, number * half : (number + 1) * half])
                wide = rows.astype(f32)
                squares = wide * wide if squares is None else squares + wide * wide
            inverse = lax.rsqrt(jnp.sum(squares, axis=1, keepdims=True) / width + EPSILON)
            joined = jnp.concatenate(pieces, axis=1)
            gate = jnp.dot(joined, gate_ref[...], preferred_element_type=f32) * inverse
            up = jnp.dot(joined, up_ref[...], preferred_element_type=f32) * inverse
            hidden = (swish(gate) * up * slot_weights[source][:, :1]).astype(bf16)
            hidden_rows[source] = hidden
            for number, row in ((0, y), (1, 1 - y)):
                slab = (row * 2 + 1 - core) * (2 * half)
                block = down_ref[:, pl.ds(pl.multiple_of(slab, 2 * half), 2 * half)]
                core_out[source, number] = jnp.dot(
                    hidden, block, preferred_element_type=f32
                ).astype(bf16)
            begin(
                remote(
                    core_out.at[source],
                    core_in.at[source],
                    back_core_send.at[source],
                    back_core_recv.at[source],
                    over_core,
                )
            )

    def pairs(k):
        for which in range(2):
            source = order[k] * 2 + (x if which == 0 else 1 - x)
            arrive(core_in.at[source], back_core_recv.at[source])
            hidden = hidden_rows[source]

            def summed(number, row):
                slab = (row * 2 + core) * (2 * half)
                block = down_ref[:, pl.ds(pl.multiple_of(slab, 2 * half), 2 * half)]
                return jnp.dot(hidden, block, preferred_element_type=f32) + core_in[
                    source, number
                ].astype(f32)

            other = summed(1, 1 - y)
            y_out[source] = other[:, half:].astype(bf16)
            begin(
                remote(
                    y_out.at[source],
                    y_in.at[source],
                    back_y_send.at[source],
                    back_y_recv.at[source],
                    over_y,
                )
            )
            results[source, 2] = other[:, :half].astype(bf16)
            mine = summed(0, y)
            results[source, 1] = mine[:, :half].astype(bf16)
            kept_rows[source] = mine[:, half:]

    def ready(k):
        at = order[k]
        for which in (1, 0):
            source = at * 2 + (x if which == 0 else 1 - x)
            if which == 1:
                for part in (2, 1):
                    give_side(at, source, part)
            arrive(y_in.at[source], back_y_recv.at[source])
            results[source, 0] = (kept_rows[source] + y_in[source].astype(f32)).astype(bf16)
            if which == 1:
                give_side(at, source, 0)

    def give_side(at, source, part):
        begin(
            remote(
                results.at[source, part],
                side_in.at[at, part],
                back_side_send.at[at, part],
                back_side_recv.at[at, part],
                side,
            )
        )

    def spread_back(at, part):
        arrive(side_in.at[at, part], back_side_recv.at[at, part])
        rows = jnp.concatenate([results[at * 2 + x, part], side_in[at, part]], axis=0)
        return jnp.dot(turned[at], rows, preferred_element_type=f32)

    def arrived(at, part):
        from_right = jnp.logical_and(at <= z, has_right)
        from_left = jnp.logical_and(at >= z, has_left)

        @pl.when(from_right)
        def _():
            arrive(right_in.at[at, part], right_recv.at[at, part])

        @pl.when(from_left)
        def _():
            arrive(left_in.at[at, part], left_recv.at[at, part])

        return jnp.where(from_right, right_in[at, part].astype(f32), 0.0) + jnp.where(
            from_left, left_in[at, part].astype(f32), 0.0
        )

    def back_lines(k):
        at = back_order[k]
        for part in (2, 1, 0):
            routed[part] = spread_back(at, part) + arrived(at, part)
            line_out[at, part] = routed[part].astype(bf16)
            source = line_out.at[at, part]
            begin(
                remote(
                    source,
                    right_in.at[at, part],
                    back_line_send.at[at, part],
                    right_recv.at[at, part],
                    left,
                ),
                at < z,
            )
            begin(
                remote(
                    source,
                    left_in.at[at, part],
                    back_line_send.at[at, part],
                    left_recv.at[at, part],
                    right,
                ),
                at > z,
            )

    def own_lines(part):
        routed[part] = spread_back(z, part) + arrived(z, part)

    def shared_first():
        for number in range(4):
            arrive(core_rows.at[number], core_recv.at[number])
        blocks = [
            (own_rows[1], tp * 2),
            (own_rows[0], tp * 2 + 1),
            (line_rows[z, 2], tp_y * 2),
            (partner_high[...], tp_y * 2 + 1),
            (core_rows[0], tp_core * 2),
            (core_rows[1], tp_core * 2 + 1),
            (core_rows[2], other_held[2]),
            (core_rows[3], other_late),
        ]
        squares = gate = up = 0.0
        for rows, number in blocks:
            wide = rows.astype(f32)
            squares = squares + wide * wide
            span = pl.ds(pl.multiple_of(number * half, half), half)
            scaled = rows * gain_ref[:, span]
            gate = gate + jnp.dot(scaled, shared_gate_ref[span, :], preferred_element_type=f32)
            up = up + jnp.dot(scaled, shared_up_ref[span, :], preferred_element_type=f32)
        inverse = lax.rsqrt(jnp.sum(squares, axis=1, keepdims=True) / width + EPSILON)
        shared_hidden[tp] = (swish(gate * inverse) * (up * inverse)).astype(bf16)
        for step in range(1, tp_count):
            peer = lax.rem(tp + step, tp_count)
            begin(
                remote(
                    shared_hidden.at[tp],
                    shared_hidden.at[tp],
                    shared_send.at[step],
                    shared_recv.at[tp],
                    (sp, peer),
                )
            )

    def shared_second():
        for step in range(1, tp_count):
            peer = lax.rem(tp + step, tp_count)
            arrive(shared_hidden.at[peer], shared_recv.at[peer])
        joined = jnp.concatenate([shared_hidden[number] for number in range(tp_count)], axis=1)
        base[...] = mid_ref[...].astype(f32) + jnp.dot(
            joined, shared_down_ref[...], preferred_element_type=f32
        )

    own_block()
    prepare(order[1], False)
    line(0)
    prepare(order[2], False)
    line(1)
    line(2)
    line(3)
    sides(0)
    prepare(order[3], False)
    line(4)
    lates(0, 1)
    for load in loads:
        load.wait()
    line(5)
    experts(0)
    line(6)
    sides(1)
    line(7)
    pairs(0)
    line(8)
    shared_first()
    sides(2)
    lates(1, 0)
    lates(1, 1)
    experts(1)
    ready(0)
    pairs(1)
    turn()
    lates(2, 0)
    lates(2, 1)
    experts(2)
    sides(3)
    pairs(2)
    ready(1)
    lates(3, 0)
    lates(3, 1)
    experts(3)
    pairs(3)
    ready(2)
    back_lines(0)
    ready(3)
    back_lines(1)
    back_lines(2)
    shared_second()
    own_lines(2)
    last_out[...] = routed[2].astype(bf16)
    begin(remote(last_out, last_in, last_send, last_recv, over_y))
    own_lines(1)
    own_lines(0)
    out_ref[:, half:] = (base[:, half:] + routed[0]).astype(bf16)
    arrive(last_in, last_recv)
    out_ref[:, :half] = (base[:, :half] + routed[1] + last_in[...].astype(f32)).astype(bf16)
    for copy, when in pending:
        if when is None:
            copy.wait_send()
        else:
            pl.when(when)(copy.wait_send)


def exchange_experts(
    mid_local,
    feedforward_gain,
    routing,
    router_score,
    expert_gate_weight,
    expert_up_weight,
    expert_down_weight,
    shared_expert_gate,
    shared_expert_up,
    shared_expert_down,
):
    sp_count, tp_count = lax.axis_size("sp"), lax.axis_size("tp")
    depth = sp_count // 2
    tokens, slab = mid_local.shape
    half = slab // 2
    parts = 2 * tp_count
    picked = routing.shape[1]
    most = 3 * tokens * picked // (2 * sp_count)
    gain = feedforward_gain.reshape(1, parts * half)
    bf16, f32 = jnp.bfloat16, jnp.float32
    vmem = pltpu.VMEM
    dma = pltpu.SemaphoreType.DMA
    hidden_width = expert_gate_weight.shape[1]
    in_vmem = pl.BlockSpec(memory_space=pltpu.VMEM)
    in_any = pl.BlockSpec(memory_space=pl.ANY)
    weights = (
        expert_gate_weight,
        expert_up_weight,
        expert_down_weight,
        shared_expert_gate,
        shared_expert_up,
        shared_expert_down,
    )
    return pl.pallas_call(
        functools.partial(exchange_kernel, most),
        name="exchange_experts",
        out_shape=jax.ShapeDtypeStruct(mid_local.shape, bf16),
        in_specs=[in_vmem] * 4 + [in_any] * len(weights),
        out_specs=in_vmem,
        scratch_shapes=[vmem(weight.shape, bf16) for weight in weights]
        + [
            vmem((sp_count, tokens), f32),
            vmem((sp_count, sp_count, tokens), f32),
            vmem((sp_count, sp_count, tokens), f32),
            vmem((sp_count, most, 128), f32),
            vmem((depth, 2 * most, tokens), bf16),
            vmem((depth, tokens, 2 * most), bf16),
            vmem((2, tokens, half), bf16),
            vmem((tokens, half), bf16),
            vmem((4, tokens, half), bf16),
            vmem((depth, EXPERT_PARTS, tokens, half), bf16),
            vmem((depth, EXPERT_PARTS, most, half), bf16),
            vmem((parts, sp_count, most, half), bf16),
            vmem((sp_count, most, hidden_width), bf16),
            vmem((sp_count, 2, most, slab), bf16),
            vmem((sp_count, 2, most, slab), bf16),
            vmem((sp_count, most, half), f32),
            vmem((sp_count, most, half), bf16),
            vmem((sp_count, most, half), bf16),
            vmem((sp_count, EXPERT_PARTS, most, half), bf16),
            vmem((depth, EXPERT_PARTS, most, half), bf16),
            vmem((depth, EXPERT_PARTS, tokens, half), bf16),
            vmem((depth, EXPERT_PARTS, tokens, half), bf16),
            vmem((depth, EXPERT_PARTS, tokens, half), bf16),
            vmem((tokens, half), bf16),
            vmem((tokens, half), bf16),
            vmem((tp_count, tokens, shared_expert_gate.shape[1]), bf16),
            vmem((EXPERT_PARTS, tokens, half), f32),
            vmem((tokens, slab), f32),
            dma((len(weights) + 1,)),
            dma((sp_count,)),
            dma((sp_count,)),
            dma((2,)),
            dma((2,)),
            dma((4,)),
            dma((4,)),
            dma((depth, EXPERT_PARTS)),
            dma((depth, EXPERT_PARTS)),
            dma((depth, EXPERT_PARTS)),
            dma((depth, EXPERT_PARTS)),
            dma((depth, EXPERT_PARTS)),
            dma((sp_count,)),
            dma((sp_count,)),
            dma((parts, sp_count)),
            dma((parts, sp_count)),
            dma((sp_count,)),
            dma((sp_count,)),
            dma((sp_count,)),
            dma((sp_count,)),
            dma((depth, EXPERT_PARTS)),
            dma((depth, EXPERT_PARTS)),
            dma((depth, EXPERT_PARTS)),
            dma((depth, EXPERT_PARTS)),
            dma((depth, EXPERT_PARTS)),
            dma((tp_count,)),
            dma((tp_count,)),
            dma,
            dma,
        ],
        compiler_params=pltpu.CompilerParams(
            collective_id=1, has_side_effects=True, vmem_limit_bytes=60 * 1024 * 1024
        ),
    )(mid_local, gain, routing.T, router_score.T, *weights)


def attend_kernel(
    extra_ref,
    norm_gain_ref,
    decay_hbm,
    key_hbm,
    value_hbm,
    query_hbm,
    gate_hbm,
    residual_hbm,
    projection_hbm,
    out_ref,
    decay_ref,
    key_ref,
    value_ref,
    query_ref,
    gate_ref,
    residual_ref,
    projection_ref,
    inside,
    query_start,
    decays,
    decays_in,
    state_out,
    state_in,
    carry_first,
    carry_out,
    carry_in,
    local_mixed,
    head_rows,
    total,
    load_sem,
    decay_sems,
    state_send,
    state_recv,
    carry_send,
    carry_recv,
    y_send,
    y_recv,
    core_send,
    core_recv,
    pass_send,
    pass_recv,
):
    bf16, f32 = jnp.bfloat16, jnp.float32
    sp_count, tp_count = lax.axis_size("sp"), lax.axis_size("tp")
    depth = sp_count // 2
    head_count, tokens = extra_ref.shape
    blocks = tokens // BLOCK_POSITIONS
    sp, tp = lax.axis_index("sp"), lax.axis_index("tp")
    z, x = sp // 2, sp % 2
    y, core = tp // 2, tp % 2
    tp_y = (1 - y) * 2 + core
    tp_core = y * 2 + (1 - core)
    tp_far = (1 - y) * 2 + (1 - core)
    side, right = (z * 2 + 1 - x, tp), (sp + 2, tp)
    over_y, over_core = (sp, tp_y), (sp, tp_core)
    has_left, has_right = z > 0, z < depth - 1
    pending = []

    def begin(copy, when=None):
        if when is None:
            copy.start()
        else:
            pl.when(when)(copy.start)
        pending.append((copy, when))

    def arrive(target, sem):
        remote(target, target, decay_sems.at[0], sem, (sp, tp)).wait_recv()

    arrays = [
        (decay_hbm, decay_ref),
        (key_hbm, key_ref),
        (value_hbm, value_ref),
        (query_hbm, query_ref),
        (gate_hbm, gate_ref),
        (residual_hbm, residual_ref),
        (projection_hbm, projection_ref),
    ]
    loads = [
        pltpu.make_async_copy(hbm, ref, load_sem.at[number])
        for number, (hbm, ref) in enumerate(arrays)
    ]
    for load in loads:
        load.start()
    barrier = pltpu.get_barrier_semaphore()
    for peer in (side, over_y, over_core):
        pl.semaphore_signal(barrier, inc=1, device_id=peer, device_id_type=pl.DeviceIdType.MESH)
    for peer, exists in (((sp - 2, tp), has_left), (right, has_right)):
        @pl.when(exists)
        def _():
            pl.semaphore_signal(
                barrier, inc=1, device_id=peer, device_id_type=pl.DeviceIdType.MESH
            )

    row = lax.broadcasted_iota(jnp.int32, (tokens, tokens), 0)
    column = lax.broadcasted_iota(jnp.int32, (tokens, tokens), 1)
    causal = jnp.logical_and(
        column <= row, row // BLOCK_POSITIONS == column // BLOCK_POSITIONS
    )
    triangle = jnp.where(causal, 1.0, 0.0).astype(f32)
    over_first, over_rows = (((0,), (0,)), ((), ())), (((1,), (1,)), ((), ()))
    owner = (
        lax.broadcasted_iota(jnp.int32, (head_count, head_count * DK), 1) // DK
        == lax.broadcasted_iota(jnp.int32, (head_count, head_count * DK), 0)
    )
    extra = lax.dot_general(
        extra_ref[...],
        jnp.where(owner, 1.0, 0.0),
        over_first,
        precision=HIGHEST,
        preferred_element_type=f32,
    )
    loads[0].wait()
    preactivation = decay_ref[...].astype(f32)
    logs = jnp.minimum(preactivation, 0.0) - jnp.log1p(jnp.exp(-jnp.abs(preactivation)))
    logs = logs / GATE_TEMPER + extra
    inside[...] = jnp.dot(triangle, logs, precision=HIGHEST, preferred_element_type=f32)
    ends = [
        inside[(block + 1) * BLOCK_POSITIONS - 1 : (block + 1) * BLOCK_POSITIONS, :]
        for block in range(blocks)
    ]
    before = [jnp.zeros_like(ends[0])]
    for end in ends:
        before.append(before[-1] + end)
    decays[...] = jnp.broadcast_to(jnp.exp(before[blocks]), decays.shape)

    def span(block):
        return slice(block * BLOCK_POSITIONS, (block + 1) * BLOCK_POSITIONS)

    def columns(head, width):
        return slice(head * width, (head + 1) * width)

    loads[1].wait()
    loads[2].wait()
    pl.semaphore_wait(
        barrier, 3 + jnp.where(has_left, 1, 0) + jnp.where(has_right, 1, 0)
    )
    begin(remote(decays, decays_in, decay_sems.at[1], decay_sems.at[2], side))
    for head in range(head_count):
        wide = columns(head, DK)
        tail = jnp.concatenate(
            [
                before[blocks][:, wide] - before[block][:, wide] - inside[span(block), wide]
                for block in range(blocks)
            ],
            axis=0,
        )
        faded = (key_ref[:, wide].astype(f32) * jnp.exp(tail)).astype(bf16)
        state_out[head] = lax.dot_general(
            value_ref[:, columns(head, DV)], faded, over_first, preferred_element_type=f32
        ).astype(bf16)
        begin(
            remote(
                state_out.at[head],
                state_in.at[head],
                state_send.at[head],
                state_recv.at[head],
                side,
            )
        )

    def local(head):
        wide = columns(head, DK)
        values = value_ref[:, columns(head, DV)]
        keys = key_ref[:, wide].astype(f32)
        logs_inside = inside[:, wide]
        queries = query_ref[:, wide].astype(f32) * (DK**-0.5) * jnp.exp(logs_inside)
        query_decay = queries.astype(bf16)
        key_decay = (keys * jnp.exp(-logs_inside)).astype(bf16)
        scores = lax.dot_general(
            query_decay, key_decay, over_rows, preferred_element_type=f32
        )
        scores = jnp.where(causal, scores, 0.0).astype(bf16)
        mixed = jnp.dot(scores, values, preferred_element_type=f32)
        state, pieces, starts = None, [mixed[span(0)]], []
        for block in range(blocks):
            starts.append(queries[span(block)] * jnp.exp(before[block][:, wide]))
            if block == blocks - 1:
                break
            end = ends[block][:, wide]
            key_end = (keys[span(block)] * jnp.exp(end - logs_inside[span(block)])).astype(bf16)
            fresh = lax.dot_general(
                values[span(block)], key_end, over_first, preferred_element_type=f32
            )
            state = fresh if state is None else state * jnp.exp(end) + fresh
            passed = lax.dot_general(
                query_decay[span(block + 1)],
                state.astype(bf16),
                over_rows,
                preferred_element_type=f32,
            )
            pieces.append(mixed[span(block + 1)] + passed)
        local_mixed[head] = jnp.concatenate(pieces, axis=0)
        query_start[head] = jnp.concatenate(starts, axis=0).astype(bf16)

    def joined(head):
        wide = columns(head, DK)
        own, other = state_out[head].astype(f32), state_in[head].astype(f32)
        first = jnp.where(x == 0, own, other)
        second = jnp.where(x == 0, other, own)
        decay_second = jnp.where(x == 0, decays_in[0:1, wide], decays[0:1, wide])
        return decay_second * first + second

    def give(source, head, when):
        begin(
            remote(
                source.at[head],
                carry_in.at[head],
                carry_send.at[head],
                carry_recv.at[head],
                right,
            ),
            when,
        )

    def lead(head):
        arrive(state_in.at[head], state_recv.at[head])
        carry_first[head] = joined(head).astype(bf16)
        give(carry_first, head, jnp.logical_not(has_left))

    def chain(head):
        wide = columns(head, DK)
        decay_own, decay_other = decays[0:1, wide], decays_in[0:1, wide]

        @pl.when(has_left)
        def _():
            arrive(carry_in.at[head], carry_recv.at[head])

        entering = jnp.where(has_left, carry_in[head].astype(f32), 0.0)
        carry_out[head] = (decay_own * decay_other * entering + joined(head)).astype(bf16)
        give(carry_out, head, jnp.logical_and(has_left, has_right))
        other = state_in[head].astype(f32)
        return jnp.where(x == 0, entering, decay_other * entering + other).astype(bf16)

    def finish(head, entering):
        mixed = local_mixed[head] + lax.dot_general(
            query_start[head], entering, over_rows, preferred_element_type=f32
        )
        inverse = lax.rsqrt(jnp.mean(mixed * mixed, axis=1, keepdims=True) + EPSILON)
        opened = swish(gate_ref[:, columns(head, DV)].astype(f32))
        head_rows[tp, head] = (
            mixed * inverse * norm_gain_ref[...].astype(f32) * opened
        ).astype(bf16)
        source = head_rows.at[tp, head]
        begin(remote(source, source, y_send.at[head], y_recv.at[head], over_y))
        begin(remote(source, source, core_send.at[head], core_recv.at[head], over_core))

    def project(owner, head):
        start = (owner * head_count + head) * DV
        return jnp.dot(
            head_rows[owner, head],
            projection_ref[pl.ds(pl.multiple_of(start, DV), DV), :],
            preferred_element_type=f32,
        )

    def relay(head):
        target = head_rows.at[tp_y, head]
        arrive(target, y_recv.at[head])
        begin(remote(target, target, pass_send.at[head], pass_recv.at[head], over_core))

    loads[3].wait()
    local(0)
    arrive(decays_in, decay_sems.at[2])
    for head in range(head_count):
        lead(head)
        if head + 1 < head_count:
            local(head + 1)
    loads[4].wait()
    for head in range(head_count):
        entering = chain(head)
        finish(head, entering)
        if head >= 2:
            relay(head - 2)
    loads[5].wait()
    loads[6].wait()
    total[...] = residual_ref[...].astype(f32) + sum(
        project(tp, head) for head in range(head_count)
    )
    for head in range(head_count):
        arrive(head_rows.at[tp_core, head], core_recv.at[head])
    total[...] = total[...] + sum(project(tp_core, head) for head in range(head_count))
    for head in range(head_count):
        if head >= 2:
            relay(head)
    for head in range(head_count):
        total[...] = total[...] + project(tp_y, head)
        arrive(head_rows.at[tp_far, head], pass_recv.at[head])
        total[...] = total[...] + project(tp_far, head)
    out_ref[...] = total[...].astype(bf16)
    for copy, when in pending:
        if when is None:
            copy.wait_send()
        else:
            pl.when(when)(copy.wait_send)


def attend_project(
    queries,
    key_matrix,
    value_matrix,
    output_gate_preactivation,
    decay_preactivation,
    extra_log_decay,
    head_norm_gain,
    residual,
    output_projection,
):
    bf16, f32 = jnp.bfloat16, jnp.float32
    arrays = (
        decay_preactivation,
        key_matrix,
        value_matrix,
        queries,
        output_gate_preactivation,
        residual,
        output_projection,
    )
    tokens, head_count = extra_log_decay.shape
    tp_count = lax.axis_size("tp")
    vmem, dma = pltpu.VMEM, pltpu.SemaphoreType.DMA
    in_vmem = pl.BlockSpec(memory_space=pltpu.VMEM)
    in_any = pl.BlockSpec(memory_space=pl.ANY)
    return pl.pallas_call(
        attend_kernel,
        name="attend_project",
        out_shape=jax.ShapeDtypeStruct(residual.shape, bf16),
        in_specs=[in_vmem] * 2 + [in_any] * len(arrays),
        out_specs=in_vmem,
        scratch_shapes=[vmem(array.shape, bf16) for array in arrays]
        + [
            vmem((tokens, head_count * DK), f32),
            vmem((head_count, tokens, DK), bf16),
            vmem((8, head_count * DK), f32),
            vmem((8, head_count * DK), f32),
            vmem((head_count, DV, DK), bf16),
            vmem((head_count, DV, DK), bf16),
            vmem((head_count, DV, DK), bf16),
            vmem((head_count, DV, DK), bf16),
            vmem((head_count, DV, DK), bf16),
            vmem((head_count, tokens, DV), f32),
            vmem((tp_count, head_count, tokens, DV), bf16),
            vmem(residual.shape, f32),
            dma((len(arrays),)),
            dma((3,)),
            dma((head_count,)),
            dma((head_count,)),
            dma((head_count,)),
            dma((head_count,)),
            dma((head_count,)),
            dma((head_count,)),
            dma((head_count,)),
            dma((head_count,)),
            dma((head_count,)),
            dma((head_count,)),
        ],
        compiler_params=pltpu.CompilerParams(
            collective_id=2, has_side_effects=True, vmem_limit_bytes=62 * 1024 * 1024
        ),
    )(extra_log_decay.T, head_norm_gain.reshape(1, DV), *arrays)


def attention_heads(queries, key_matrix, value_matrix, decay_preactivation, extra_log_decay):
    tokens = queries.shape[0]
    local_head_count = extra_log_decay.shape[1]
    block_count = tokens // BLOCK_POSITIONS
    query_block = queries.astype(jnp.float32).reshape(
        block_count, BLOCK_POSITIONS, local_head_count, DK
    ) * DK ** (-0.5)
    key_block = key_matrix.astype(jnp.float32).reshape(
        block_count, BLOCK_POSITIONS, local_head_count, DK
    )
    value_block = value_matrix.astype(jnp.float32).reshape(
        block_count, BLOCK_POSITIONS, local_head_count, DV
    )
    log_decay_rows = (
        jax.nn.log_sigmoid(decay_preactivation.astype(jnp.float32)).reshape(
            block_count, BLOCK_POSITIONS, local_head_count, DK
        )
        / GATE_TEMPER
    )
    log_decay_rows = (
        log_decay_rows
        + extra_log_decay.reshape(block_count, BLOCK_POSITIONS, local_head_count)[..., None]
    )
    inside = jnp.cumsum(log_decay_rows, axis=1)
    block_total = inside[:, -1]
    query_decay = query_block * jnp.exp(inside)
    key_decay = key_block * jnp.exp(-inside)
    causal = jnp.tril(jnp.ones((BLOCK_POSITIONS, BLOCK_POSITIONS), dtype=bool))
    scores = jnp.where(
        causal, jnp.einsum("nthd,nshd->nhts", query_decay, key_decay, precision=HIGHEST), 0.0
    )
    within = jnp.einsum("nhts,nshv->nthv", scores, value_block, precision=HIGHEST)
    key_end = key_block * jnp.exp(block_total[:, None] - inside)
    update = jnp.einsum("nshd,nshv->nhdv", key_end, value_block, precision=HIGHEST)
    before = jnp.cumsum(block_total, axis=0) - block_total
    ending = jnp.concatenate([before, (before[-1] + block_total[-1])[None]], axis=0)
    after_block = before + block_total
    earlier_mask = jnp.arange(block_count + 1)[:, None] > jnp.arange(block_count)[None, :]
    span_logs = jnp.where(
        earlier_mask[:, :, None, None], ending[:, None] - after_block[None], -1e30
    )
    states = jnp.einsum("nmhd,mhdv->nhdv", jnp.exp(span_logs), update, precision=HIGHEST)
    passed = jnp.einsum("nthd,nhdv->nthv", query_decay, states[:block_count], precision=HIGHEST)
    query_start = query_block * jnp.exp(inside + before[:, None])
    return (within + passed, query_start, jnp.exp(ending[block_count]), states[block_count])


def body(
    queries,
    key_matrix,
    value_matrix,
    output_gate_preactivation,
    decay_preactivation,
    extra_log_decay,
    head_norm_gain,
    output_projection,
    residual,
    feedforward_gain,
    routing,
    router_score,
    expert_gate_weight,
    expert_up_weight,
    expert_down_weight,
    shared_expert_gate,
    shared_expert_up,
    shared_expert_down,
):
    tokens = queries.shape[0]
    local_head_count = extra_log_decay.shape[1]
    if lax.axis_size("tp") == FF_PARTS and lax.axis_size("sp") == 8:
        mid_local = attend_project(
            queries,
            key_matrix,
            value_matrix,
            output_gate_preactivation,
            decay_preactivation,
            extra_log_decay,
            head_norm_gain,
            residual,
            output_projection,
        )
        return exchange_experts(
            mid_local,
            feedforward_gain,
            routing,
            router_score,
            expert_gate_weight,
            expert_up_weight,
            expert_down_weight,
            shared_expert_gate,
            shared_expert_up,
            shared_expert_down,
        )
    local_part, query_start, dev_decay, dev_update = attention_heads(
        queries, key_matrix, value_matrix, decay_preactivation, extra_log_decay
    )
    _, entering = prefix(
        (dev_decay, dev_update),
        "sp",
        carry_combine,
        (jnp.ones_like(dev_decay), jnp.zeros_like(dev_update)),
    )
    attention_output = local_part + jnp.einsum(
        "nthd,hdv->nthv", query_start, entering, precision=HIGHEST
    )
    attention_output = attention_output.reshape(tokens, local_head_count, DV)
    inverse_rms = lax.rsqrt(
        jnp.mean(attention_output * attention_output, axis=-1, keepdims=True) + EPSILON
    )
    gate_act = jax.nn.silu(
        output_gate_preactivation.astype(jnp.float32).reshape(tokens, local_head_count, DV)
    )
    head_rows = (
        (attention_output * inverse_rms * head_norm_gain.astype(jnp.float32) * gate_act)
        .reshape(tokens, local_head_count * DV)
        .astype(jnp.bfloat16)
    )
    tp_steps = [("tp", bit) for bit in range(lax.axis_size("tp").bit_length() - 1)][::-1]
    projected = jnp.dot(
        spread(head_rows, tp_steps),
        relative_rows(output_projection, lax.axis_index("tp"), masks_of(tp_steps, "tp")),
        preferred_element_type=jnp.float32,
    )
    mid_local = (residual.astype(jnp.float32) + projected).astype(jnp.bfloat16)
    mid_rows = lax.all_gather(mid_local, "tp", axis=1, tiled=True).astype(jnp.float32)
    normed = (
        mid_rows
        * lax.rsqrt(jnp.mean(mid_rows * mid_rows, axis=-1, keepdims=True) + EPSILON)
        * feedforward_gain.astype(jnp.float32)
    ).astype(jnp.bfloat16)
    shared_pre = jnp.dot(normed, shared_expert_gate, preferred_element_type=jnp.float32)
    shared_lin = jnp.dot(normed, shared_expert_up, preferred_element_type=jnp.float32)
    shared_hidden = (jax.nn.silu(shared_pre) * shared_lin).astype(jnp.bfloat16)
    senders = lax.axis_size("sp")
    tp_count = lax.axis_size("tp")
    tp_bits = tp_count.bit_length() - 1
    tp_index = lax.axis_index("tp")
    groups = tp_count // FF_PARTS
    group_here = tp_index // FF_PARTS
    part_here = tp_index % FF_PARTS
    model_width = normed.shape[1]
    picks = routing.shape[1]
    expert_total = senders * groups
    rows_most = max(2, 3 * tokens * picks // (2 * expert_total))
    slot_count = senders * rows_most
    flat_expert = routing.reshape(-1)
    one_hot = (flat_expert[:, None] == jnp.arange(expert_total, dtype=jnp.int32)[None, :]).astype(
        jnp.int32
    )
    rank_before = jnp.sum((jnp.cumsum(one_hot, axis=0) - one_hot) * one_hot, axis=1)
    owned = flat_expert % groups == group_here
    slot_index = jnp.where(owned, flat_expert // groups * rows_most + rank_before, slot_count)
    token_index = jnp.arange(flat_expert.shape[0], dtype=jnp.int32) // picks
    part_width = model_width // FF_PARTS
    normed_part = lax.dynamic_slice_in_dim(normed, part_here * part_width, part_width, 1)
    outgoing = (
        jnp.zeros((slot_count, part_width), jnp.bfloat16)
        .at[slot_index]
        .set(normed_part[token_index], mode="drop")
    )
    arrived = lax.all_to_all(
        outgoing.reshape(senders, rows_most, part_width),
        "sp",
        split_axis=0,
        concat_axis=0,
        tiled=True,
    )
    for bit in range(2):
        partner_cols = from_partner(arrived, "tp", bit)
        upper = (tp_index >> bit) % 2
        arrived = jnp.where(
            upper == 1,
            jnp.concatenate([partner_cols, arrived], axis=2),
            jnp.concatenate([arrived, partner_cols], axis=2),
        )
    rows_in = arrived.reshape(slot_count, model_width)
    gate_pre = jnp.dot(rows_in, expert_gate_weight, preferred_element_type=jnp.float32)
    up_pre = jnp.dot(rows_in, expert_up_weight, preferred_element_type=jnp.float32)
    routed_hidden = (jax.nn.silu(gate_pre) * up_pre).astype(jnp.bfloat16)
    partial_out = jnp.dot(routed_hidden, expert_down_weight, preferred_element_type=jnp.float32)
    slab_width = model_width // tp_count
    partial_out = partial_out.reshape(slot_count, groups, FF_PARTS, slab_width)
    for bit in (1, 0):
        paired = partial_out.reshape(slot_count, groups, 2, 2**bit, slab_width)
        upper = (tp_index >> bit) % 2
        kept = lax.dynamic_index_in_dim(paired, upper, 2, keepdims=False)
        given = lax.dynamic_index_in_dim(paired, 1 - upper, 2, keepdims=False)
        partial_out = kept + from_partner(given.astype(jnp.bfloat16), "tp", bit).astype(given.dtype)
    expert_out = partial_out.reshape(senders, rows_most, groups, slab_width).astype(jnp.bfloat16)
    shared_out = jnp.dot(
        lax.all_gather(shared_hidden, "tp", axis=1, tiled=True),
        shared_expert_down,
        preferred_element_type=jnp.float32,
    )
    returned = lax.all_to_all(expert_out, "sp", split_axis=0, concat_axis=0, tiled=True).reshape(
        slot_count, groups, slab_width
    )
    safe_slot = jnp.minimum(slot_index, slot_count - 1)
    route_weight = ROUTE_SCALE * router_score / jnp.sum(router_score, axis=1, keepdims=True)
    pair_weight = jnp.where(owned, route_weight.reshape(-1), 0.0)
    picked = returned[safe_slot].astype(jnp.float32) * pair_weight[:, None, None]
    routed_part = jnp.sum(picked.reshape(tokens, picks, groups, slab_width), axis=1)
    for bit in range(tp_bits - 1, 1, -1):
        paired = routed_part.reshape(tokens, 2, 2 ** (bit - 2), slab_width)
        upper = (tp_index >> bit) % 2
        kept = lax.dynamic_index_in_dim(paired, upper, 1, keepdims=False)
        given = lax.dynamic_index_in_dim(paired, 1 - upper, 1, keepdims=False)
        routed_part = kept + from_partner(as_sent(given), "tp", bit).astype(given.dtype)
    routed = routed_part.reshape(tokens, slab_width)
    return (mid_local.astype(jnp.float32) + routed + shared_out).astype(jnp.bfloat16)


def solution(mesh):
    return jax.shard_map(
        body,
        mesh=mesh,
        in_specs=(
            P("sp", "tp"),
            P("sp", "tp"),
            P("sp", "tp"),
            P("sp", "tp"),
            P("sp", "tp"),
            P("sp", "tp"),
            P(),
            P(None, "tp"),
            P("sp", "tp"),
            P(),
            P("sp", None),
            P("sp", None),
            P(None, ("sp", "tp")),
            P(None, ("sp", "tp")),
            P(("sp", "tp"), None),
            P(None, "tp"),
            P(None, "tp"),
            P(None, "tp"),
        ),
        out_specs=P("sp", "tp"),
        check_vma=False,
    )
```
